32 devices in a mesh: sp: 8 (over z, y), tp: 4 (over x, core).
Axes of the slice: x: 2, y: 2, z: 4, core: 2. Of those that a mesh axis runs over, the one named last changes fastest.
Arguments:
- tokens: bfloat16 [2048, 2048], P(('sp', 'tp')), may hold values from -6 to 6
- pre_gain: float32 [2048], replicated, may hold values from 0.1 to 1.9
- w_query_ret: bfloat16 [2048, 768], P('sp', 'tp'), may hold values from -0.125 to 0.125
- w_key_ret: bfloat16 [2048, 768], P('sp', 'tp'), may hold values from -0.125 to 0.125
- w_value_ret: bfloat16 [2048, 768], P('sp', 'tp'), may hold values from -0.125 to 0.125
- w_query_att: bfloat16 [2048, 768], P('sp', 'tp'), may hold values from -0.5 to 0.5
- w_key_att: bfloat16 [2048, 256], P('sp', 'tp'), may hold values from -0.125 to 0.125
- w_value_att: bfloat16 [2048, 256], P('sp', 'tp'), may hold values from -0.125 to 0.125
- w_out_ret: bfloat16 [768, 2048], P('tp', 'sp'), may hold values from -0.15625 to 0.15625
- w_out_att: bfloat16 [768, 2048], P('tp', 'sp'), may hold values from -0.15625 to 0.15625
- retain_log: float32 [2048, 12], P('sp', 'tp')
- forget_total: float32 [12, 2048], P('tp'), as said below
Outputs:
- mixed: bfloat16 [2048, 2048], P(('sp', 'tp'))
The draws below stay inside these ranges and needn't reach their ends.
Inputs may be any that keep to these rules, and one draw needn't show every extreme that they name: `forget_total`: never rises along positions.
All inputs are finite; a program needn't handle non-finite values.
Results may differ from the reference program's by a relative error of at most 0.019.
Values may be sent and summed in bfloat16 or wider, within the bound.
A program may use at most 64 MiB of HBM per device.

```python
import math
import jax
import jax.numpy as jnp
from jax import lax

D = 2048
HEAD = 64
R_HEADS = 12
F_HEADS = 12
KV_HEADS = 4
SPAN = 256
TOK_DEV = 256
TOKENS = 2048
N_TP = 4


def log_rates(key, heads):
    keys = jax.random.split(key, 6)
    order = jax.random.permutation(keys[0], heads)
    slow = order < heads // 2
    blocks = TOKENS // TOK_DEV
    spread = jnp.exp(jax.random.uniform(keys[1], (blocks, heads), jnp.float32, math.log(0.4), math.log(2.5)))
    spread = jnp.repeat(spread, TOK_DEV, axis=0)
    rough = jax.random.uniform(keys[2], (TOKENS, heads), jnp.float32, 0.5, 1.5)
    fast = jnp.exp(jax.random.uniform(keys[3], (heads,), jnp.float32, math.log(0.03), math.log(0.1)))
    base = jnp.where(slow, 0.2 * math.log(10.0) / TOKENS, fast)
    rates = base[None, :] * spread * rough
    places = jax.random.randint(keys[4], (2, heads), 0, TOKENS)
    losses = jax.random.uniform(keys[5], (2, heads), jnp.float32, 0.2, 0.4)
    struck = jnp.arange(TOKENS, dtype=jnp.int32)[:, None, None] == places[None, :, :]
    rates = rates - jnp.sum(jnp.where(struck, jnp.log(1.0 - losses)[None, :, :], 0.0), axis=1)
    return -rates


def draw_retain_log(key, part):
    return log_rates(jax.random.fold_in(key, 11), R_HEADS)


def draw_forget_total(key, part):
    return jnp.transpose(jnp.cumsum(log_rates(jax.random.fold_in(key, 23), F_HEADS), axis=0))


def block_levels(own_key, extent, cuts, least, high):
    factor_of, own = 1.0, jax.random.fold_in(own_key, 6)
    for dim, shards_of in cuts:
        heights = jnp.exp(jax.random.uniform(jax.random.fold_in(own, dim), (shards_of,), jnp.float32, least / len(cuts), high / len(cuts)))
        factor_of = factor_of * jnp.repeat(heights, extent[dim] // shards_of).reshape([-1 if axis == dim else 1 for axis in range(len(extent))])
    return factor_of


def scatter_about(stream_key, dims, deviation, reach, cuts=(), kind=jnp.bfloat16):
    values = deviation * jax.random.normal(stream_key, dims, jnp.float32)
    if cuts:
        values = values * block_levels(stream_key, dims, cuts, -0.22, 0.18)
    return jnp.clip(values, -reach, reach).astype(kind)


def setup_inputs(seed: int = 0) -> dict:
    seeds = jax.random.split(jax.random.key(seed), 13)
    tokens = scatter_about(seeds[0], (TOKENS, D), 1.0, 6.0, ((0, 32),))
    pre_gain = jnp.clip(1.0 + 0.18 * jax.random.normal(seeds[1], (D,), jnp.float32), 0.1, 1.9)
    w_query_ret = scatter_about(seeds[2], (D, R_HEADS * HEAD), D ** -0.5, 0.125, ((0, 8), (1, 4)))
    w_key_ret = scatter_about(seeds[3], (D, R_HEADS * HEAD), D ** -0.5, 0.125, ((0, 8), (1, 4)))
    w_value_ret = scatter_about(seeds[4], (D, R_HEADS * HEAD), D ** -0.5, 0.125, ((0, 8), (1, 4)))
    w_query_att = scatter_about(seeds[5], (D, F_HEADS * HEAD), (D // 16) ** -0.5, 0.5, ((0, 8), (1, 4)))
    w_key_att = scatter_about(seeds[6], (D, KV_HEADS * HEAD), D ** -0.5, 0.125, ((0, 8), (1, 4)))
    w_value_att = scatter_about(seeds[7], (D, KV_HEADS * HEAD), D ** -0.5, 0.125, ((0, 8), (1, 4)))
    w_out_ret = scatter_about(seeds[8], (R_HEADS * HEAD, D), (2 * R_HEADS * HEAD) ** -0.5, 0.15625, ((0, 4), (1, 8)))
    w_out_att = scatter_about(seeds[9], (F_HEADS * HEAD, D), (2 * F_HEADS * HEAD) ** -0.5, 0.15625, ((0, 4), (1, 8)))
    retain_log = draw_retain_log(jax.random.fold_in(seeds[12], 71), 0)
    forget_total = draw_forget_total(jax.random.fold_in(seeds[12], 71), 0)
    return dict(tokens=tokens, pre_gain=pre_gain, w_query_ret=w_query_ret, w_key_ret=w_key_ret, w_value_ret=w_value_ret, w_query_att=w_query_att, w_key_att=w_key_att, w_value_att=w_value_att, w_out_ret=w_out_ret, w_out_att=w_out_att, retain_log=retain_log, forget_total=forget_total)


EPS = 1e-06
THETA = 10000.0

def rotate(field, positions):
    half = field.shape[-1] // 2
    inverse = THETA ** (-jnp.arange(half, dtype=jnp.float32) / half)
    angles = positions[:, None] * inverse[None, :]
    cosine = jnp.cos(angles)[:, None, :]
    sine = jnp.sin(angles)[:, None, :]
    first_half = field[..., :half]
    second_half = field[..., half:]
    return jnp.concatenate([first_half * cosine - second_half * sine, first_half * sine + second_half * cosine], axis=-1)

def head_norm(values):
    centre = lax.optimization_barrier(jnp.mean(values, axis=-1, keepdims=True))
    spread = lax.optimization_barrier(jnp.mean(jnp.square(values - centre), axis=-1, keepdims=True))
    return (values - centre) * lax.rsqrt(spread + EPS)

def lowered(values):
    return lax.optimization_barrier(values.astype(jnp.bfloat16)).astype(jnp.float32)

def retain_block(state, inputs):
    query, key_rows, value_rows, logs = inputs
    within = jnp.cumsum(logs, axis=0)
    span = logs.shape[0]
    causal = jnp.arange(span)[:, None] >= jnp.arange(span)[None, :]
    scores = jnp.einsum('thd,shd->hts', query.astype(jnp.float32), key_rows.astype(jnp.float32))
    gap = jnp.where(causal, jnp.transpose(within)[:, :, None] - jnp.transpose(within)[:, None, :], 0.0)
    weights = jnp.where(causal, scores * jnp.exp(gap), 0.0).astype(jnp.bfloat16)
    local = jnp.einsum('hts,shd->thd', weights.astype(jnp.float32), value_rows.astype(jnp.float32))
    lifted = lowered(query.astype(jnp.float32) * jnp.exp(within)[:, :, None])
    carried = jnp.einsum('thd,hde->the', lifted, lowered(state))
    last = within[-1]
    faded = lowered(key_rows.astype(jnp.float32) * jnp.exp(last[None, :] - within)[:, :, None])
    update = jnp.einsum('shd,she->hde', faded, value_rows.astype(jnp.float32))
    return (jnp.exp(last)[:, None, None] * state + update, local + carried)

def project(normed, weight):
    return jnp.dot(normed, weight, preferred_element_type=jnp.float32)

def reference(tokens, pre_gain, w_query_ret, w_key_ret, w_value_ret, w_query_att, w_key_att, w_value_att, w_out_ret, w_out_att, retain_log, forget_total):
    rows = tokens.astype(jnp.float32)
    normed = (rows * lax.rsqrt(lax.optimization_barrier(jnp.mean(rows * rows, axis=-1, keepdims=True)) + EPS) * pre_gain.astype(jnp.float32)).astype(jnp.bfloat16)
    positions = jnp.arange(TOKENS, dtype=jnp.int32).astype(jnp.float32)
    shape = (TOKENS, R_HEADS, HEAD)
    ret_query = (rotate(project(normed, w_query_ret).reshape(shape), positions) * HEAD ** (-0.5)).astype(jnp.bfloat16)
    ret_key = rotate(project(normed, w_key_ret).reshape(shape), positions).astype(jnp.bfloat16)
    ret_value = project(normed, w_value_ret).astype(jnp.bfloat16).reshape(shape)
    blocks = TOKENS // SPAN
    start_state = jnp.zeros((R_HEADS, HEAD, HEAD), jnp.float32)
    inputs = (ret_query.reshape(blocks, SPAN, R_HEADS, HEAD), ret_key.reshape(blocks, SPAN, R_HEADS, HEAD), ret_value.reshape(blocks, SPAN, R_HEADS, HEAD), retain_log.reshape(blocks, SPAN, R_HEADS))
    _, inside = lax.scan(retain_block, start_state, inputs)
    retained = head_norm(inside.reshape(shape)).astype(jnp.bfloat16).reshape(TOKENS, R_HEADS * HEAD)
    group = F_HEADS // KV_HEADS
    pieces = TOKENS // TOK_DEV
    att_query = (project(normed, w_query_att) * HEAD ** (-0.5)).astype(jnp.bfloat16).reshape(pieces, TOK_DEV, KV_HEADS, group, HEAD)
    att_key = project(normed, w_key_att).astype(jnp.bfloat16).reshape(pieces, TOK_DEV, KV_HEADS, HEAD)
    att_value = project(normed, w_value_att).astype(jnp.bfloat16).reshape(pieces, TOK_DEV, KV_HEADS, HEAD)
    gates = forget_total.reshape(KV_HEADS, group, pieces, TOK_DEV)
    local_places = jnp.arange(TOK_DEV, dtype=jnp.int32)

    def attend_block(index):
        query_rows = lax.dynamic_index_in_dim(att_query, index, 0, keepdims=False).astype(jnp.float32)
        gate_rows = lax.dynamic_index_in_dim(gates, index, 2, keepdims=False)
        query_places = index * TOK_DEV + local_places

        def add_keys(other, carry):
            weighted, total = carry
            key_rows = lax.dynamic_index_in_dim(att_key, other, 0, keepdims=False).astype(jnp.float32)
            value_rows = lax.dynamic_index_in_dim(att_value, other, 0, keepdims=False).astype(jnp.float32)
            gate_keys = lax.dynamic_index_in_dim(gates, other, 2, keepdims=False)
            scores = jnp.einsum('tcgd,scd->cgts', query_rows, key_rows)
            logits = scores + gate_rows[:, :, :, None] - gate_keys[:, :, None, :]
            allowed = (other * TOK_DEV + local_places)[None, :] <= query_places[:, None]
            weights = jnp.exp(jnp.where(allowed, logits, -jnp.inf))
            total = total + lax.optimization_barrier(jnp.sum(weights, axis=-1))
            weighted = weighted + jnp.einsum('cgts,scd->cgtd', weights.astype(jnp.bfloat16).astype(jnp.float32), value_rows)
            return (weighted, total)
        init = (jnp.zeros((KV_HEADS, group, TOK_DEV, HEAD), jnp.float32), jnp.zeros((KV_HEADS, group, TOK_DEV), jnp.float32))
        weighted, total = lax.fori_loop(0, index + 1, add_keys, init)
        return (weighted / total[..., None]).astype(jnp.bfloat16)
    outputs = lax.map(attend_block, jnp.arange(pieces, dtype=jnp.int32))
    attended = jnp.transpose(outputs, (0, 3, 1, 2, 4)).reshape(TOKENS, F_HEADS * HEAD)
    ret_width = R_HEADS // N_TP * HEAD
    att_width = F_HEADS // N_TP * HEAD
    summed = jnp.zeros((TOKENS, D), jnp.float32)
    for part in range(N_TP):
        term = jnp.dot(retained[:, part * ret_width:(part + 1) * ret_width], w_out_ret[part * ret_width:(part + 1) * ret_width], preferred_element_type=jnp.float32)
        term = term + jnp.dot(attended[:, part * att_width:(part + 1) * att_width], w_out_att[part * att_width:(part + 1) * att_width], preferred_element_type=jnp.float32)
        summed = summed + lax.optimization_barrier(term.astype(jnp.bfloat16)).astype(jnp.float32)
    return summed.astype(jnp.bfloat16)
```

```python
import functools

import jax
import jax.numpy as jnp
import numpy as np
from jax import lax
from jax.experimental import pallas as pl
from jax.experimental.pallas import tpu as pltpu
from jax.sharding import PartitionSpec as P

HEAD = 64
EPS = 1e-06
THETA = 10000.0
F32 = jnp.float32
BF16 = jnp.bfloat16
MESH = pl.DeviceIdType.MESH
SPAN = 256
KEY_SPAN = 256
LANES = 128
HIGH = lax.Precision.HIGHEST


def dot(a, b, dims=((1,), (0,))):
    return lax.dot_general(a, b, (dims, ((), ())), preferred_element_type=F32)


def kernel(
    n,
    m,
    heads,
    tok_hbm,
    gain_ref,
    wq_ret_hbm,
    wk_ret_hbm,
    wv_ret_hbm,
    wq_att_hbm,
    wk_att_hbm,
    wv_att_hbm,
    wo_ret_hbm,
    wo_att_hbm,
    table_hbm,
    logs_hbm,
    gate_hbm,
    out_ref,
    tokens,
    table,
    lbuf,
    gbuf,
    xbuf,
    abuf,
    bbuf,
    obuf,
    kvbuf,
    state,
    num,
    den,
    outbuf,
    rsbuf,
    load,
    small_send,
    small_recv,
    x_send,
    x_fwd,
    x_recv,
    w_send,
    w_part,
    w_y,
    w_recv,
    k_send,
    k_y,
    k_part,
    k_recv,
    r_send,
    r_recv,
):
    s, t = lax.axis_index("sp"), lax.axis_index("tp")
    nh, nx = n // 4, m // 2
    y, zl, zh = s % 2, (s // 2) % 2, s // 4
    c, x = t % 2, t // 2
    own = zl == c
    apart = zl != c

    def sp_of(zh_, zl_, y_):
        return zh_ * 4 + zl_ * 2 + y_

    def tp_of(x_, c_):
        return x_ * 2 + c_

    def device(zh_, zl_, y_, x_, c_):
        return {"sp": sp_of(zh_, zl_, y_), "tp": tp_of(x_, c_)}

    q, g = sp_of(zh, c, y), tp_of(x, zl)
    partner = device(zh, zl, y, x, 1 - c)
    across = device(zh, zl, 1 - y, x, c)
    rows = tokens.shape[0]
    tok = rows * m
    width = heads * HEAD
    half_o = wo_ret_hbm.shape[0]

    slot = jnp.where(own, s, n)
    piece = jnp.where(own, t, m)
    loads = [
        pltpu.make_async_copy(source, target, load.at[k])
        for k, (source, target) in enumerate((
            (tok_hbm, tokens),
            (wk_att_hbm, abuf.at[slot, pl.ds(0, HEAD)]),
            (wv_att_hbm, abuf.at[slot, pl.ds(HEAD, HEAD)]),
            (wk_ret_hbm, abuf.at[slot, pl.ds(2 * HEAD, width)]),
            (wv_ret_hbm, abuf.at[slot, pl.ds(2 * HEAD + width, width)]),
            (wq_att_hbm, bbuf.at[slot, pl.ds(0, width)]),
            (wq_ret_hbm, bbuf.at[slot, pl.ds(width, width)]),
            (wo_ret_hbm, obuf.at[slot, pl.ds(0, half_o)]),
            (wo_att_hbm, obuf.at[slot, pl.ds(half_o, wo_att_hbm.shape[0])]),
            (table_hbm.at[pl.ds(pl.multiple_of(q * tok, tok), tok)], table),
            (logs_hbm, lbuf.at[0]),
            (gate_hbm, gbuf.at[0]),
        ))
    ]
    for copy in loads:
        copy.start()

    barrier = pltpu.get_barrier_semaphore()
    greeted = [across]
    for i in reversed(range(nh)):
        for j in reversed(range(2)):
            for k in range(2):
                if i or j or k:
                    greeted.append(device((zh + i) % nh, (zl + j) % 2, y, x, (c + k) % 2))
    for r in range(1, nx):
        for j in range(2):
            for k in range(2):
                greeted.append(device(zh, (zl + j) % 2, y, (x + r) % nx, (c + k) % 2))
    for other in greeted:
        pl.semaphore_signal(barrier, inc=1, device_id=other, device_id_type=MESH)

    started = []

    def guarded(condition, action):
        if condition is None:
            action()
        else:
            pl.when(condition)(action)

    def send(source, target, send_sem, recv_sem, where, condition=None):
        copy = pltpu.make_async_remote_copy(
            src_ref=source, dst_ref=target, send_sem=send_sem, recv_sem=recv_sem,
            device_id=where, device_id_type=MESH,
        )
        guarded(condition, copy.start)
        started.append((copy, condition))

    def receive(target, recv_sem, condition=None):
        copy = pltpu.make_async_remote_copy(
            src_ref=target, dst_ref=target, send_sem=recv_sem, recv_sem=recv_sem,
            device_id=partner, device_id_type=MESH,
        )
        guarded(condition, copy.wait_recv)

    loads[0].wait()
    values = tokens[...].astype(F32)
    scale = lax.rsqrt(jnp.mean(values * values, axis=-1, keepdims=True) + EPS)
    xbuf[pl.ds(pl.multiple_of(piece * rows, rows), rows), :] = (
        values * scale * gain_ref[...]
    ).astype(BF16)
    for copy in loads[1:]:
        copy.wait()
    pl.semaphore_wait(barrier, len(greeted))

    parts = (abuf, bbuf, obuf)

    def half(buf, index, k):
        length = buf.shape[1] // 2
        return buf.at[index, pl.ds(pl.multiple_of(k * length, length), length)]

    def scatter(p, i):
        buf = parts[p]
        for k in (1, 0):
            core = (c + k) % 2
            send(
                half(buf, slot, core), half(buf, s, core),
                w_send.at[p, i, k], w_recv.at[p, s, core],
                device((zh + i) % nh, c, y, x, core),
                apart if i == 0 and k == 0 else None,
            )

    def entry(p, i, j):
        buf = parts[p]
        index = sp_of((zh + i) % nh, (zl + j) % 2, y)
        here = i == 0 and j == 0
        spot = half(buf, index, c)
        receive(spot, w_recv.at[p, index, c], apart if here else None)
        send(spot, spot, w_y.at[p, i, j], w_recv.at[p, index, c], across)
        send(
            spot, spot, w_part.at[p, i, j, 0], w_recv.at[p, index, c], partner,
            own if here else None,
        )

    def beside(p, i, j):
        buf = parts[p]
        index = sp_of((zh + i) % nh, (zl + j) % 2, 1 - y)
        spot = half(buf, index, c)
        receive(spot, w_recv.at[p, index, c])
        send(spot, spot, w_part.at[p, i, j, 1], w_recv.at[p, index, c], partner)

    def rest(p):
        buf = parts[p]
        for i in range(nh):
            for j in range(2):
                for k in range(2):
                    index = sp_of((zh + i) % nh, (zl + j) % 2, (y + k) % 2)
                    receive(
                        half(buf, index, 1 - c), w_recv.at[p, index, 1 - c],
                        apart if i == 0 and j == 0 and k == 0 else None,
                    )

    order = [(i, j) for i in range(nh) for j in range(2)]

    def rows_of(index):
        return xbuf.at[pl.ds(pl.multiple_of(index * rows, rows), rows)]

    scatter(0, 0)
    entry_first = order[0]
    send(rows_of(piece), rows_of(t), x_send.at[0], x_recv.at[t], device(zh, 1 - zl, y, x, zl))
    for r in range(1, nx):
        send(
            rows_of(piece), rows_of(t), x_send.at[1 + r], x_recv.at[t],
            device(zh, zl, y, (x + r) % nx, zl),
        )
    send(rows_of(piece), rows_of(t), x_send.at[1], x_recv.at[t], device(zh, zl, y, x, zl), apart)
    send(
        lbuf.at[0], lbuf.at[1], small_send.at[0], small_recv.at[0],
        device(zh, c, y, x, zl), apart,
    )
    send(gbuf.at[0], gbuf.at[1], small_send.at[1], small_recv.at[1], partner, own)
    for i in range(1, nh):
        scatter(0, i)
    entry(0, *entry_first)
    for i in range(nh):
        scatter(1, i)

    def pass_tokens(k):
        index = tp_of(x, (c + k) % 2)
        spot = rows_of(index)
        receive(spot, x_recv.at[index], apart if k == 0 else None)
        for r in range(1, nx):
            send(
                spot, spot, x_fwd.at[r - 1, k], x_recv.at[index],
                device(zh, zl, y, (x + r) % nx, c), apart,
            )

    entry(0, *order[1])
    beside(0, *order[0])
    for k in range(2):
        pass_tokens(k)
    for a in range(2, len(order)):
        entry(0, *order[a])
        beside(0, *order[a - 1])
    beside(0, *order[-1])

    lines = lax.broadcasted_iota(jnp.int32, (tok, tok), 0)
    lanes = lax.broadcasted_iota(jnp.int32, (tok, tok), 1)
    causal = lines >= lanes
    upto = jnp.where(lines <= lanes, 1.0, 0.0)
    receive(lbuf.at[1], small_recv.at[0], apart)
    receive(gbuf.at[1], small_recv.at[1], apart)
    pick = jnp.where(own, 0, 1)
    logs = jnp.concatenate([lbuf[pick], jnp.zeros((8 - heads, tok), F32)], axis=0)
    turned = lax.dot_general(
        logs, upto, (((1,), (0,)), ((), ())),
        preferred_element_type=F32, precision=lax.Precision.HIGHEST,
    )
    fill = jnp.zeros((LANES - 8, tok), F32)
    within = jnp.concatenate([turned, fill], axis=0).T
    gates_own = gbuf[pick, :, pl.ds(pl.multiple_of(q * tok, tok), tok)]
    gate_col = jnp.concatenate(
        [gates_own, jnp.zeros((LANES - heads, tok), F32)], axis=0
    ).T
    cosine, sine = table[:, : HEAD // 2], table[:, HEAD // 2 :]

    for r in range(1, nx):
        for k in range(2):
            index = tp_of((x + r) % nx, k)
            receive(rows_of(index), x_recv.at[index])
    rest(0)

    def rope(field):
        first, second = field[:, : HEAD // 2], field[:, HEAD // 2 :]
        return jnp.concatenate(
            [first * cosine - second * sine, first * sine + second * cosine], axis=-1
        )

    def project(buf):
        deep = buf.shape[2]
        return sum(
            dot(xbuf[:tok, k * deep : (k + 1) * deep], buf[k], ((1,), (1,))) for k in range(n)
        )

    proj = project(abuf)
    pair = proj[:, : 2 * HEAD].astype(BF16)
    keys, vals, updates, marks = [], [], [], []
    for h in range(heads):
        base = 2 * HEAD + h * HEAD
        key = rope(proj[:, base : base + HEAD]).astype(BF16)
        val = proj[:, base + width : base + width + HEAD].astype(BF16)
        column = within[:, h : h + 1]
        last = column[tok - 1 :, :]
        faded = (key.astype(F32) * jnp.exp(last - column)).astype(BF16)
        updates.append(dot(faded, val, ((0,), (0,))))
        high = last.astype(BF16).astype(F32)
        low = last - high
        marks.append(jnp.broadcast_to(high, (8, HEAD)))
        marks.append(jnp.broadcast_to(low, (8, HEAD)))
        keys.append(key)
        vals.append(val)
    kvbuf[q, :tok, :] = pair
    marks.append(jnp.zeros((HEAD - 16 * heads, HEAD), F32))
    blocks = updates + [jnp.concatenate(marks, axis=0)]
    if len(blocks) % 2:
        blocks.append(jnp.zeros((HEAD, HEAD), F32))
    for k in range(0, len(blocks), 2):
        both = jnp.concatenate(blocks[k : k + 2], axis=1).astype(BF16)
        kvbuf[q, tok + k // 2 * HEAD : tok + (k // 2 + 1) * HEAD, :] = both

    def piece_of(index, k):
        spot = slice(k % 2 * HEAD, (k % 2 + 1) * HEAD)
        return kvbuf[index, tok + k // 2 * HEAD : tok + (k // 2 + 1) * HEAD, spot].astype(F32)

    def share(index, sem, where, condition=None):
        send(kvbuf.at[index], kvbuf.at[index], sem, k_recv.at[index], where, condition)

    def arrive(index, condition=None):
        receive(kvbuf.at[index], k_recv.at[index], condition)

    for i in range(1, nh):
        share(q, k_send.at[i - 1], device((zh + i) % nh, zl, y, x, c), zh + i < nh)
    share(q, k_y.at[0], across, c + y < 2)
    share(q, k_part.at[0, 0], partner, c == 0)
    for i in range(nh):
        scatter(2, i)

    for a in range(len(order)):
        entry(1, *order[a])
        if a:
            beside(1, *order[a - 1])
        if a == 0:
            index = sp_of(zh, c, 1 - y)
            arrive(index, c <= y)
            share(index, k_part.at[0, 1], partner, c == 0)
    for i in range(1, nh):
        index = sp_of((zh + nh - i) % nh, c, y)
        arrive(index, zh >= i)
        share(index, k_y.at[i], across, zh >= i)
        share(index, k_part.at[i, 0], partner, zh >= i)
    beside(1, *order[-1])
    entry(2, *order[0])
    for i in range(1, nh):
        index = sp_of((zh + nh - i) % nh, c, 1 - y)
        arrive(index, zh >= i)
        share(index, k_part.at[i, 1], partner, zh >= i)
    rest(1)

    projq = project(bbuf)
    entry(2, *order[1])
    beside(2, *order[0])
    local, lifts = [], []
    for h in range(heads):
        base = width + h * HEAD
        query = (rope(projq[:, base : base + HEAD]) * HEAD ** (-0.5)).astype(BF16)
        column = within[:, h : h + 1]
        gap = jnp.where(causal, column - turned[h : h + 1, :], 0.0)
        scores = dot(query, keys[h], ((1,), (1,)))
        weights = jnp.where(causal, scores * jnp.exp(gap), 0.0).astype(BF16)
        local.append(dot(weights, vals[h]))
        lifts.append((query.astype(F32) * jnp.exp(column)).astype(BF16))

    queries = [
        (projq[:, h * HEAD : (h + 1) * HEAD] * HEAD ** (-0.5)).astype(BF16) for h in range(heads)
    ]

    def attend(index, masked):
        block = kvbuf[index, :tok, :]
        key, val = block[:, :HEAD], block[:, HEAD:]
        gates = gbuf[pick, :, pl.ds(pl.multiple_of(index * tok, tok), tok)]
        for h in range(heads):
            logits = dot(queries[h], key, ((1,), (1,)))
            logits = logits + gate_col[:, h : h + 1] - gates[h : h + 1, :]
            if masked:
                logits = jnp.where(causal, logits, -jnp.inf)
            weights = jnp.exp(logits)
            den[h] += jnp.broadcast_to(jnp.sum(weights, axis=-1, keepdims=True), (tok, HEAD))
            num[h] += dot(weights.astype(BF16), val)

    den[...] = jnp.zeros_like(den)
    num[...] = jnp.zeros_like(num)
    state[...] = jnp.zeros_like(state)
    attend(q, True)
    entry(2, *order[2])
    beside(2, *order[1])
    for k in range(2):
        arrive(sp_of(zh, 1 - c, (y + k) % 2), c == 1)
    for i in range(1, nh):
        for k in range(2):
            arrive(sp_of((zh + nh - i) % nh, 1 - c, (y + k) % 2), zh >= i)
    pending = [(entry, a) for a in order[3:]]
    after = [(beside, a) for a in order[2:]]
    steps = []
    for a in range(len(after)):
        if a < len(pending):
            steps.append(pending[a])
        steps.append(after[a])
    for j in range(n - 1):
        def earlier(j=j):
            marked = piece_of(j, heads)
            for h in range(heads):
                total = marked[16 * h : 16 * h + 1] + marked[16 * h + 8 : 16 * h + 9]
                state[h] = jnp.exp(total) * state[h] + piece_of(j, h)
            attend(j, False)

        pl.when(q > j)(earlier)
        if j % 2 == 0 and steps:
            call, a = steps.pop(0)
            call(2, *a)
    for call, a in steps:
        call(2, *a)
    rest(2)

    retained, attended = [], []
    for h in range(heads):
        raw = local[h] + dot(lifts[h], state[h].astype(BF16))
        centre = jnp.mean(raw, axis=-1, keepdims=True)
        spread = jnp.mean(jnp.square(raw - centre), axis=-1, keepdims=True)
        retained.append(((raw - centre) * lax.rsqrt(spread + EPS)).astype(BF16))
        attended.append((num[h] / den[h]).astype(BF16))
    mixed = jnp.concatenate(retained + attended, axis=-1)

    columns = obuf.shape[2]
    group = 2
    for part in range(n // group):
        for k in range(part * group, part * group + group):
            term = dot(mixed, obuf[k]).astype(BF16)
            outbuf[:, :, k * columns : (k + 1) * columns] = term.reshape(m, rows, columns)
        span = pl.ds(part * group * columns, group * columns)
        for r in reversed(range(nx)):
            for k in range(2):
                index = tp_of((x + r) % nx, (c + k) % 2)
                send(
                    outbuf.at[index, :, span], rsbuf.at[g, :, span],
                    r_send.at[part, r, k], r_recv.at[part, g],
                    device(zh, c, y, (x + r) % nx, (c + k) % 2),
                    apart if r == 0 and k == 0 else None,
                )
    for part in range(n // group):
        span = pl.ds(part * group * columns, group * columns)

        def keep():
            rsbuf[g, :, span] = outbuf[t, :, span]

        pl.when(own)(keep)
        total = None
        for r in range(nx):
            for j in range(2):
                index = tp_of((x + r) % nx, (zl + j) % 2)
                receive(
                    rsbuf.at[index, :, span], r_recv.at[part, index],
                    apart if r == 0 and j == 0 else None,
                )
                term = rsbuf[index, :, span].astype(F32)
                total = term if total is None else total + term
        out_ref[:, span] = total.astype(BF16)

    for copy, condition in started:
        guarded(condition, copy.wait_send)


def body(
    n,
    m,
    tokens,
    pre_gain,
    w_query_ret,
    w_key_ret,
    w_value_ret,
    w_query_att,
    w_key_att,
    w_value_att,
    w_out_ret,
    w_out_att,
    retain_log,
    forget_total,
):
    rows, depth = tokens.shape
    tok = rows * m
    heads = retain_log.shape[1]
    nh, nx = n // 4, m // 2
    half = HEAD // 2
    inverse = np.float32(THETA) ** (-np.arange(half, dtype=np.float32) / np.float32(half))
    angles = np.arange(n * tok, dtype=np.float32)[:, None] * inverse[None, :]
    table = np.concatenate([np.cos(angles), np.sin(angles)], axis=1).astype(np.float32)
    wide_a = 2 * HEAD + 2 * heads * HEAD
    wide_b = 2 * heads * HEAD
    deep = w_key_ret.shape[0]
    deep_o = w_out_ret.shape[0] + w_out_att.shape[0]
    tall = tok + (heads // 2 + 1) * HEAD
    hbm = pl.BlockSpec(memory_space=pl.ANY)
    vmem = pl.BlockSpec(memory_space=pltpu.VMEM)
    dma = pltpu.SemaphoreType.DMA
    return pl.pallas_call(
        functools.partial(kernel, n, m, heads),
        out_shape=jax.ShapeDtypeStruct((rows, depth), BF16),
        in_specs=[hbm, vmem] + [hbm] * 11,
        out_specs=vmem,
        scratch_shapes=[
            pltpu.VMEM(tokens.shape, BF16),
            pltpu.VMEM((tok, HEAD), F32),
            pltpu.VMEM((2,) + retain_log.shape[::-1], F32),
            pltpu.VMEM((2,) + forget_total.shape, F32),
            pltpu.VMEM((tok + rows, depth), BF16),
            pltpu.VMEM((n + 1, wide_a, deep), BF16),
            pltpu.VMEM((n + 1, wide_b, deep), BF16),
            pltpu.VMEM((n + 1, deep_o, w_out_ret.shape[1]), BF16),
            pltpu.VMEM((n, tall, 2 * HEAD), BF16),
            pltpu.VMEM((heads, HEAD, HEAD), F32),
            pltpu.VMEM((heads, tok, HEAD), F32),
            pltpu.VMEM((heads, tok, HEAD), F32),
            pltpu.VMEM((m, rows, depth), BF16),
            pltpu.VMEM((m, rows, depth), BF16),
            dma((12,)),
            dma((2,)),
            dma((2,)),
            dma((1 + nx,)),
            dma((nx - 1, 2)),
            dma((m,)),
            dma((3, nh, 2)),
            dma((3, nh, 2, 2)),
            dma((3, nh, 2)),
            dma((3, n, 2)),
            dma((nh - 1,)),
            dma((nh,)),
            dma((nh, 2)),
            dma((n,)),
            dma((n // 2, nx, 2)),
            dma((n // 2, m)),
        ],
        compiler_params=pltpu.CompilerParams(
            collective_id=0, has_side_effects=True, vmem_limit_bytes=60 * 1024 * 1024
        ),
    )(
        tokens,
        pre_gain[None, :],
        w_query_ret.T,
        w_key_ret.T,
        w_value_ret.T,
        w_query_att.T,
        w_key_att.T,
        w_value_att.T,
        w_out_ret,
        w_out_att,
        jnp.asarray(table),
        retain_log.T,
        forget_total,
    )


def rotate(field, positions):
    half = field.shape[-1] // 2
    inverse = THETA ** (-jnp.arange(half, dtype=jnp.float32) / half)
    angles = positions[:, None] * inverse[None, :]
    cosine = jnp.cos(angles)[:, None, :]
    sine = jnp.sin(angles)[:, None, :]
    first_half = field[..., :half]
    second_half = field[..., half:]
    return jnp.concatenate(
        [first_half * cosine - second_half * sine, first_half * sine + second_half * cosine],
        axis=-1,
    )


def head_norm(values):
    centre = jnp.mean(values, axis=-1, keepdims=True)
    spread = jnp.mean(jnp.square(values - centre), axis=-1, keepdims=True)
    return (values - centre) * lax.rsqrt(spread + EPS)


def advance(state, pair):
    decay, update = pair
    return (jnp.exp(decay)[:, None, None] * state + update, state)


def plain_body(
    tokens,
    pre_gain,
    w_query_ret,
    w_key_ret,
    w_value_ret,
    w_query_att,
    w_key_att,
    w_value_att,
    w_out_ret,
    w_out_att,
    retain_log,
    forget_total,
):
    rows = tokens.astype(jnp.float32)
    normed = (
        rows * lax.rsqrt(jnp.mean(rows * rows, axis=-1, keepdims=True) + EPS) * pre_gain
    ).astype(jnp.bfloat16)
    gathered = lax.all_gather(normed, "tp", axis=0, tiled=True)
    tok_dev = gathered.shape[0]
    offset = lax.axis_index("sp") * tok_dev
    query_places = offset + jnp.arange(tok_dev, dtype=jnp.int32)
    positions = query_places.astype(jnp.float32)

    def blocked(values):
        return values.reshape((tok_dev // SPAN, SPAN) + values.shape[1:])

    pieces = (
        lax.all_gather(w_query_ret, "sp", axis=0, tiled=True),
        lax.all_gather(w_key_ret, "sp", axis=0, tiled=True),
        lax.all_gather(w_value_ret, "sp", axis=0, tiled=True),
        lax.all_gather(w_query_att, "sp", axis=0, tiled=True),
        lax.all_gather(w_key_att, "sp", axis=0, tiled=True),
        lax.all_gather(w_value_att, "sp", axis=0, tiled=True),
    )
    projected = tuple(
        (jnp.dot(gathered, piece, preferred_element_type=jnp.float32) for piece in pieces)
    )
    heads = retain_log.shape[1]
    shape = (tok_dev, heads, HEAD)
    query = blocked(
        (rotate(projected[0].reshape(shape), positions) * HEAD ** (-0.5)).astype(jnp.bfloat16)
    )
    key_rows = blocked(rotate(projected[1].reshape(shape), positions).astype(jnp.bfloat16))
    value_rows = blocked(projected[2].astype(jnp.bfloat16).reshape(shape))
    within = jnp.cumsum(blocked(retain_log), axis=1)
    causal = jnp.arange(SPAN)[:, None] >= jnp.arange(SPAN)[None, :]
    scores = jnp.einsum("bthd,bshd->bhts", query, key_rows, preferred_element_type=jnp.float32)
    turned = jnp.transpose(within, (0, 2, 1))
    gap = jnp.where(causal, turned[:, :, :, None] - turned[:, :, None, :], 0.0)
    weights = jnp.where(causal, scores * jnp.exp(gap), 0.0).astype(jnp.bfloat16)
    local = jnp.einsum("bhts,bshd->bthd", weights, value_rows, preferred_element_type=jnp.float32)
    last = within[:, -1]
    faded = (key_rows.astype(jnp.float32) * jnp.exp(last[:, None, :] - within)[..., None]).astype(
        jnp.bfloat16
    )
    updates = jnp.einsum("bshd,bshe->bhde", faded, value_rows, preferred_element_type=jnp.float32)
    zero_state = jnp.zeros((heads, HEAD, HEAD), jnp.float32)
    final, _ = lax.scan(advance, zero_state, (last, updates))
    decay_total = jnp.sum(last, axis=0)
    own_state = final.reshape(heads, HEAD * HEAD)
    every_total = lax.all_gather(
        decay_total[None].astype(jnp.bfloat16), "sp", axis=0, tiled=True
    ).astype(jnp.float32)
    every_state = lax.all_gather(
        own_state[None].astype(jnp.bfloat16), "sp", axis=0, tiled=True
    ).astype(jnp.float32)
    device_order = jnp.arange(every_total.shape[0], dtype=jnp.int32)[:, None]
    earlier = device_order < lax.axis_index("sp")
    before = jnp.sum(jnp.where(earlier, every_total, 0.0), axis=0)
    through = jnp.cumsum(every_total, axis=0)
    fading = jnp.where(earlier, jnp.exp(jnp.where(earlier, before[None, :] - through, 0.0)), 0.0)
    incoming = jnp.einsum("jh,jhe->he", fading, every_state, precision=HIGH)
    _, befores = lax.scan(advance, incoming.reshape(heads, HEAD, HEAD), (last, updates))
    lifted = (query.astype(jnp.float32) * jnp.exp(within)[..., None]).astype(jnp.bfloat16)
    carried = jnp.einsum(
        "bthd,bhde->bthe", lifted, befores.astype(jnp.bfloat16), preferred_element_type=jnp.float32
    )
    retained = (
        head_norm((local + carried).reshape(shape))
        .astype(jnp.bfloat16)
        .reshape(tok_dev, heads * HEAD)
    )
    raw_key = projected[4]
    gate_heads = forget_total.shape[0]
    kv_local = raw_key.shape[1] // HEAD
    group = gate_heads // kv_local
    query = (
        (projected[3] * HEAD ** (-0.5)).astype(jnp.bfloat16).reshape(tok_dev, kv_local, group, HEAD)
    )
    key_rows = raw_key.astype(jnp.bfloat16)
    value_rows = projected[5].astype(jnp.bfloat16)
    gate_rows = lax.dynamic_slice_in_dim(forget_total, offset, tok_dev, 1).reshape(
        kv_local, group, tok_dev
    )
    last_row = offset + tok_dev - 1
    init = (
        jnp.zeros((kv_local, group, tok_dev, HEAD), jnp.float32),
        jnp.zeros((kv_local, group, tok_dev), jnp.float32),
    )
    key_piece = lax.all_gather(key_rows, "sp", axis=0, tiled=True)
    value_piece = lax.all_gather(value_rows, "sp", axis=0, tiled=True)
    count = key_piece.shape[0] // KEY_SPAN

    def one_block(index, inner):
        first = index * KEY_SPAN

        def compute(state):
            weighted, total = state
            key_block = lax.dynamic_slice_in_dim(key_piece, index * KEY_SPAN, KEY_SPAN, 0).reshape(
                KEY_SPAN, kv_local, HEAD
            )
            value_block = lax.dynamic_slice_in_dim(
                value_piece, index * KEY_SPAN, KEY_SPAN, 0
            ).reshape(KEY_SPAN, kv_local, HEAD)
            gate_keys = lax.dynamic_slice_in_dim(forget_total, first, KEY_SPAN, 1).reshape(
                kv_local, group, KEY_SPAN
            )
            scores = jnp.einsum(
                "tcgd,scd->cgts", query, key_block, preferred_element_type=jnp.float32
            )
            logits = scores + gate_rows[:, :, :, None] - gate_keys[:, :, None, :]
            allowed = (first + jnp.arange(KEY_SPAN, dtype=jnp.int32))[None, :] <= query_places[
                :, None
            ]
            weights = jnp.exp(jnp.where(allowed, logits, -jnp.inf))
            total = total + jnp.sum(weights, axis=-1)
            weighted = weighted + jnp.einsum(
                "cgts,scd->cgtd",
                weights.astype(jnp.bfloat16),
                value_block,
                preferred_element_type=jnp.float32,
            )
            return (weighted, total)

        def skipped(state):
            return state

        return lax.cond(first <= last_row, compute, skipped, inner)

    weighted, total = lax.fori_loop(0, count, one_block, init)
    result = weighted / total[..., None]
    attended = (
        jnp.transpose(result, (2, 0, 1, 3)).reshape(tok_dev, gate_heads * HEAD).astype(jnp.bfloat16)
    )
    out_ret, out_att = (
        lax.all_gather(w_out_ret, "sp", axis=1, tiled=True),
        lax.all_gather(w_out_att, "sp", axis=1, tiled=True),
    )
    return lax.psum_scatter(
        (
            jnp.dot(retained, out_ret, preferred_element_type=jnp.float32)
            + jnp.dot(attended, out_att, preferred_element_type=jnp.float32)
        ).astype(jnp.bfloat16),
        "tp",
        scatter_dimension=0,
        tiled=True,
    )


def choose(n, m, *arrays):
    tokens, w_key_ret, w_out_ret = arrays[0], arrays[3], arrays[8]
    whole_tiles = w_out_ret.shape[1] % LANES == 0 and w_key_ret.shape[0] % LANES == 0
    heads = arrays[10].shape[1]
    small = 16 * heads <= HEAD and arrays[7].shape[1] == HEAD and arrays[11].shape[0] == heads
    paired = n % 4 == 0 and n > 4 and m % 2 == 0 and m > 2
    if paired and whole_tiles and small and tokens.shape[0] * m == SPAN:
        return body(n, m, *arrays)
    return plain_body(*arrays)


def solution(mesh):
    return jax.shard_map(
        functools.partial(choose, mesh.shape["sp"], mesh.shape["tp"]),
        mesh=mesh,
        in_specs=(
            P(("sp", "tp"), None),
            P(),
            P("sp", "tp"),
            P("sp", "tp"),
            P("sp", "tp"),
            P("sp", "tp"),
            P("sp", "tp"),
            P("sp", "tp"),
            P("tp", "sp"),
            P("tp", "sp"),
            P("sp", "tp"),
            P("tp", None),
        ),
        out_specs=P(("sp", "tp"), None),
        check_vma=False,
    )
```

```python
import functools

import jax
import jax.numpy as jnp
import numpy as np
from jax import lax
from jax.experimental import pallas as pl
from jax.experimental.pallas import tpu as pltpu
from jax.sharding import PartitionSpec as P

HEAD = 64
EPS = 1e-06
THETA = 10000.0
F32 = jnp.float32
BF16 = jnp.bfloat16
MESH = pl.DeviceIdType.MESH
SPAN = 256
KEY_SPAN = 256
LANES = 128
CUT = 2
TOKEN_CUT = 2
HIGH = lax.Precision.HIGHEST


def dot(a, b, dims=((1,), (0,))):
    return lax.dot_general(a, b, (dims, ((), ())), preferred_element_type=F32)


def kernel(
    n,
    m,
    heads,
    tok_hbm,
    gain_ref,
    wq_ret_hbm,
    wk_ret_hbm,
    wv_ret_hbm,
    wq_att_hbm,
    wk_att_hbm,
    wv_att_hbm,
    wo_ret_hbm,
    wo_att_hbm,
    table_hbm,
    logs_hbm,
    gate_hbm,
    out_ref,
    tokens,
    table,
    lbuf,
    gbuf,
    xbuf,
    abuf,
    bbuf,
    obuf,
    kvbuf,
    stbuf,
    state,
    num,
    den,
    outbuf,
    rsbuf,
    load,
    small_send,
    small_recv,
    x_send,
    x_fwd,
    x_recv,
    w_send,
    w_near,
    w_part,
    w_y,
    w_recv,
    k_send,
    k_y,
    k_part,
    k_recv,
    st_send,
    st_recv,
    r_send,
    r_recv,
):
    s, t = lax.axis_index("sp"), lax.axis_index("tp")
    nh, nx = n // 4, m // 2
    y, zl, zh = s % 2, (s // 2) % 2, s // 4
    c, x = t % 2, t // 2
    own = zl == c
    apart = zl != c

    def sp_of(zh_, zl_, y_):
        return zh_ * 4 + zl_ * 2 + y_

    def tp_of(x_, c_):
        return x_ * 2 + c_

    def device(zh_, zl_, y_, x_, c_):
        return {"sp": sp_of(zh_, zl_, y_), "tp": tp_of(x_, c_)}

    q, g = sp_of(zh, c, y), tp_of(x, zl)
    partner = device(zh, zl, y, x, 1 - c)
    across = device(zh, zl, 1 - y, x, c)
    rows = tokens.shape[0]
    tok = rows * m
    width = heads * HEAD
    half_o = wo_ret_hbm.shape[0]

    slot = jnp.where(own, s, n)
    piece = jnp.where(own, t, m)
    loads = [
        pltpu.make_async_copy(source, target, load.at[k])
        for k, (source, target) in enumerate((
            (tok_hbm, tokens),
            (wk_att_hbm, abuf.at[slot, pl.ds(0, HEAD)]),
            (wv_att_hbm, abuf.at[slot, pl.ds(HEAD, HEAD)]),
            (wq_att_hbm, abuf.at[slot, pl.ds(2 * HEAD, width)]),
            (wk_ret_hbm, bbuf.at[slot, pl.ds(0, width)]),
            (wv_ret_hbm, bbuf.at[slot, pl.ds(width, width)]),
            (wq_ret_hbm, bbuf.at[slot, pl.ds(2 * width, width)]),
            (wo_ret_hbm, obuf.at[slot, pl.ds(0, half_o)]),
            (wo_att_hbm, obuf.at[slot, pl.ds(half_o, wo_att_hbm.shape[0])]),
            (table_hbm.at[pl.ds(pl.multiple_of(q * tok, tok), tok)], table),
            (logs_hbm, lbuf.at[0]),
            (gate_hbm, gbuf.at[0]),
        ))
    ]
    for copy in loads:
        copy.start()

    barrier = pltpu.get_barrier_semaphore()
    greeted = [
        device((zh + i) % nh, zl, 1 - y, x, (c + k) % 2) for i in range(nh) for k in range(2)
    ]
    for i in reversed(range(nh)):
        for j in reversed(range(2)):
            for k in range(2):
                if i or j or k:
                    greeted.append(device((zh + i) % nh, (zl + j) % 2, y, x, (c + k) % 2))
    for r in range(1, nx):
        for j in range(2):
            for k in range(2):
                greeted.append(device(zh, (zl + j) % 2, y, (x + r) % nx, (c + k) % 2))
    for other in greeted:
        pl.semaphore_signal(barrier, inc=1, device_id=other, device_id_type=MESH)

    started = []

    def guarded(condition, action):
        if condition is None:
            action()
        else:
            pl.when(condition)(action)

    def send(source, target, send_sem, recv_sem, where, condition=None):
        copy = pltpu.make_async_remote_copy(
            src_ref=source, dst_ref=target, send_sem=send_sem, recv_sem=recv_sem,
            device_id=where, device_id_type=MESH,
        )
        guarded(condition, copy.start)
        started.append((copy, condition))

    def receive(target, recv_sem, condition=None):
        copy = pltpu.make_async_remote_copy(
            src_ref=target, dst_ref=target, send_sem=recv_sem, recv_sem=recv_sem,
            device_id=partner, device_id_type=MESH,
        )
        guarded(condition, copy.wait_recv)

    loads[0].wait()
    values = tokens[...].astype(F32)
    scale = lax.rsqrt(jnp.mean(values * values, axis=-1, keepdims=True) + EPS)
    xbuf[pl.ds(pl.multiple_of(piece * rows, rows), rows), :] = (
        values * scale * gain_ref[...]
    ).astype(BF16)
    for copy in loads[1:]:
        copy.wait()
    pl.semaphore_wait(barrier, len(greeted))

    parts = (abuf, bbuf, obuf)
    cut = w_recv.shape[3]

    def chunk(buf, index, k, u):
        length = buf.shape[1] // (2 * cut)
        return buf.at[index, pl.ds(pl.multiple_of((k * cut + u) * length, length), length)]

    def scatter_one(p, i, k, u, condition):
        buf = parts[p]
        core = (c + k) % 2
        send(
            chunk(buf, slot, core, u), chunk(buf, s, core, u),
            w_send.at[p, i, k, u], w_recv.at[p, s, core, u],
            device((zh + i) % nh, c, y, x, core), condition,
        )

    def scatter_chip(p):
        for u in range(cut):
            scatter_one(p, 0, 1, u, own)

    def scatter_near(p, u):
        buf = parts[p]
        for k in range(2):
            core = (c + k) % 2
            send(
                chunk(buf, slot, core, u), chunk(buf, s, core, u),
                w_near.at[p, k, u], w_recv.at[p, s, core, u],
                device(zh, c, y, x, core), apart,
            )

    def scatter_far(p, u):
        for i in range(1, nh):
            for k in range(2):
                scatter_one(p, i, k, u, None)

    def entry(p, i, j, u):
        buf = parts[p]
        index = sp_of((zh + i) % nh, (zl + j) % 2, y)
        here = i == 0 and j == 0
        spot = chunk(buf, index, c, u)
        receive(spot, w_recv.at[p, index, c, u], apart if here else None)
        send(spot, spot, w_y.at[p, i, j, u], w_recv.at[p, index, c, u], across)
        send(
            spot, spot, w_part.at[p, i, j, 0, u], w_recv.at[p, index, c, u], partner,
            own if here else None,
        )

    def beside(p, i, j, u):
        buf = parts[p]
        index = sp_of((zh + i) % nh, (zl + j) % 2, 1 - y)
        spot = chunk(buf, index, c, u)
        receive(spot, w_recv.at[p, index, c, u])
        send(spot, spot, w_part.at[p, i, j, 1, u], w_recv.at[p, index, c, u], partner)

    def rest(p):
        buf = parts[p]
        for i in range(nh):
            for j in range(2):
                for k in range(2):
                    for u in range(cut):
                        index = sp_of((zh + i) % nh, (zl + j) % 2, (y + k) % 2)
                        receive(
                            chunk(buf, index, 1 - c, u), w_recv.at[p, index, 1 - c, u],
                            apart if i == 0 and j == 0 and k == 0 else None,
                        )

    far = [(i, j) for i in range(1, nh) for j in range(2)]
    near = (0, 1)
    pieces = x_recv.shape[1]

    def rows_of(index, u):
        length = rows // pieces
        return xbuf.at[pl.ds(pl.multiple_of((index * pieces + u) * length, length), length)]

    def pass_tokens(k, u):
        index = tp_of(x, (c + k) % 2)
        spot = rows_of(index, u)
        receive(spot, x_recv.at[index, u], apart if k == 0 else None)
        for r in range(1, nx):
            send(
                spot, spot, x_fwd.at[r - 1, k, u], x_recv.at[index, u],
                device(zh, zl, y, (x + r) % nx, c), apart,
            )

    for u in range(cut):
        scatter_far(0, u)
    scatter_chip(0)
    for u in range(pieces):
        send(
            rows_of(piece, u), rows_of(t, u), x_send.at[0, u], x_recv.at[t, u],
            device(zh, 1 - zl, y, x, zl),
        )
        for r in range(1, nx):
            send(
                rows_of(piece, u), rows_of(t, u), x_send.at[1 + r, u], x_recv.at[t, u],
                device(zh, zl, y, (x + r) % nx, zl),
            )
        send(
            rows_of(piece, u), rows_of(t, u), x_send.at[1, u], x_recv.at[t, u],
            device(zh, zl, y, x, zl), apart,
        )
    for u in range(cut):
        scatter_near(0, u)
    scatter_chip(1)
    scatter_chip(2)
    for u in range(cut):
        scatter_far(1, u)
        scatter_near(1, u)
    send(
        lbuf.at[0], lbuf.at[1], small_send.at[0], small_recv.at[0],
        device(zh, c, y, x, zl), apart,
    )
    send(gbuf.at[0], gbuf.at[1], small_send.at[1], small_recv.at[1], partner, own)
    for p in range(3):
        for u in range(cut):
            entry(p, 0, 0, u)
    for u in range(cut):
        beside(0, 0, 0, u)
    for a in far:
        entry(0, *a, 0)
    for k in range(2):
        pass_tokens(k, 0)
    for u in range(cut):
        beside(1, 0, 0, u)
    for u in range(1, cut):
        for a in far:
            entry(0, *a, u)
    for a in far:
        beside(0, *a, 0)
    for u in range(1, pieces):
        for k in range(2):
            pass_tokens(k, u)
    for u in range(cut):
        entry(0, *near, u)
    for u in range(1, cut):
        for a in far:
            beside(0, *a, u)
    for a in far:
        entry(1, *a, 0)
    for u in range(cut):
        beside(0, *near, u)

    lines = lax.broadcasted_iota(jnp.int32, (tok, tok), 0)
    lanes = lax.broadcasted_iota(jnp.int32, (tok, tok), 1)
    causal = lines >= lanes
    upto = jnp.where(lines <= lanes, 1.0, 0.0)
    receive(lbuf.at[1], small_recv.at[0], apart)
    receive(gbuf.at[1], small_recv.at[1], apart)
    pick = jnp.where(own, 0, 1)
    logs = jnp.concatenate([lbuf[pick], jnp.zeros((8 - heads, tok), F32)], axis=0)
    turned = lax.dot_general(
        logs, upto, (((1,), (0,)), ((), ())),
        preferred_element_type=F32, precision=lax.Precision.HIGHEST,
    )
    fill = jnp.zeros((LANES - 8, tok), F32)
    within = jnp.concatenate([turned, fill], axis=0).T
    gates_own = gbuf[pick, :, pl.ds(pl.multiple_of(q * tok, tok), tok)]
    gate_col = jnp.concatenate(
        [gates_own, jnp.zeros((LANES - heads, tok), F32)], axis=0
    ).T
    cosine, sine = table[:, : HEAD // 2], table[:, HEAD // 2 :]

    for r in range(1, nx):
        for k in range(2):
            index = tp_of((x + r) % nx, k)
            for u in range(pieces):
                receive(rows_of(index, u), x_recv.at[index, u])
    rest(0)

    def exchange(buf, e, index, sem, where, condition):
        send(buf.at[index], buf.at[index], sem, k_recv.at[e, index], where, condition)

    def arrive(buf, e, index, condition):
        receive(buf.at[index], k_recv.at[e, index], condition)

    def exchange_send(buf, e):
        for i in range(1, nh):
            exchange(
                buf, e, q, k_send.at[e, i - 1], device((zh + i) % nh, zl, y, x, c), zh + i < nh
            )
        exchange(buf, e, q, k_y.at[e, 0], across, c + y < 2)
        exchange(buf, e, q, k_part.at[e, 0, 0], partner, c == 0)

    def exchange_across(buf, e):
        index = sp_of(zh, c, 1 - y)
        arrive(buf, e, index, c <= y)
        exchange(buf, e, index, k_part.at[e, 0, 1], partner, c == 0)

    def exchange_part(buf, e):
        for k in range(2):
            arrive(buf, e, sp_of(zh, 1 - c, (y + k) % 2), c == 1)

    def exchange_far(buf, e):
        for i in range(1, nh):
            index = sp_of((zh + nh - i) % nh, c, y)
            arrive(buf, e, index, zh >= i)
            exchange(buf, e, index, k_y.at[e, i], across, zh >= i)
            exchange(buf, e, index, k_part.at[e, i, 0], partner, zh >= i)

    def exchange_far_across(buf, e):
        for i in range(1, nh):
            index = sp_of((zh + nh - i) % nh, c, 1 - y)
            arrive(buf, e, index, zh >= i)
            exchange(buf, e, index, k_part.at[e, i, 1], partner, zh >= i)

    def exchange_far_part(buf, e):
        for i in range(1, nh):
            for k in range(2):
                arrive(buf, e, sp_of((zh + nh - i) % nh, 1 - c, (y + k) % 2), zh >= i)

    def rope(field):
        first, second = field[:, : HEAD // 2], field[:, HEAD // 2 :]
        return jnp.concatenate(
            [first * cosine - second * sine, first * sine + second * cosine], axis=-1
        )

    def project(buf):
        deep = buf.shape[2]
        return sum(
            dot(xbuf[:tok, k * deep : (k + 1) * deep], buf[k], ((1,), (1,))) for k in range(n)
        )

    proj = project(abuf)
    kvbuf[q] = proj[:, : 2 * HEAD].astype(BF16)
    exchange_send(kvbuf, 0)
    for u in range(cut):
        scatter_far(2, u)
        scatter_near(2, u)
    queries = [
        (proj[:, (2 + h) * HEAD : (3 + h) * HEAD] * HEAD ** (-0.5)).astype(BF16)
        for h in range(heads)
    ]

    def attend(index, masked):
        block = kvbuf[index]
        key, val = block[:, :HEAD], block[:, HEAD:]
        gates = gbuf[pick, :, pl.ds(pl.multiple_of(index * tok, tok), tok)]
        for h in range(heads):
            logits = dot(queries[h], key, ((1,), (1,)))
            logits = logits + gate_col[:, h : h + 1] - gates[h : h + 1, :]
            if masked:
                logits = jnp.where(causal, logits, -jnp.inf)
            weights = jnp.exp(logits)
            den[h] += jnp.broadcast_to(jnp.sum(weights, axis=-1, keepdims=True), (tok, HEAD))
            num[h] += dot(weights.astype(BF16), val)

    den[...] = jnp.zeros_like(den)
    num[...] = jnp.zeros_like(num)
    attend(q, True)
    for u in range(1, cut):
        for a in far:
            entry(1, *a, u)
    entry(1, *near, 0)
    exchange_across(kvbuf, 0)
    for a in far:
        beside(1, *a, 0)
    for u in range(cut):
        beside(2, 0, 0, u)
    exchange_part(kvbuf, 0)
    index = sp_of(zh, 0, 0)
    pl.when(index < q)(functools.partial(attend, index, False))
    for u in range(1, cut):
        entry(1, *near, u)
    exchange_far(kvbuf, 0)
    pl.when(index + 1 < q)(functools.partial(attend, index + 1, False))
    for u in range(1, cut):
        for a in far:
            beside(1, *a, u)
    beside(1, *near, 0)
    pl.when(index + 2 < q)(functools.partial(attend, index + 2, False))
    exchange_far_across(kvbuf, 0)
    for u in range(1, cut):
        beside(1, *near, u)
    for a in far:
        entry(2, *a, 0)
    rest(1)

    proj = project(bbuf)
    keys, vals, updates, marks = [], [], [], []
    for h in range(heads):
        base = h * HEAD
        key = rope(proj[:, base : base + HEAD]).astype(BF16)
        val = proj[:, base + width : base + width + HEAD].astype(BF16)
        column = within[:, h : h + 1]
        last = column[tok - 1 :, :]
        faded = (key.astype(F32) * jnp.exp(last - column)).astype(BF16)
        updates.append(dot(faded, val, ((0,), (0,))))
        high = last.astype(BF16).astype(F32)
        low = last - high
        marks.append(jnp.broadcast_to(high, (8, HEAD)))
        marks.append(jnp.broadcast_to(low, (8, HEAD)))
        keys.append(key)
        vals.append(val)
    marks.append(jnp.zeros((HEAD - 16 * heads, HEAD), F32))
    blocks = updates + [jnp.concatenate(marks, axis=0)]
    if len(blocks) % 2:
        blocks.append(jnp.zeros((HEAD, HEAD), F32))
    for k in range(0, len(blocks), 2):
        both = jnp.concatenate(blocks[k : k + 2], axis=1).astype(BF16)
        stbuf[q, k // 2 * HEAD : (k // 2 + 1) * HEAD, :] = both

    def piece_of(index, k):
        spot = slice(k % 2 * HEAD, (k % 2 + 1) * HEAD)
        return stbuf[index, k // 2 * HEAD : (k // 2 + 1) * HEAD, spot].astype(F32)

    for i in range(nh):
        for l in range(2):
            for e in range(2):
                if i or l or e:
                    index = sp_of((zh + i) % nh, (c + e) % 2, (y + l) % 2)
                    send(
                        stbuf.at[q], stbuf.at[q], st_send.at[i, l, e], st_recv.at[q],
                        device((zh + i) % nh, zl, (y + l) % 2, x, (c + e) % 2), index > q,
                    )
    exchange_far_part(kvbuf, 0)
    steps = [(entry, near, 0)]
    steps += [(entry, a, u) for u in range(1, cut) for a in far]
    steps += [(entry, near, u) for u in range(1, cut)]
    steps += [(beside, a, 0) for a in far]
    for i in range(1, nh):
        for j in range(4):
            index = sp_of((zh + nh - i) % nh, 0, 0) + j
            pl.when(zh >= i)(functools.partial(attend, index, False))
            for call, a, u in steps[:1]:
                call(2, *a, u)
            steps = steps[1:]
    local, lifts = [], []
    for h in range(heads):
        base = 2 * width + h * HEAD
        query = (rope(proj[:, base : base + HEAD]) * HEAD ** (-0.5)).astype(BF16)
        column = within[:, h : h + 1]
        gap = jnp.where(causal, column - turned[h : h + 1, :], 0.0)
        scores = dot(query, keys[h], ((1,), (1,)))
        weights = jnp.where(causal, scores * jnp.exp(gap), 0.0).astype(BF16)
        local.append(dot(weights, vals[h]))
        lifts.append((query.astype(F32) * jnp.exp(column)).astype(BF16))
    for call, a, u in steps:
        call(2, *a, u)
    for j in range(n - 1):
        receive(stbuf.at[j], st_recv.at[j], q > j)
    state[...] = jnp.zeros_like(state)
    for j in range(n - 1):
        def earlier(j=j):
            marked = piece_of(j, heads)
            for h in range(heads):
                total = marked[16 * h : 16 * h + 1] + marked[16 * h + 8 : 16 * h + 9]
                state[h] = jnp.exp(total) * state[h] + piece_of(j, h)

        pl.when(q > j)(earlier)
    retained, attended = [], []
    for h in range(heads):
        raw = local[h] + dot(lifts[h], state[h].astype(BF16))
        centre = jnp.mean(raw, axis=-1, keepdims=True)
        spread = jnp.mean(jnp.square(raw - centre), axis=-1, keepdims=True)
        retained.append(((raw - centre) * lax.rsqrt(spread + EPS)).astype(BF16))
        attended.append((num[h] / den[h]).astype(BF16))
    mixed = jnp.concatenate(retained + attended, axis=-1)
    beside(2, *near, 0)
    for u in range(1, cut):
        for a in far:
            beside(2, *a, u)
        beside(2, *near, u)
    rest(2)

    columns = obuf.shape[2]
    group = 2
    for part in range(n // group):
        for k in range(part * group, part * group + group):
            term = dot(mixed, obuf[k]).astype(BF16)
            outbuf[:, :, k * columns : (k + 1) * columns] = term.reshape(m, rows, columns)
        span = pl.ds(part * group * columns, group * columns)
        for r in reversed(range(nx)):
            for k in range(2):
                index = tp_of((x + r) % nx, (c + k) % 2)
                send(
                    outbuf.at[index, :, span], rsbuf.at[g, :, span],
                    r_send.at[part, r, k], r_recv.at[part, g],
                    device(zh, c, y, (x + r) % nx, (c + k) % 2),
                    apart if r == 0 and k == 0 else None,
                )
    for part in range(n // group):
        span = pl.ds(part * group * columns, group * columns)

        def keep():
            rsbuf[g, :, span] = outbuf[t, :, span]

        pl.when(own)(keep)
        total = None
        for r in range(nx):
            for j in range(2):
                index = tp_of((x + r) % nx, (zl + j) % 2)
                receive(
                    rsbuf.at[index, :, span], r_recv.at[part, index],
                    apart if r == 0 and j == 0 else None,
                )
                term = rsbuf[index, :, span].astype(F32)
                total = term if total is None else total + term
        out_ref[:, span] = total.astype(BF16)

    for copy, condition in started:
        guarded(condition, copy.wait_send)


def body(
    n,
    m,
    tokens,
    pre_gain,
    w_query_ret,
    w_key_ret,
    w_value_ret,
    w_query_att,
    w_key_att,
    w_value_att,
    w_out_ret,
    w_out_att,
    retain_log,
    forget_total,
):
    rows, depth = tokens.shape
    tok = rows * m
    heads = retain_log.shape[1]
    nh, nx = n // 4, m // 2
    half = HEAD // 2
    inverse = np.float32(THETA) ** (-np.arange(half, dtype=np.float32) / np.float32(half))
    angles = np.arange(n * tok, dtype=np.float32)[:, None] * inverse[None, :]
    table = np.concatenate([np.cos(angles), np.sin(angles)], axis=1).astype(np.float32)
    wide_a = 2 * HEAD + heads * HEAD
    wide_b = 3 * heads * HEAD
    deep = w_key_ret.shape[0]
    deep_o = w_out_ret.shape[0] + w_out_att.shape[0]
    tall = (heads // 2 + 1) * HEAD
    hbm = pl.BlockSpec(memory_space=pl.ANY)
    vmem = pl.BlockSpec(memory_space=pltpu.VMEM)
    dma = pltpu.SemaphoreType.DMA
    return pl.pallas_call(
        functools.partial(kernel, n, m, heads),
        out_shape=jax.ShapeDtypeStruct((rows, depth), BF16),
        in_specs=[hbm, vmem] + [hbm] * 11,
        out_specs=vmem,
        scratch_shapes=[
            pltpu.VMEM(tokens.shape, BF16),
            pltpu.VMEM((tok, HEAD), F32),
            pltpu.VMEM((2,) + retain_log.shape[::-1], F32),
            pltpu.VMEM((2,) + forget_total.shape, F32),
            pltpu.VMEM((tok + rows, depth), BF16),
            pltpu.VMEM((n + 1, wide_a, deep), BF16),
            pltpu.VMEM((n + 1, wide_b, deep), BF16),
            pltpu.VMEM((n + 1, deep_o, w_out_ret.shape[1]), BF16),
            pltpu.VMEM((n, tok, 2 * HEAD), BF16),
            pltpu.VMEM((n, tall, 2 * HEAD), BF16),
            pltpu.VMEM((heads, HEAD, HEAD), F32),
            pltpu.VMEM((heads, tok, HEAD), F32),
            pltpu.VMEM((heads, tok, HEAD), F32),
            pltpu.VMEM((m, rows, depth), BF16),
            pltpu.VMEM((m, rows, depth), BF16),
            dma((12,)),
            dma((2,)),
            dma((2,)),
            dma((1 + nx, TOKEN_CUT)),
            dma((nx - 1, 2, TOKEN_CUT)),
            dma((m, TOKEN_CUT)),
            dma((3, nh, 2, CUT)),
            dma((3, 2, CUT)),
            dma((3, nh, 2, 2, CUT)),
            dma((3, nh, 2, CUT)),
            dma((3, n, 2, CUT)),
            dma((1, nh - 1)),
            dma((1, nh)),
            dma((1, nh, 2)),
            dma((1, n)),
            dma((nh, 2, 2)),
            dma((n,)),
            dma((n // 2, nx, 2)),
            dma((n // 2, m)),
        ],
        compiler_params=pltpu.CompilerParams(
            collective_id=0, has_side_effects=True, vmem_limit_bytes=60 * 1024 * 1024
        ),
    )(
        tokens,
        pre_gain[None, :],
        w_query_ret.T,
        w_key_ret.T,
        w_value_ret.T,
        w_query_att.T,
        w_key_att.T,
        w_value_att.T,
        w_out_ret,
        w_out_att,
        jnp.asarray(table),
        retain_log.T,
        forget_total,
    )


def rotate(field, positions):
    half = field.shape[-1] // 2
    inverse = THETA ** (-jnp.arange(half, dtype=jnp.float32) / half)
    angles = positions[:, None] * inverse[None, :]
    cosine = jnp.cos(angles)[:, None, :]
    sine = jnp.sin(angles)[:, None, :]
    first_half = field[..., :half]
    second_half = field[..., half:]
    return jnp.concatenate(
        [first_half * cosine - second_half * sine, first_half * sine + second_half * cosine],
        axis=-1,
    )


def head_norm(values):
    centre = jnp.mean(values, axis=-1, keepdims=True)
    spread = jnp.mean(jnp.square(values - centre), axis=-1, keepdims=True)
    return (values - centre) * lax.rsqrt(spread + EPS)


def advance(state, pair):
    decay, update = pair
    return (jnp.exp(decay)[:, None, None] * state + update, state)


def plain_body(
    tokens,
    pre_gain,
    w_query_ret,
    w_key_ret,
    w_value_ret,
    w_query_att,
    w_key_att,
    w_value_att,
    w_out_ret,
    w_out_att,
    retain_log,
    forget_total,
):
    rows = tokens.astype(jnp.float32)
    normed = (
        rows * lax.rsqrt(jnp.mean(rows * rows, axis=-1, keepdims=True) + EPS) * pre_gain
    ).astype(jnp.bfloat16)
    gathered = lax.all_gather(normed, "tp", axis=0, tiled=True)
    tok_dev = gathered.shape[0]
    offset = lax.axis_index("sp") * tok_dev
    query_places = offset + jnp.arange(tok_dev, dtype=jnp.int32)
    positions = query_places.astype(jnp.float32)

    def blocked(values):
        return values.reshape((tok_dev // SPAN, SPAN) + values.shape[1:])

    pieces = (
        lax.all_gather(w_query_ret, "sp", axis=0, tiled=True),
        lax.all_gather(w_key_ret, "sp", axis=0, tiled=True),
        lax.all_gather(w_value_ret, "sp", axis=0, tiled=True),
        lax.all_gather(w_query_att, "sp", axis=0, tiled=True),
        lax.all_gather(w_key_att, "sp", axis=0, tiled=True),
        lax.all_gather(w_value_att, "sp", axis=0, tiled=True),
    )
    projected = tuple(
        (jnp.dot(gathered, piece, preferred_element_type=jnp.float32) for piece in pieces)
    )
    heads = retain_log.shape[1]
    shape = (tok_dev, heads, HEAD)
    query = blocked(
        (rotate(projected[0].reshape(shape), positions) * HEAD ** (-0.5)).astype(jnp.bfloat16)
    )
    key_rows = blocked(rotate(projected[1].reshape(shape), positions).astype(jnp.bfloat16))
    value_rows = blocked(projected[2].astype(jnp.bfloat16).reshape(shape))
    within = jnp.cumsum(blocked(retain_log), axis=1)
    causal = jnp.arange(SPAN)[:, None] >= jnp.arange(SPAN)[None, :]
    scores = jnp.einsum("bthd,bshd->bhts", query, key_rows, preferred_element_type=jnp.float32)
    turned = jnp.transpose(within, (0, 2, 1))
    gap = jnp.where(causal, turned[:, :, :, None] - turned[:, :, None, :], 0.0)
    weights = jnp.where(causal, scores * jnp.exp(gap), 0.0).astype(jnp.bfloat16)
    local = jnp.einsum("bhts,bshd->bthd", weights, value_rows, preferred_element_type=jnp.float32)
    last = within[:, -1]
    faded = (key_rows.astype(jnp.float32) * jnp.exp(last[:, None, :] - within)[..., None]).astype(
        jnp.bfloat16
    )
    updates = jnp.einsum("bshd,bshe->bhde", faded, value_rows, preferred_element_type=jnp.float32)
    zero_state = jnp.zeros((heads, HEAD, HEAD), jnp.float32)
    final, _ = lax.scan(advance, zero_state, (last, updates))
    decay_total = jnp.sum(last, axis=0)
    own_state = final.reshape(heads, HEAD * HEAD)
    every_total = lax.all_gather(
        decay_total[None].astype(jnp.bfloat16), "sp", axis=0, tiled=True
    ).astype(jnp.float32)
    every_state = lax.all_gather(
        own_state[None].astype(jnp.bfloat16), "sp", axis=0, tiled=True
    ).astype(jnp.float32)
    device_order = jnp.arange(every_total.shape[0], dtype=jnp.int32)[:, None]
    earlier = device_order < lax.axis_index("sp")
    before = jnp.sum(jnp.where(earlier, every_total, 0.0), axis=0)
    through = jnp.cumsum(every_total, axis=0)
    fading = jnp.where(earlier, jnp.exp(jnp.where(earlier, before[None, :] - through, 0.0)), 0.0)
    incoming = jnp.einsum("jh,jhe->he", fading, every_state, precision=HIGH)
    _, befores = lax.scan(advance, incoming.reshape(heads, HEAD, HEAD), (last, updates))
    lifted = (query.astype(jnp.float32) * jnp.exp(within)[..., None]).astype(jnp.bfloat16)
    carried = jnp.einsum(
        "bthd,bhde->bthe", lifted, befores.astype(jnp.bfloat16), preferred_element_type=jnp.float32
    )
    retained = (
        head_norm((local + carried).reshape(shape))
        .astype(jnp.bfloat16)
        .reshape(tok_dev, heads * HEAD)
    )
    raw_key = projected[4]
    gate_heads = forget_total.shape[0]
    kv_local = raw_key.shape[1] // HEAD
    group = gate_heads // kv_local
    query = (
        (projected[3] * HEAD ** (-0.5)).astype(jnp.bfloat16).reshape(tok_dev, kv_local, group, HEAD)
    )
    key_rows = raw_key.astype(jnp.bfloat16)
    value_rows = projected[5].astype(jnp.bfloat16)
    gate_rows = lax.dynamic_slice_in_dim(forget_total, offset, tok_dev, 1).reshape(
        kv_local, group, tok_dev
    )
    last_row = offset + tok_dev - 1
    init = (
        jnp.zeros((kv_local, group, tok_dev, HEAD), jnp.float32),
        jnp.zeros((kv_local, group, tok_dev), jnp.float32),
    )
    key_piece = lax.all_gather(key_rows, "sp", axis=0, tiled=True)
    value_piece = lax.all_gather(value_rows, "sp", axis=0, tiled=True)
    count = key_piece.shape[0] // KEY_SPAN

    def one_block(index, inner):
        first = index * KEY_SPAN

        def compute(state):
            weighted, total = state
            key_block = lax.dynamic_slice_in_dim(key_piece, index * KEY_SPAN, KEY_SPAN, 0).reshape(
                KEY_SPAN, kv_local, HEAD
            )
            value_block = lax.dynamic_slice_in_dim(
                value_piece, index * KEY_SPAN, KEY_SPAN, 0
            ).reshape(KEY_SPAN, kv_local, HEAD)
            gate_keys = lax.dynamic_slice_in_dim(forget_total, first, KEY_SPAN, 1).reshape(
                kv_local, group, KEY_SPAN
            )
            scores = jnp.einsum(
                "tcgd,scd->cgts", query, key_block, preferred_element_type=jnp.float32
            )
            logits = scores + gate_rows[:, :, :, None] - gate_keys[:, :, None, :]
            allowed = (first + jnp.arange(KEY_SPAN, dtype=jnp.int32))[None, :] <= query_places[
                :, None
            ]
            weights = jnp.exp(jnp.where(allowed, logits, -jnp.inf))
            total = total + jnp.sum(weights, axis=-1)
            weighted = weighted + jnp.einsum(
                "cgts,scd->cgtd",
                weights.astype(jnp.bfloat16),
                value_block,
                preferred_element_type=jnp.float32,
            )
            return (weighted, total)

        def skipped(state):
            return state

        return lax.cond(first <= last_row, compute, skipped, inner)

    weighted, total = lax.fori_loop(0, count, one_block, init)
    result = weighted / total[..., None]
    attended = (
        jnp.transpose(result, (2, 0, 1, 3)).reshape(tok_dev, gate_heads * HEAD).astype(jnp.bfloat16)
    )
    out_ret, out_att = (
        lax.all_gather(w_out_ret, "sp", axis=1, tiled=True),
        lax.all_gather(w_out_att, "sp", axis=1, tiled=True),
    )
    return lax.psum_scatter(
        (
            jnp.dot(retained, out_ret, preferred_element_type=jnp.float32)
            + jnp.dot(attended, out_att, preferred_element_type=jnp.float32)
        ).astype(jnp.bfloat16),
        "tp",
        scatter_dimension=0,
        tiled=True,
    )


def choose(n, m, *arrays):
    tokens, w_key_ret, w_out_ret = arrays[0], arrays[3], arrays[8]
    whole_tiles = w_out_ret.shape[1] % LANES == 0 and w_key_ret.shape[0] % LANES == 0
    heads = arrays[10].shape[1]
    small = 16 * heads <= HEAD and arrays[7].shape[1] == HEAD and arrays[11].shape[0] == heads
    paired = n % 4 == 0 and n > 4 and m % 2 == 0 and m > 2
    if paired and whole_tiles and small and tokens.shape[0] * m == SPAN:
        return body(n, m, *arrays)
    return plain_body(*arrays)


def solution(mesh):
    return jax.shard_map(
        functools.partial(choose, mesh.shape["sp"], mesh.shape["tp"]),
        mesh=mesh,
        in_specs=(
            P(("sp", "tp"), None),
            P(),
            P("sp", "tp"),
            P("sp", "tp"),
            P("sp", "tp"),
            P("sp", "tp"),
            P("sp", "tp"),
            P("sp", "tp"),
            P("tp", "sp"),
            P("tp", "sp"),
            P("sp", "tp"),
            P("tp", None),
        ),
        out_specs=P(("sp", "tp"), None),
        check_vma=False,
    )
```

```python
import functools

import jax
import jax.numpy as jnp
import numpy as np
from jax import lax
from jax.experimental import pallas as pl
from jax.experimental.pallas import tpu as pltpu
from jax.sharding import PartitionSpec as P

HEAD = 64
EPS = 1e-06
THETA = 10000.0
F32 = jnp.float32
BF16 = jnp.bfloat16
MESH = pl.DeviceIdType.MESH
SPAN = 256
KEY_SPAN = 256
LANES = 128
CUTS = (2, 2, 1, 2)
LOG2E = float(np.log2(np.e))
TOKEN_CUT = 2
HIGH = lax.Precision.HIGHEST


def dot(a, b, dims=((1,), (0,))):
    return lax.dot_general(a, b, (dims, ((), ())), preferred_element_type=F32)


def kernel(
    n,
    m,
    heads,
    tok_hbm,
    gain_ref,
    wq_ret_hbm,
    wk_ret_hbm,
    wv_ret_hbm,
    wq_att_hbm,
    wk_att_hbm,
    wv_att_hbm,
    wo_ret_hbm,
    wo_att_hbm,
    table_hbm,
    logs_hbm,
    gate_hbm,
    out_ref,
    tokens,
    table,
    lbuf,
    gbuf,
    xbuf,
    abuf,
    bbuf,
    cbuf,
    obuf,
    kvbuf,
    stbuf,
    state,
    num,
    qbuf,
    cbuf_gate,
    outbuf,
    rsbuf,
    load,
    small_send,
    small_recv,
    x_send,
    x_fwd,
    x_recv,
    w_send,
    w_near,
    w_part,
    w_y,
    w_recv,
    k_send,
    k_y,
    k_part,
    k_recv,
    st_send,
    st_fwd,
    st_recv,
    r_send,
    r_recv,
):
    s, t = lax.axis_index("sp"), lax.axis_index("tp")
    nh, nx = n // 4, m // 2
    y, zl, zh = s % 2, (s // 2) % 2, s // 4
    c, x = t % 2, t // 2
    own = zl == c
    apart = zl != c

    def sp_of(zh_, zl_, y_):
        return zh_ * 4 + zl_ * 2 + y_

    def tp_of(x_, c_):
        return x_ * 2 + c_

    def device(zh_, zl_, y_, x_, c_):
        return {"sp": sp_of(zh_, zl_, y_), "tp": tp_of(x_, c_)}

    q, g = sp_of(zh, c, y), tp_of(x, zl)
    partner = device(zh, zl, y, x, 1 - c)
    across = device(zh, zl, 1 - y, x, c)
    rows = tokens.shape[0]
    tok = rows * m
    width = heads * HEAD
    half_o = wo_ret_hbm.shape[0]

    slot = jnp.where(own, s, n)
    piece = jnp.where(own, t, m)
    loads = [
        pltpu.make_async_copy(source, target, load.at[k])
        for k, (source, target) in enumerate((
            (tok_hbm, tokens),
            (wk_att_hbm, abuf.at[slot, pl.ds(0, HEAD)]),
            (wv_att_hbm, abuf.at[slot, pl.ds(HEAD, HEAD)]),
            (wq_att_hbm, abuf.at[slot, pl.ds(2 * HEAD, width)]),
            (wk_ret_hbm, bbuf.at[slot, pl.ds(0, width)]),
            (wv_ret_hbm, bbuf.at[slot, pl.ds(width, width)]),
            (wq_ret_hbm, cbuf.at[slot]),
            (wo_ret_hbm, obuf.at[slot, pl.ds(0, half_o)]),
            (wo_att_hbm, obuf.at[slot, pl.ds(half_o, wo_att_hbm.shape[0])]),
            (table_hbm.at[pl.ds(pl.multiple_of(q * tok, tok), tok)], table),
            (logs_hbm, lbuf.at[0]),
            (gate_hbm, gbuf.at[0]),
        ))
    ]
    for copy in loads:
        copy.start()

    barrier = pltpu.get_barrier_semaphore()
    greeted = [
        device((zh + i) % nh, zl, 1 - y, x, (c + k) % 2) for i in range(nh) for k in range(2)
    ]
    for i in reversed(range(nh)):
        for j in reversed(range(2)):
            for k in range(2):
                if i or j or k:
                    greeted.append(device((zh + i) % nh, (zl + j) % 2, y, x, (c + k) % 2))
    for r in range(1, nx):
        for j in range(2):
            for k in range(2):
                greeted.append(device(zh, (zl + j) % 2, y, (x + r) % nx, (c + k) % 2))
    for other in greeted:
        pl.semaphore_signal(barrier, inc=1, device_id=other, device_id_type=MESH)

    started = []

    def guarded(condition, action):
        if condition is None:
            action()
        else:
            pl.when(condition)(action)

    def send(source, target, send_sem, recv_sem, where, condition=None):
        copy = pltpu.make_async_remote_copy(
            src_ref=source, dst_ref=target, send_sem=send_sem, recv_sem=recv_sem,
            device_id=where, device_id_type=MESH,
        )
        guarded(condition, copy.start)
        started.append((copy, condition))

    def receive(target, recv_sem, condition=None):
        copy = pltpu.make_async_remote_copy(
            src_ref=target, dst_ref=target, send_sem=recv_sem, recv_sem=recv_sem,
            device_id=partner, device_id_type=MESH,
        )
        guarded(condition, copy.wait_recv)

    loads[0].wait()
    values = tokens[...].astype(F32)
    scale = lax.rsqrt(jnp.mean(values * values, axis=-1, keepdims=True) + EPS)
    xbuf[pl.ds(pl.multiple_of(piece * rows, rows), rows), :] = (
        values * scale * gain_ref[...]
    ).astype(BF16)
    for copy in loads[1:]:
        copy.wait()
    pl.semaphore_wait(barrier, len(greeted))

    parts = (abuf, bbuf, cbuf, obuf)
    cuts = CUTS

    def chunk(p, index, k, u):
        length = parts[p].shape[1] // (2 * cuts[p])
        start = pl.multiple_of((k * cuts[p] + u) * length, length)
        return parts[p].at[index, pl.ds(start, length)]

    def scatter_one(p, i, k, u, condition):
        core = (c + k) % 2
        send(
            chunk(p, slot, core, u), chunk(p, s, core, u),
            w_send.at[p, i, k, u], w_recv.at[p, s, core, u],
            device((zh + i) % nh, c, y, x, core), condition,
        )

    def scatter_chip(p):
        for u in range(cuts[p]):
            scatter_one(p, 0, 1, u, own)

    def scatter_near(p, u):
        for k in range(2):
            core = (c + k) % 2
            send(
                chunk(p, slot, core, u), chunk(p, s, core, u),
                w_near.at[p, k, u], w_recv.at[p, s, core, u],
                device(zh, c, y, x, core), apart,
            )

    def scatter_far(p, u, condition=None):
        for i in range(1, nh):
            for k in range(2):
                scatter_one(p, i, k, u, condition)

    middle = zl != zh % 2
    outer = zl == zh % 2

    def entry(p, i, j, u, condition=None):
        index = sp_of((zh + i) % nh, (zl + j) % 2, y)
        here = i == 0 and j == 0
        spot = chunk(p, index, c, u)
        receive(spot, w_recv.at[p, index, c, u], apart if here else condition)
        send(spot, spot, w_y.at[p, i, j, u], w_recv.at[p, index, c, u], across, condition)
        send(
            spot, spot, w_part.at[p, i, j, 0, u], w_recv.at[p, index, c, u], partner,
            own if here else condition,
        )

    def beside(p, i, j, u):
        index = sp_of((zh + i) % nh, (zl + j) % 2, 1 - y)
        spot = chunk(p, index, c, u)
        receive(spot, w_recv.at[p, index, c, u])
        send(spot, spot, w_part.at[p, i, j, 1, u], w_recv.at[p, index, c, u], partner)

    def ready(p, i, j, l):
        index = sp_of((zh + i) % nh, (zl + j) % 2, (y + l) % 2)
        for u in range(cuts[p]):
            receive(
                chunk(p, index, 1 - c, u), w_recv.at[p, index, 1 - c, u],
                apart if i == 0 and j == 0 and l == 0 else None,
            )

    def rest(p):
        for i in range(nh):
            for j in range(2):
                for l in range(2):
                    ready(p, i, j, l)

    far = [(i, j) for i in range(1, nh) for j in range(2)]
    near = (0, 1)
    pieces = x_recv.shape[1]

    def rows_of(index, u):
        length = rows // pieces
        return xbuf.at[pl.ds(pl.multiple_of((index * pieces + u) * length, length), length)]

    def pass_tokens(k, u):
        index = tp_of(x, (c + k) % 2)
        spot = rows_of(index, u)
        receive(spot, x_recv.at[index, u], apart if k == 0 else None)
        for r in range(1, nx):
            send(
                spot, spot, x_fwd.at[r - 1, k, u], x_recv.at[index, u],
                device(zh, zl, y, (x + r) % nx, c), apart,
            )

    send(
        lbuf.at[0], lbuf.at[1], small_send.at[0], small_recv.at[0],
        device(zh, c, y, x, zl), apart,
    )
    send(gbuf.at[0], gbuf.at[1], small_send.at[1], small_recv.at[1], partner, own)
    for u in range(cuts[0]):
        scatter_far(0, u)
    scatter_chip(0)
    for u in range(pieces):
        send(
            rows_of(piece, u), rows_of(t, u), x_send.at[0, u], x_recv.at[t, u],
            device(zh, 1 - zl, y, x, zl),
        )
        for r in range(1, nx):
            send(
                rows_of(piece, u), rows_of(t, u), x_send.at[1 + r, u], x_recv.at[t, u],
                device(zh, zl, y, (x + r) % nx, zl),
            )
        send(
            rows_of(piece, u), rows_of(t, u), x_send.at[1, u], x_recv.at[t, u],
            device(zh, zl, y, x, zl), apart,
        )
    for u in range(cuts[0]):
        scatter_near(0, u)
    for p in range(1, 4):
        scatter_chip(p)
    for p in range(1, 3):
        for u in range(cuts[p]):
            scatter_far(p, u)
            scatter_near(p, u)
    for p in range(4):
        for u in range(cuts[p]):
            entry(p, 0, 0, u)
    lines = lax.broadcasted_iota(jnp.int32, (tok, tok), 0)
    lanes = lax.broadcasted_iota(jnp.int32, (tok, tok), 1)
    causal = lines >= lanes
    upto = jnp.where(lines <= lanes, 1.0, 0.0)
    receive(lbuf.at[1], small_recv.at[0], apart)
    receive(gbuf.at[1], small_recv.at[1], apart)
    pick = jnp.where(own, 0, 1)
    logs = jnp.concatenate([lbuf[pick], jnp.zeros((8 - heads, tok), F32)], axis=0)
    turned = lax.dot_general(
        logs, upto, (((1,), (0,)), ((), ())),
        preferred_element_type=F32, precision=lax.Precision.HIGHEST,
    )
    fill = jnp.zeros((LANES - 8, tok), F32)
    within = jnp.concatenate([turned, fill], axis=0).T
    gates_own = gbuf[pick, :, pl.ds(pl.multiple_of(q * tok, tok), tok)]
    gate_col = jnp.concatenate(
        [gates_own, jnp.zeros((LANES - heads, tok), F32)], axis=0
    ).T
    cosine, sine = table[:, : HEAD // 2], table[:, HEAD // 2 :]

    for u in range(cuts[0]):
        beside(0, 0, 0, u)
    for a in far:
        entry(0, *a, 0)
    for k in range(2):
        pass_tokens(k, 0)
    for u in range(cuts[1]):
        beside(1, 0, 0, u)
    for u in range(1, cuts[0]):
        for a in far:
            entry(0, *a, u)
    for a in far:
        beside(0, *a, 0)
    for u in range(1, pieces):
        for k in range(2):
            pass_tokens(k, u)
    for u in range(cuts[0]):
        entry(0, *near, u)
    for a in far:
        entry(1, *a, 0, middle)
    for u in range(1, cuts[0]):
        for a in far:
            beside(0, *a, u)
    for p in range(2, 4):
        for u in range(cuts[p]):
            beside(p, 0, 0, u)
    for u in range(cuts[0]):
        beside(0, *near, u)
    for a in far:
        entry(1, *a, 0, outer)

    for r in range(1, nx):
        for k in range(2):
            index = tp_of((x + r) % nx, k)
            for u in range(pieces):
                receive(rows_of(index, u), x_recv.at[index, u])
    rest(0)

    def exchange(buf, e, index, sem, where, condition):
        send(buf.at[index], buf.at[index], sem, k_recv.at[e, index], where, condition)

    def arrive(buf, e, index, condition):
        receive(buf.at[index], k_recv.at[e, index], condition)

    def exchange_send(buf, e):
        for i in range(1, nh):
            exchange(
                buf, e, q, k_send.at[e, i - 1], device((zh + i) % nh, zl, y, x, c), zh + i < nh
            )
        exchange(buf, e, q, k_y.at[e, 0], across, c + y < 2)
        exchange(buf, e, q, k_part.at[e, 0, 0], partner, c == 0)

    def exchange_across(buf, e):
        index = sp_of(zh, c, 1 - y)
        arrive(buf, e, index, c <= y)
        exchange(buf, e, index, k_part.at[e, 0, 1], partner, c == 0)

    def exchange_part(buf, e):
        for k in range(2):
            arrive(buf, e, sp_of(zh, 1 - c, (y + k) % 2), c == 1)

    def exchange_far(buf, e):
        for i in range(1, nh):
            index = sp_of((zh + nh - i) % nh, c, y)
            arrive(buf, e, index, zh >= i)
            exchange(buf, e, index, k_y.at[e, i], across, zh >= i)
            exchange(buf, e, index, k_part.at[e, i, 0], partner, zh >= i)

    def exchange_far_across(buf, e):
        for i in range(1, nh):
            index = sp_of((zh + nh - i) % nh, c, 1 - y)
            arrive(buf, e, index, zh >= i)
            exchange(buf, e, index, k_part.at[e, i, 1], partner, zh >= i)

    def exchange_far_part(buf, e):
        for i in range(1, nh):
            for k in range(2):
                arrive(buf, e, sp_of((zh + nh - i) % nh, 1 - c, (y + k) % 2), zh >= i)

    def rope(field):
        first, second = field[:, : HEAD // 2], field[:, HEAD // 2 :]
        return jnp.concatenate(
            [first * cosine - second * sine, first * sine + second * cosine], axis=-1
        )

    def project(buf):
        deep = buf.shape[2]
        return sum(
            dot(xbuf[:tok, k * deep : (k + 1) * deep], buf[k], ((1,), (1,))) for k in range(n)
        )

    proj = project(abuf)
    kvbuf[q] = proj[:, : 2 * HEAD].astype(BF16)
    exchange_send(kvbuf, 0)
    scatter_far(3, 0)
    scatter_near(3, 0)
    for u in range(1, cuts[3]):
        scatter_far(3, u, zh == nh - 1)
        scatter_near(3, u)
    wide = heads * tok
    zeros = jnp.zeros((tok, HEAD), F32)
    for h in range(heads):
        query = proj[:, (2 + h) * HEAD : (3 + h) * HEAD] * (HEAD ** (-0.5) * LOG2E)
        qbuf[h * tok : (h + 1) * tok, :] = jnp.concatenate([query, zeros], axis=1).astype(BF16)
        cbuf_gate[h * tok : (h + 1) * tok, :] = jnp.broadcast_to(
            gate_col[:, h : h + 1] * LOG2E, (tok, LANES)
        )
    low_lanes = lax.broadcasted_iota(jnp.int32, (tok, 2 * HEAD), 1) < HEAD

    def attend(indices, masked=False):
        total = None if masked else num[...]
        for index in indices:
            block = kvbuf[index]
            values = jnp.where(low_lanes, jnp.ones_like(block), block)
            gates = gbuf[pick, :, pl.ds(pl.multiple_of(index * tok, tok), tok)] * LOG2E
            logits = dot(qbuf[...], block, ((1,), (1,)))
            column = cbuf_gate[...]
            column = jnp.concatenate([column] * (tok // LANES), axis=1)
            pieces_ = []
            for h in range(heads):
                part = slice(h * tok, (h + 1) * tok)
                shifted = logits[part] + column[part] - gates[h : h + 1, :]
                if masked:
                    shifted = jnp.where(causal, shifted, -jnp.inf)
                pieces_.append(jnp.exp2(shifted).astype(BF16))
            term = dot(jnp.concatenate(pieces_, axis=0), values)
            total = term if total is None else total + term
        num[...] = total

    for u in range(1, cuts[1]):
        for a in far:
            entry(1, *a, u)
    attend([q], True)
    for a in far:
        beside(1, *a, 0)
    for u in range(cuts[1]):
        entry(1, *near, u)
    exchange_across(kvbuf, 0)
    exchange_part(kvbuf, 0)
    index = sp_of(zh, 0, 0)
    pl.when(index < q)(functools.partial(attend, [index]))
    exchange_far(kvbuf, 0)
    pl.when(index + 1 < q)(functools.partial(attend, [index + 1]))
    for u in range(1, cuts[1]):
        for a in far:
            beside(1, *a, u)
    for u in range(cuts[2]):
        for a in far:
            entry(2, *a, u)
    pl.when(index + 2 < q)(functools.partial(attend, [index + 2]))
    for u in range(cuts[1]):
        beside(1, *near, u)
    for u in range(cuts[2]):
        entry(2, *near, u)
    exchange_far_across(kvbuf, 0)
    for a in far:
        entry(3, *a, 0)
    rest(1)

    proj = project(bbuf)
    keys, vals, updates, marks = [], [], [], []
    for h in range(heads):
        base = h * HEAD
        key = rope(proj[:, base : base + HEAD]).astype(BF16)
        val = proj[:, base + width : base + width + HEAD].astype(BF16)
        column = within[:, h : h + 1]
        last = column[tok - 1 :, :]
        faded = (key.astype(F32) * jnp.exp(last - column)).astype(BF16)
        updates.append(dot(faded, val, ((0,), (0,))))
        high = last.astype(BF16).astype(F32)
        low = last - high
        marks.append(jnp.broadcast_to(high, (8, HEAD)))
        marks.append(jnp.broadcast_to(low, (8, HEAD)))
        keys.append(key)
        vals.append(val)
    marks.append(jnp.zeros((HEAD - 16 * heads, HEAD), F32))
    blocks = updates + [jnp.concatenate(marks, axis=0)]
    if len(blocks) % 2:
        blocks.append(jnp.zeros((HEAD, HEAD), F32))
    for k in range(0, len(blocks), 2):
        both = jnp.concatenate(blocks[k : k + 2], axis=1).astype(BF16)
        stbuf[q, k // 2 * HEAD : (k // 2 + 1) * HEAD, :] = both

    def piece_of(index, k):
        spot = slice(k % 2 * HEAD, (k % 2 + 1) * HEAD)
        return stbuf[index, k // 2 * HEAD : (k // 2 + 1) * HEAD, spot].astype(F32)

    for i in range(1, nh):
        send(
            stbuf.at[q], stbuf.at[q], st_send.at[i, 0, 0], st_recv.at[q],
            device((zh + i) % nh, zl, y, x, c), zh + i < nh,
        )
    for l in range(2):
        for e in range(2):
            if l or e:
                index = sp_of(zh, (c + e) % 2, (y + l) % 2)
                send(
                    stbuf.at[q], stbuf.at[q], st_send.at[0, l, e], st_recv.at[q],
                    device(zh, zl, (y + l) % 2, x, (c + e) % 2), index > q,
                )
    for u in range(1, cuts[3]):
        scatter_far(3, u, zh < nh - 1)
    for u in range(cuts[2]):
        for a in far:
            beside(2, *a, u)
        beside(2, *near, u)
    entry(3, *near, 0)
    rest(2)

    for i in range(1, nh):
        index = sp_of((zh + nh - i) % nh, c, y)
        receive(stbuf.at[index], st_recv.at[index], zh >= i)
        for l in range(2):
            for e in range(2):
                if l or e:
                    send(
                        stbuf.at[index], stbuf.at[index], st_fwd.at[i, l, e], st_recv.at[index],
                        device(zh, zl, (y + l) % 2, x, (c + e) % 2), zh >= i,
                    )
    proj = project(cbuf)
    local, lifts = [], []
    for h in range(heads):
        query = (rope(proj[:, h * HEAD : (h + 1) * HEAD]) * HEAD ** (-0.5)).astype(BF16)
        column = within[:, h : h + 1]
        gap = jnp.where(causal, column - turned[h : h + 1, :], 0.0)
        scores = dot(query, keys[h], ((1,), (1,)))
        weights = jnp.where(causal, scores * jnp.exp(gap), 0.0).astype(BF16)
        local.append(dot(weights, vals[h]))
        lifts.append((query.astype(F32) * jnp.exp(column)).astype(BF16))
    exchange_far_part(kvbuf, 0)
    steps = [(beside, near, 0)]
    steps += [(entry, a, u) for u in range(1, cuts[3]) for a in far]
    steps += [(entry, near, u) for u in range(1, cuts[3])]
    for i in range(1, nh):
        index = sp_of((zh + nh - i) % nh, 0, 0)
        for half in range(2):
            pl.when(zh >= i)(
                functools.partial(attend, [index + 2 * half, index + 2 * half + 1])
            )
            for call, a, u in steps[:1]:
                call(3, *a, u)
            steps = steps[1:]
    for call, a, u in steps:
        call(3, *a, u)
    for i in range(1, nh):
        for l in range(2):
            for e in range(2):
                if l or e:
                    index = sp_of((zh + nh - i) % nh, (c + e) % 2, (y + l) % 2)
                    receive(stbuf.at[index], st_recv.at[index], zh >= i)
    for l in range(2):
        for e in range(2):
            if l or e:
                index = sp_of(zh, (c + e) % 2, (y + l) % 2)
                receive(stbuf.at[index], st_recv.at[index], index < q)
    state[...] = jnp.zeros_like(state)
    for j in range(n - 1):
        def earlier(j=j):
            marked = piece_of(j, heads)
            for h in range(heads):
                total = marked[16 * h : 16 * h + 1] + marked[16 * h + 8 : 16 * h + 9]
                state[h] = jnp.exp(total) * state[h] + piece_of(j, h)

        pl.when(q > j)(earlier)
    retained, attended = [], []
    for h in range(heads):
        raw = local[h] + dot(lifts[h], state[h].astype(BF16))
        centre = jnp.mean(raw, axis=-1, keepdims=True)
        spread = jnp.mean(jnp.square(raw - centre), axis=-1, keepdims=True)
        retained.append(((raw - centre) * lax.rsqrt(spread + EPS)).astype(BF16))
        both = num[h * tok : (h + 1) * tok, :]
        attended.append((both[:, HEAD:] / both[:, :HEAD]).astype(BF16))
    mixed = jnp.concatenate(retained + attended, axis=-1)
    order = [(i, j) for i in range(nh) for j in range(2)]

    def produce(i, j, l):
        index = sp_of((zh + i) % nh, (zl + j) % 2, (y + l) % 2)
        ready(3, i, j, l)
        outbuf[index] = dot(mixed, obuf[index]).astype(BF16)
        for r in reversed(range(nx)):
            for k in range(2):
                where = tp_of((x + r) % nx, (c + k) % 2)
                rows_there = pl.ds(pl.multiple_of(where * rows, rows), rows)
                send(
                    outbuf.at[index, rows_there], rsbuf.at[g, index],
                    r_send.at[index, r, k], r_recv.at[index, g],
                    device(zh, c, y, (x + r) % nx, (c + k) % 2),
                    apart if r == 0 and k == 0 else None,
                )

    plan = [(i, j, l) for i in range(nh) for l in range(2) for j in range(2)]
    for i, j, l in plan[:2]:
        produce(i, j, l)
    for u in range(1, cuts[3]):
        beside(3, *near, u)
    for a in far:
        beside(3, *a, 0)
    for i, j, l in plan[2:6]:
        produce(i, j, l)
    for u in range(1, cuts[3]):
        for a in far:
            beside(3, *a, u)
    for i, j, l in plan[6:]:
        produce(i, j, l)
    columns = obuf.shape[2]
    for i, j, l in plan:
        index = sp_of((zh + i) % nh, (zl + j) % 2, (y + l) % 2)

        def keep(index=index):
            rsbuf[g, index] = outbuf[index, pl.ds(pl.multiple_of(t * rows, rows), rows)]

        pl.when(own)(keep)
        total = None
        for r in range(nx):
            for e in range(2):
                other = tp_of((x + r) % nx, (zl + e) % 2)
                receive(
                    rsbuf.at[other, index], r_recv.at[index, other],
                    apart if r == 0 and e == 0 else None,
                )
                term = rsbuf[other, index].astype(F32)
                total = term if total is None else total + term
        span = pl.ds(pl.multiple_of(index * columns, columns), columns)
        out_ref[:, span] = total.astype(BF16)
    for copy, condition in started:
        guarded(condition, copy.wait_send)


def body(
    n,
    m,
    tokens,
    pre_gain,
    w_query_ret,
    w_key_ret,
    w_value_ret,
    w_query_att,
    w_key_att,
    w_value_att,
    w_out_ret,
    w_out_att,
    retain_log,
    forget_total,
):
    rows, depth = tokens.shape
    tok = rows * m
    heads = retain_log.shape[1]
    nh, nx = n // 4, m // 2
    half = HEAD // 2
    inverse = np.float32(THETA) ** (-np.arange(half, dtype=np.float32) / np.float32(half))
    angles = np.arange(n * tok, dtype=np.float32)[:, None] * inverse[None, :]
    table = np.concatenate([np.cos(angles), np.sin(angles)], axis=1).astype(np.float32)
    wide_a = 2 * HEAD + heads * HEAD
    wide_b, wide_c = 2 * heads * HEAD, heads * HEAD
    deep = w_key_ret.shape[0]
    deep_o = w_out_ret.shape[0] + w_out_att.shape[0]
    tall = (heads // 2 + 1) * HEAD
    hbm = pl.BlockSpec(memory_space=pl.ANY)
    vmem = pl.BlockSpec(memory_space=pltpu.VMEM)
    dma = pltpu.SemaphoreType.DMA
    return pl.pallas_call(
        functools.partial(kernel, n, m, heads),
        out_shape=jax.ShapeDtypeStruct((rows, depth), BF16),
        in_specs=[hbm, vmem] + [hbm] * 11,
        out_specs=vmem,
        scratch_shapes=[
            pltpu.VMEM(tokens.shape, BF16),
            pltpu.VMEM((tok, HEAD), F32),
            pltpu.VMEM((2,) + retain_log.shape[::-1], F32),
            pltpu.VMEM((2,) + forget_total.shape, F32),
            pltpu.VMEM((tok + rows, depth), BF16),
            pltpu.VMEM((n + 1, wide_a, deep), BF16),
            pltpu.VMEM((n + 1, wide_b, deep), BF16),
            pltpu.VMEM((n + 1, wide_c, deep), BF16),
            pltpu.VMEM((n + 1, deep_o, w_out_ret.shape[1]), BF16),
            pltpu.VMEM((n, tok, 2 * HEAD), BF16),
            pltpu.VMEM((n, tall, 2 * HEAD), BF16),
            pltpu.VMEM((heads, HEAD, HEAD), F32),
            pltpu.VMEM((heads * tok, 2 * HEAD), F32),
            pltpu.VMEM((heads * tok, 2 * HEAD), BF16),
            pltpu.VMEM((heads * tok, LANES), F32),
            pltpu.VMEM((n, tok, w_out_ret.shape[1]), BF16),
            pltpu.VMEM((m, n, rows, w_out_ret.shape[1]), BF16),
            dma((12,)),
            dma((2,)),
            dma((2,)),
            dma((1 + nx, TOKEN_CUT)),
            dma((nx - 1, 2, TOKEN_CUT)),
            dma((m, TOKEN_CUT)),
            dma((len(CUTS), nh, 2, max(CUTS))),
            dma((len(CUTS), 2, max(CUTS))),
            dma((len(CUTS), nh, 2, 2, max(CUTS))),
            dma((len(CUTS), nh, 2, max(CUTS))),
            dma((len(CUTS), n, 2, max(CUTS))),
            dma((1, nh - 1)),
            dma((1, nh)),
            dma((1, nh, 2)),
            dma((1, n)),
            dma((nh, 2, 2)),
            dma((nh, 2, 2)),
            dma((n,)),
            dma((n, nx, 2)),
            dma((n, m)),
        ],
        compiler_params=pltpu.CompilerParams(
            collective_id=0, has_side_effects=True, vmem_limit_bytes=60 * 1024 * 1024
        ),
    )(
        tokens,
        pre_gain[None, :],
        w_query_ret.T,
        w_key_ret.T,
        w_value_ret.T,
        w_query_att.T,
        w_key_att.T,
        w_value_att.T,
        w_out_ret,
        w_out_att,
        jnp.asarray(table),
        retain_log.T,
        forget_total,
    )


def rotate(field, positions):
    half = field.shape[-1] // 2
    inverse = THETA ** (-jnp.arange(half, dtype=jnp.float32) / half)
    angles = positions[:, None] * inverse[None, :]
    cosine = jnp.cos(angles)[:, None, :]
    sine = jnp.sin(angles)[:, None, :]
    first_half = field[..., :half]
    second_half = field[..., half:]
    return jnp.concatenate(
        [first_half * cosine - second_half * sine, first_half * sine + second_half * cosine],
        axis=-1,
    )


def head_norm(values):
    centre = jnp.mean(values, axis=-1, keepdims=True)
    spread = jnp.mean(jnp.square(values - centre), axis=-1, keepdims=True)
    return (values - centre) * lax.rsqrt(spread + EPS)


def advance(state, pair):
    decay, update = pair
    return (jnp.exp(decay)[:, None, None] * state + update, state)


def plain_body(
    tokens,
    pre_gain,
    w_query_ret,
    w_key_ret,
    w_value_ret,
    w_query_att,
    w_key_att,
    w_value_att,
    w_out_ret,
    w_out_att,
    retain_log,
    forget_total,
):
    rows = tokens.astype(jnp.float32)
    normed = (
        rows * lax.rsqrt(jnp.mean(rows * rows, axis=-1, keepdims=True) + EPS) * pre_gain
    ).astype(jnp.bfloat16)
    gathered = lax.all_gather(normed, "tp", axis=0, tiled=True)
    tok_dev = gathered.shape[0]
    offset = lax.axis_index("sp") * tok_dev
    query_places = offset + jnp.arange(tok_dev, dtype=jnp.int32)
    positions = query_places.astype(jnp.float32)

    def blocked(values):
        return values.reshape((tok_dev // SPAN, SPAN) + values.shape[1:])

    pieces = (
        lax.all_gather(w_query_ret, "sp", axis=0, tiled=True),
        lax.all_gather(w_key_ret, "sp", axis=0, tiled=True),
        lax.all_gather(w_value_ret, "sp", axis=0, tiled=True),
        lax.all_gather(w_query_att, "sp", axis=0, tiled=True),
        lax.all_gather(w_key_att, "sp", axis=0, tiled=True),
        lax.all_gather(w_value_att, "sp", axis=0, tiled=True),
    )
    projected = tuple(
        (jnp.dot(gathered, piece, preferred_element_type=jnp.float32) for piece in pieces)
    )
    heads = retain_log.shape[1]
    shape = (tok_dev, heads, HEAD)
    query = blocked(
        (rotate(projected[0].reshape(shape), positions) * HEAD ** (-0.5)).astype(jnp.bfloat16)
    )
    key_rows = blocked(rotate(projected[1].reshape(shape), positions).astype(jnp.bfloat16))
    value_rows = blocked(projected[2].astype(jnp.bfloat16).reshape(shape))
    within = jnp.cumsum(blocked(retain_log), axis=1)
    causal = jnp.arange(SPAN)[:, None] >= jnp.arange(SPAN)[None, :]
    scores = jnp.einsum("bthd,bshd->bhts", query, key_rows, preferred_element_type=jnp.float32)
    turned = jnp.transpose(within, (0, 2, 1))
    gap = jnp.where(causal, turned[:, :, :, None] - turned[:, :, None, :], 0.0)
    weights = jnp.where(causal, scores * jnp.exp(gap), 0.0).astype(jnp.bfloat16)
    local = jnp.einsum("bhts,bshd->bthd", weights, value_rows, preferred_element_type=jnp.float32)
    last = within[:, -1]
    faded = (key_rows.astype(jnp.float32) * jnp.exp(last[:, None, :] - within)[..., None]).astype(
        jnp.bfloat16
    )
    updates = jnp.einsum("bshd,bshe->bhde", faded, value_rows, preferred_element_type=jnp.float32)
    zero_state = jnp.zeros((heads, HEAD, HEAD), jnp.float32)
    final, _ = lax.scan(advance, zero_state, (last, updates))
    decay_total = jnp.sum(last, axis=0)
    own_state = final.reshape(heads, HEAD * HEAD)
    every_total = lax.all_gather(
        decay_total[None].astype(jnp.bfloat16), "sp", axis=0, tiled=True
    ).astype(jnp.float32)
    every_state = lax.all_gather(
        own_state[None].astype(jnp.bfloat16), "sp", axis=0, tiled=True
    ).astype(jnp.float32)
    device_order = jnp.arange(every_total.shape[0], dtype=jnp.int32)[:, None]
    earlier = device_order < lax.axis_index("sp")
    before = jnp.sum(jnp.where(earlier, every_total, 0.0), axis=0)
    through = jnp.cumsum(every_total, axis=0)
    fading = jnp.where(earlier, jnp.exp(jnp.where(earlier, before[None, :] - through, 0.0)), 0.0)
    incoming = jnp.einsum("jh,jhe->he", fading, every_state, precision=HIGH)
    _, befores = lax.scan(advance, incoming.reshape(heads, HEAD, HEAD), (last, updates))
    lifted = (query.astype(jnp.float32) * jnp.exp(within)[..., None]).astype(jnp.bfloat16)
    carried = jnp.einsum(
        "bthd,bhde->bthe", lifted, befores.astype(jnp.bfloat16), preferred_element_type=jnp.float32
    )
    retained = (
        head_norm((local + carried).reshape(shape))
        .astype(jnp.bfloat16)
        .reshape(tok_dev, heads * HEAD)
    )
    raw_key = projected[4]
    gate_heads = forget_total.shape[0]
    kv_local = raw_key.shape[1] // HEAD
    group = gate_heads // kv_local
    query = (
        (projected[3] * HEAD ** (-0.5)).astype(jnp.bfloat16).reshape(tok_dev, kv_local, group, HEAD)
    )
    key_rows = raw_key.astype(jnp.bfloat16)
    value_rows = projected[5].astype(jnp.bfloat16)
    gate_rows = lax.dynamic_slice_in_dim(forget_total, offset, tok_dev, 1).reshape(
        kv_local, group, tok_dev
    )
    last_row = offset + tok_dev - 1
    init = (
        jnp.zeros((kv_local, group, tok_dev, HEAD), jnp.float32),
        jnp.zeros((kv_local, group, tok_dev), jnp.float32),
    )
    key_piece = lax.all_gather(key_rows, "sp", axis=0, tiled=True)
    value_piece = lax.all_gather(value_rows, "sp", axis=0, tiled=True)
    count = key_piece.shape[0] // KEY_SPAN

    def one_block(index, inner):
        first = index * KEY_SPAN

        def compute(state):
            weighted, total = state
            key_block = lax.dynamic_slice_in_dim(key_piece, index * KEY_SPAN, KEY_SPAN, 0).reshape(
                KEY_SPAN, kv_local, HEAD
            )
            value_block = lax.dynamic_slice_in_dim(
                value_piece, index * KEY_SPAN, KEY_SPAN, 0
            ).reshape(KEY_SPAN, kv_local, HEAD)
            gate_keys = lax.dynamic_slice_in_dim(forget_total, first, KEY_SPAN, 1).reshape(
                kv_local, group, KEY_SPAN
            )
            scores = jnp.einsum(
                "tcgd,scd->cgts", query, key_block, preferred_element_type=jnp.float32
            )
            logits = scores + gate_rows[:, :, :, None] - gate_keys[:, :, None, :]
            allowed = (first + jnp.arange(KEY_SPAN, dtype=jnp.int32))[None, :] <= query_places[
                :, None
            ]
            weights = jnp.exp(jnp.where(allowed, logits, -jnp.inf))
            total = total + jnp.sum(weights, axis=-1)
            weighted = weighted + jnp.einsum(
                "cgts,scd->cgtd",
                weights.astype(jnp.bfloat16),
                value_block,
                preferred_element_type=jnp.float32,
            )
            return (weighted, total)

        def skipped(state):
            return state

        return lax.cond(first <= last_row, compute, skipped, inner)

    weighted, total = lax.fori_loop(0, count, one_block, init)
    result = weighted / total[..., None]
    attended = (
        jnp.transpose(result, (2, 0, 1, 3)).reshape(tok_dev, gate_heads * HEAD).astype(jnp.bfloat16)
    )
    out_ret, out_att = (
        lax.all_gather(w_out_ret, "sp", axis=1, tiled=True),
        lax.all_gather(w_out_att, "sp", axis=1, tiled=True),
    )
    return lax.psum_scatter(
        (
            jnp.dot(retained, out_ret, preferred_element_type=jnp.float32)
            + jnp.dot(attended, out_att, preferred_element_type=jnp.float32)
        ).astype(jnp.bfloat16),
        "tp",
        scatter_dimension=0,
        tiled=True,
    )


def choose(n, m, *arrays):
    tokens, w_key_ret, w_out_ret = arrays[0], arrays[3], arrays[8]
    whole_tiles = w_out_ret.shape[1] % LANES == 0 and w_key_ret.shape[0] % LANES == 0
    heads = arrays[10].shape[1]
    small = 16 * heads <= HEAD and arrays[7].shape[1] == HEAD and arrays[11].shape[0] == heads
    paired = n % 4 == 0 and n > 4 and m % 2 == 0 and m > 2
    if paired and whole_tiles and small and tokens.shape[0] * m == SPAN:
        return body(n, m, *arrays)
    return plain_body(*arrays)


def solution(mesh):
    return jax.shard_map(
        functools.partial(choose, mesh.shape["sp"], mesh.shape["tp"]),
        mesh=mesh,
        in_specs=(
            P(("sp", "tp"), None),
            P(),
            P("sp", "tp"),
            P("sp", "tp"),
            P("sp", "tp"),
            P("sp", "tp"),
            P("sp", "tp"),
            P("sp", "tp"),
            P("tp", "sp"),
            P("tp", "sp"),
            P("sp", "tp"),
            P("tp", None),
        ),
        out_specs=P(("sp", "tp"), None),
        check_vma=False,
    )
```

```python
import functools

import jax
import jax.numpy as jnp
import numpy as np
from jax import lax
from jax.experimental import pallas as pl
from jax.experimental.pallas import tpu as pltpu
from jax.sharding import PartitionSpec as P

HEAD = 64
EPS = 1e-06
THETA = 10000.0
F32 = jnp.float32
BF16 = jnp.bfloat16
MESH = pl.DeviceIdType.MESH
SPAN = 256
KEY_SPAN = 256
LANES = 128
CUTS = (2, 2, 1, 2)
LOG2E = float(np.log2(np.e))
TOKEN_CUT = 2
HIGH = lax.Precision.HIGHEST


def dot(a, b, dims=((1,), (0,))):
    return lax.dot_general(a, b, (dims, ((), ())), preferred_element_type=F32)


def kernel(
    n,
    m,
    heads,
    tok_hbm,
    gain_hbm,
    wq_ret_hbm,
    wk_ret_hbm,
    wv_ret_hbm,
    wq_att_hbm,
    wk_att_hbm,
    wv_att_hbm,
    wo_ret_hbm,
    wo_att_hbm,
    table_hbm,
    logs_hbm,
    gate_hbm,
    out_ref,
    tokens,
    table,
    lbuf,
    gbuf,
    xbuf,
    abuf,
    bbuf,
    cbuf,
    obuf,
    kvbuf,
    stbuf,
    state,
    num,
    qbuf,
    cbuf_gate,
    outbuf,
    rsbuf,
    gain,
    load,
    small_send,
    small_recv,
    x_send,
    x_fwd,
    x_pass,
    x_other,
    w_out,
    w_part,
    first_a,
    first_b,
    first_c,
    first_o,
    w_second,
    o_second,
    k_send,
    k_y,
    k_part,
    k_recv,
    r_send,
    r_recv,
):
    s, t = lax.axis_index("sp"), lax.axis_index("tp")
    nh, nx = n // 4, m // 2
    y, zl, zh = s % 2, (s // 2) % 2, s // 4
    c, x = t % 2, t // 2
    own = zl == c
    apart = zl != c

    def sp_of(zh_, zl_, y_):
        return zh_ * 4 + zl_ * 2 + y_

    def tp_of(x_, c_):
        return x_ * 2 + c_

    def device(zh_, zl_, y_, x_, c_):
        return {"sp": sp_of(zh_, zl_, y_), "tp": tp_of(x_, c_)}

    q, g = sp_of(zh, c, y), tp_of(x, zl)
    partner = device(zh, zl, y, x, 1 - c)
    across = device(zh, zl, 1 - y, x, c)
    rows = tokens.shape[0]
    tok = rows * m
    width = heads * HEAD
    half_o = wo_ret_hbm.shape[0]

    slot = jnp.where(own, s, n)
    piece = jnp.where(own, t, m)
    groups = (
        (tokens, ((tok_hbm, tokens),)),
        (gain, ((gain_hbm, gain),)),
        (abuf.at[slot], (
            (wk_att_hbm, abuf.at[slot, pl.ds(0, HEAD)]),
            (wv_att_hbm, abuf.at[slot, pl.ds(HEAD, HEAD)]),
            (wq_att_hbm, abuf.at[slot, pl.ds(2 * HEAD, width)]),
        )),
        (bbuf.at[slot], (
            (wk_ret_hbm, bbuf.at[slot, pl.ds(0, width)]),
            (wv_ret_hbm, bbuf.at[slot, pl.ds(width, width)]),
        )),
        (cbuf.at[slot], ((wq_ret_hbm, cbuf.at[slot]),)),
        (obuf.at[slot], (
            (wo_ret_hbm, obuf.at[slot, pl.ds(0, half_o)]),
            (wo_att_hbm, obuf.at[slot, pl.ds(half_o, wo_att_hbm.shape[0])]),
        )),
        (table, ((table_hbm.at[pl.ds(pl.multiple_of(q * tok, tok), tok)], table),)),
        (lbuf.at[0], ((logs_hbm, lbuf.at[0]),)),
        (gbuf.at[0], ((gate_hbm, gbuf.at[0]),)),
    )
    loads = []
    for k, (whole, copies) in enumerate(groups):
        for source, target in copies:
            pltpu.make_async_copy(source, target, load.at[k]).start()
        loads.append(pltpu.make_async_copy(whole, whole, load.at[k]))

    barrier = pltpu.get_barrier_semaphore()
    greeted = [
        device((zh + i) % nh, zl, 1 - y, x, (c + k) % 2) for i in range(nh) for k in range(2)
    ]
    for i in reversed(range(nh)):
        for j in reversed(range(2)):
            for k in range(2):
                if i or j or k:
                    greeted.append(device((zh + i) % nh, (zl + j) % 2, y, x, (c + k) % 2))
    for r in range(1, nx):
        for j in range(2):
            for k in range(2):
                greeted.append(device(zh, (zl + j) % 2, y, (x + r) % nx, (c + k) % 2))
    for other in greeted:
        pl.semaphore_signal(barrier, inc=1, device_id=other, device_id_type=MESH)

    started = []

    def guarded(condition, action):
        if condition is None:
            action()
        else:
            pl.when(condition)(action)

    def send(source, target, send_sem, recv_sem, where, condition=None, kept=True):
        copy = pltpu.make_async_remote_copy(
            src_ref=source, dst_ref=target, send_sem=send_sem, recv_sem=recv_sem,
            device_id=where, device_id_type=MESH,
        )
        guarded(condition, copy.start)
        if kept:
            started.append((copy, condition))

    def drain(source, send_sem, condition=None):
        started.append((
            pltpu.make_async_remote_copy(
                src_ref=source, dst_ref=source, send_sem=send_sem, recv_sem=send_sem,
                device_id=partner, device_id_type=MESH,
            ),
            condition,
        ))

    def receive(target, recv_sem, condition=None):
        copy = pltpu.make_async_remote_copy(
            src_ref=target, dst_ref=target, send_sem=recv_sem, recv_sem=recv_sem,
            device_id=partner, device_id_type=MESH,
        )
        guarded(condition, copy.wait_recv)

    for copy in loads[:2]:
        copy.wait()
    values = tokens[...].astype(F32)
    scale = lax.rsqrt(jnp.mean(values * values, axis=-1, keepdims=True) + EPS)
    xbuf[pl.ds(pl.multiple_of(piece * rows, rows), rows), :] = (
        values * scale * gain[...]
    ).astype(BF16)
    for copy in loads[2:]:
        copy.wait()
    pl.semaphore_wait(barrier, len(greeted))

    parts = (abuf, bbuf, cbuf, obuf)
    cuts = CUTS

    def chunk(p, index, k, u):
        length = parts[p].shape[1] // (2 * cuts[p])
        start = pl.multiple_of((k * cuts[p] + u) * length, length)
        return parts[p].at[index, pl.ds(start, length)]

    firsts = (first_a, first_b, first_c, first_o)

    def second(p, index):
        return o_second.at[index] if p == 3 else w_second.at[p]

    def halves(p, count):
        return parts[p].at[pl.ds(0, count), pl.ds(0, parts[p].shape[1] // 2)]

    def scatter_one(p, i, k, u, condition):
        core = (c + k) % 2
        send(
            chunk(p, slot, core, u), chunk(p, s, core, u), w_out.at[p], firsts[p].at[s, u],
            device((zh + i) % nh, c, y, x, core), condition, False,
        )

    def scatter_chip(p):
        for u in range(cuts[p]):
            scatter_one(p, 0, 1, u, own)

    def scatter_near(p, u):
        for k in range(2):
            scatter_one(p, 0, k, u, apart)

    def scatter_far(p, u, condition=None):
        for i in range(1, nh):
            for k in range(2):
                scatter_one(p, i, k, u, condition)

    middle = zl != zh % 2
    outer = zl == zh % 2

    def entry(p, i, j, u, condition=None):
        index = sp_of((zh + i) % nh, (zl + j) % 2, y)
        here = i == 0 and j == 0
        spot = chunk(p, index, c, u)
        receive(spot, firsts[p].at[index, u], apart if here else condition)
        send(spot, spot, w_out.at[p], firsts[p].at[index, u], across, condition, False)
        send(
            spot, spot, w_part.at[p], second(p, index), partner,
            own if here else condition, False,
        )

    def beside(p, i, j, u):
        index = sp_of((zh + i) % nh, (zl + j) % 2, 1 - y)
        spot = chunk(p, index, c, u)
        receive(spot, firsts[p].at[index, u])
        send(spot, spot, w_part.at[p], second(p, index), partner, None, False)

    def rest(p):
        receive(halves(p, n - 1), w_second.at[p], own)
        receive(halves(p, n), w_second.at[p], apart)

    far = [(i, j) for i in range(1, nh) for j in range(2)]
    near = (0, 1)
    pieces = x_pass.shape[1]

    def rows_of(index, u):
        length = rows // pieces
        return xbuf.at[pl.ds(pl.multiple_of((index * pieces + u) * length, length), length)]

    def pass_tokens(k, u):
        core = (c + k) % 2
        index = tp_of(x, core)
        spot = rows_of(index, u)
        receive(spot, x_pass.at[core, u], apart if k == 0 else None)
        for r in range(1, nx):
            send(
                spot, spot, x_fwd, x_other, device(zh, zl, y, (x + r) % nx, c), apart, False,
            )

    send(
        lbuf.at[0], lbuf.at[1], small_send.at[0], small_recv.at[0],
        device(zh, c, y, x, zl), apart,
    )
    send(gbuf.at[0], gbuf.at[1], small_send.at[1], small_recv.at[1], partner, own)
    for u in range(cuts[0]):
        scatter_far(0, u)
    scatter_chip(0)
    for u in range(pieces):
        ours, there = rows_of(piece, u), rows_of(t, u)
        send(ours, there, x_send, x_pass.at[c, u], device(zh, 1 - zl, y, x, zl), None, False)
        for r in range(1, nx):
            send(
                ours, there, x_send, x_other, device(zh, zl, y, (x + r) % nx, zl), None, False,
            )
        send(ours, there, x_send, x_pass.at[c, u], device(zh, zl, y, x, zl), apart, False)
    for u in range(cuts[0]):
        scatter_near(0, u)
    for p in range(1, 4):
        scatter_chip(p)
    for p in range(1, 3):
        for u in range(cuts[p]):
            scatter_far(p, u)
            scatter_near(p, u)
    for p in range(4):
        for u in range(cuts[p]):
            entry(p, 0, 0, u)
    lines = lax.broadcasted_iota(jnp.int32, (tok, tok), 0)
    lanes = lax.broadcasted_iota(jnp.int32, (tok, tok), 1)
    causal = lines >= lanes
    upto = jnp.where(lines <= lanes, 1.0, 0.0)
    receive(lbuf.at[1], small_recv.at[0], apart)
    receive(gbuf.at[1], small_recv.at[1], apart)
    pick = jnp.where(own, 0, 1)
    logs = jnp.concatenate([lbuf[pick], jnp.zeros((8 - heads, tok), F32)], axis=0)
    turned = lax.dot_general(
        logs, upto, (((1,), (0,)), ((), ())),
        preferred_element_type=F32, precision=lax.Precision.HIGHEST,
    )
    fill = jnp.zeros((LANES - 8, tok), F32)
    within = jnp.concatenate([turned, fill], axis=0).T
    gates_own = gbuf[pick, :, pl.ds(pl.multiple_of(q * tok, tok), tok)]
    gate_col = jnp.concatenate(
        [gates_own, jnp.zeros((LANES - heads, tok), F32)], axis=0
    ).T
    cosine, sine = table[:, : HEAD // 2], table[:, HEAD // 2 :]

    for u in range(cuts[0]):
        beside(0, 0, 0, u)
    for a in far:
        entry(0, *a, 0)
    for k in range(2):
        pass_tokens(k, 0)
    for u in range(cuts[1]):
        beside(1, 0, 0, u)
    for u in range(1, cuts[0]):
        for a in far:
            entry(0, *a, u)
    for a in far:
        beside(0, *a, 0)
    for u in range(1, pieces):
        for k in range(2):
            pass_tokens(k, u)
    for u in range(cuts[0]):
        entry(0, *near, u)
    for a in far:
        entry(1, *a, 0, middle)
    for u in range(1, cuts[0]):
        for a in far:
            beside(0, *a, u)
    for p in range(2, 4):
        for u in range(cuts[p]):
            beside(p, 0, 0, u)
    for u in range(cuts[0]):
        beside(0, *near, u)
    for a in far:
        entry(1, *a, 0, outer)

    receive(xbuf.at[pl.ds(0, (m - 2) * rows)], x_other)
    rest(0)

    def exchange(buf, e, index, sem, where, condition):
        send(buf.at[index], buf.at[index], sem, k_recv.at[e, index], where, condition)

    def arrive(buf, e, index, condition):
        receive(buf.at[index], k_recv.at[e, index], condition)

    def exchange_send(buf, e):
        for i in range(1, nh):
            exchange(
                buf, e, q, k_send.at[e, i - 1], device((zh + i) % nh, zl, y, x, c), zh + i < nh
            )
        exchange(buf, e, q, k_y.at[e, 0], across, c + y < 2)
        exchange(buf, e, q, k_part.at[e, 0, 0], partner, c == 0)

    def exchange_across(buf, e):
        index = sp_of(zh, c, 1 - y)
        arrive(buf, e, index, c <= y)
        exchange(buf, e, index, k_part.at[e, 0, 1], partner, c == 0)

    def exchange_part(buf, e):
        for k in range(2):
            arrive(buf, e, sp_of(zh, 1 - c, (y + k) % 2), c == 1)

    def exchange_far(buf, e):
        for i in range(1, nh):
            index = sp_of((zh + nh - i) % nh, c, y)
            arrive(buf, e, index, zh >= i)
            exchange(buf, e, index, k_y.at[e, i], across, zh >= i)
            exchange(buf, e, index, k_part.at[e, i, 0], partner, zh >= i)

    def exchange_far_across(buf, e):
        for i in range(1, nh):
            index = sp_of((zh + nh - i) % nh, c, 1 - y)
            arrive(buf, e, index, zh >= i)
            exchange(buf, e, index, k_part.at[e, i, 1], partner, zh >= i)

    def exchange_far_part(buf, e):
        for i in range(1, nh):
            for k in range(2):
                arrive(buf, e, sp_of((zh + nh - i) % nh, 1 - c, (y + k) % 2), zh >= i)

    def rope(field):
        first, second = field[:, : HEAD // 2], field[:, HEAD // 2 :]
        return jnp.concatenate(
            [first * cosine - second * sine, first * sine + second * cosine], axis=-1
        )

    def project(buf):
        deep = buf.shape[2]
        return sum(
            dot(xbuf[:tok, k * deep : (k + 1) * deep], buf[k], ((1,), (1,))) for k in range(n)
        )

    proj = project(abuf)
    kvbuf[q] = proj[:, : 2 * HEAD].astype(BF16)
    exchange_send(kvbuf, 0)
    scatter_far(3, 0)
    scatter_near(3, 0)
    for u in range(1, cuts[3]):
        scatter_far(3, u, zh == nh - 1)
        scatter_near(3, u)
    wide = heads * tok
    zeros = jnp.zeros((tok, HEAD), F32)
    for h in range(heads):
        query = proj[:, (2 + h) * HEAD : (3 + h) * HEAD] * (HEAD ** (-0.5) * LOG2E)
        qbuf[h * tok : (h + 1) * tok, :] = jnp.concatenate([query, zeros], axis=1).astype(BF16)
        cbuf_gate[h * tok : (h + 1) * tok, :] = jnp.broadcast_to(
            gate_col[:, h : h + 1] * LOG2E, (tok, LANES)
        )
    low_lanes = lax.broadcasted_iota(jnp.int32, (tok, 2 * HEAD), 1) < HEAD

    def attend(indices, masked=False):
        total = None if masked else num[...]
        for index in indices:
            block = kvbuf[index]
            values = jnp.where(low_lanes, jnp.ones_like(block), block)
            gates = gbuf[pick, :, pl.ds(pl.multiple_of(index * tok, tok), tok)] * LOG2E
            logits = dot(qbuf[...], block, ((1,), (1,)))
            column = cbuf_gate[...]
            column = jnp.concatenate([column] * (tok // LANES), axis=1)
            pieces_ = []
            for h in range(heads):
                part = slice(h * tok, (h + 1) * tok)
                shifted = logits[part] + column[part] - gates[h : h + 1, :]
                if masked:
                    shifted = jnp.where(causal, shifted, -jnp.inf)
                pieces_.append(jnp.exp2(shifted).astype(BF16))
            term = dot(jnp.concatenate(pieces_, axis=0), values)
            total = term if total is None else total + term
        num[...] = total

    for u in range(1, cuts[1]):
        for a in far:
            entry(1, *a, u)
    attend([q], True)
    for a in far:
        beside(1, *a, 0)
    for u in range(cuts[1]):
        entry(1, *near, u)
    exchange_across(kvbuf, 0)
    exchange_part(kvbuf, 0)
    index = sp_of(zh, 0, 0)
    pl.when(index < q)(functools.partial(attend, [index]))
    exchange_far(kvbuf, 0)
    pl.when(index + 1 < q)(functools.partial(attend, [index + 1]))
    for u in range(1, cuts[1]):
        for a in far:
            beside(1, *a, u)
    for u in range(cuts[2]):
        for a in far:
            entry(2, *a, u)
    pl.when(index + 2 < q)(functools.partial(attend, [index + 2]))
    for u in range(cuts[1]):
        beside(1, *near, u)
    for u in range(cuts[2]):
        entry(2, *near, u)
    exchange_far_across(kvbuf, 0)
    for a in far:
        entry(3, *a, 0)
    rest(1)

    proj = project(bbuf)
    keys, vals, updates, marks = [], [], [], []
    for h in range(heads):
        base = h * HEAD
        key = rope(proj[:, base : base + HEAD]).astype(BF16)
        val = proj[:, base + width : base + width + HEAD].astype(BF16)
        column = within[:, h : h + 1]
        last = column[tok - 1 :, :]
        faded = (key.astype(F32) * jnp.exp(last - column)).astype(BF16)
        updates.append(dot(faded, val, ((0,), (0,))))
        high = last.astype(BF16).astype(F32)
        low = last - high
        marks.append(jnp.broadcast_to(high, (8, HEAD)))
        marks.append(jnp.broadcast_to(low, (8, HEAD)))
        keys.append(key)
        vals.append(val)
    marks.append(jnp.zeros((HEAD - 16 * heads, HEAD), F32))
    blocks = updates + [jnp.concatenate(marks, axis=0)]
    if len(blocks) % 2:
        blocks.append(jnp.zeros((HEAD, HEAD), F32))
    for k in range(0, len(blocks), 2):
        both = jnp.concatenate(blocks[k : k + 2], axis=1).astype(BF16)
        stbuf[q, k // 2 * HEAD : (k // 2 + 1) * HEAD, :] = both

    def piece_of(index, k):
        spot = slice(k % 2 * HEAD, (k % 2 + 1) * HEAD)
        return stbuf[index, k // 2 * HEAD : (k // 2 + 1) * HEAD, spot].astype(F32)

    exchange_send(stbuf, 1)
    for u in range(1, cuts[3]):
        scatter_far(3, u, zh < nh - 1)
    for u in range(cuts[2]):
        for a in far:
            beside(2, *a, u)
        beside(2, *near, u)
    entry(3, *near, 0)
    rest(2)

    exchange_far(stbuf, 1)
    proj = project(cbuf)
    local, lifts = [], []
    for h in range(heads):
        query = (rope(proj[:, h * HEAD : (h + 1) * HEAD]) * HEAD ** (-0.5)).astype(BF16)
        column = within[:, h : h + 1]
        gap = jnp.where(causal, column - turned[h : h + 1, :], 0.0)
        scores = dot(query, keys[h], ((1,), (1,)))
        weights = jnp.where(causal, scores * jnp.exp(gap), 0.0).astype(BF16)
        local.append(dot(weights, vals[h]))
        lifts.append((query.astype(F32) * jnp.exp(column)).astype(BF16))
    exchange_far_part(kvbuf, 0)
    exchange_across(stbuf, 1)
    steps = [(beside, near, 0)]
    steps += [(entry, a, u) for u in range(1, cuts[3]) for a in far]
    steps += [(entry, near, u) for u in range(1, cuts[3])]
    for i in range(1, nh):
        index = sp_of((zh + nh - i) % nh, 0, 0)
        for half in range(2):
            pl.when(zh >= i)(
                functools.partial(attend, [index + 2 * half, index + 2 * half + 1])
            )
            for call, a, u in steps[:1]:
                call(3, *a, u)
            steps = steps[1:]
    for call, a, u in steps:
        call(3, *a, u)
    exchange_far_across(stbuf, 1)
    exchange_part(stbuf, 1)
    exchange_far_part(stbuf, 1)
    state[...] = jnp.zeros_like(state)
    for j in range(n - 1):
        def earlier(j=j):
            marked = piece_of(j, heads)
            for h in range(heads):
                total = marked[16 * h : 16 * h + 1] + marked[16 * h + 8 : 16 * h + 9]
                state[h] = jnp.exp(total) * state[h] + piece_of(j, h)

        pl.when(q > j)(earlier)
    retained, attended = [], []
    for h in range(heads):
        raw = local[h] + dot(lifts[h], state[h].astype(BF16))
        centre = jnp.mean(raw, axis=-1, keepdims=True)
        spread = jnp.mean(jnp.square(raw - centre), axis=-1, keepdims=True)
        retained.append(((raw - centre) * lax.rsqrt(spread + EPS)).astype(BF16))
        both = num[h * tok : (h + 1) * tok, :]
        attended.append((both[:, HEAD:] / both[:, :HEAD]).astype(BF16))
    mixed = jnp.concatenate(retained + attended, axis=-1)
    order = [(i, j) for i in range(nh) for j in range(2)]

    def produce(i, j, l):
        index = sp_of((zh + i) % nh, (zl + j) % 2, (y + l) % 2)
        receive(
            halves(3, 1), o_second.at[index], apart if i == 0 and j == 0 and l == 0 else None
        )
        outbuf[index] = dot(mixed, obuf[index]).astype(BF16)
        for r in reversed(range(nx)):
            for k in range(2):
                where = tp_of((x + r) % nx, (c + k) % 2)
                rows_there = pl.ds(pl.multiple_of(where * rows, rows), rows)
                send(
                    outbuf.at[index, rows_there], rsbuf.at[index, g], r_send, r_recv.at[index],
                    device(zh, c, y, (x + r) % nx, (c + k) % 2),
                    apart if r == 0 and k == 0 else None, False,
                )

    for i, j in order:
        produce(i, j, 0)
    for u in range(1, cuts[3]):
        beside(3, *near, u)
    for u in range(cuts[3]):
        for a in far:
            beside(3, *a, u)
    for i, j in order:
        produce(i, j, 1)
    columns = obuf.shape[2]
    for l in range(2):
        for i, j in order:
            index = sp_of((zh + i) % nh, (zl + j) % 2, (y + l) % 2)

            def keep(index=index):
                rsbuf[index, g] = outbuf[index, pl.ds(pl.multiple_of(t * rows, rows), rows)]

            receive(rsbuf.at[index, pl.ds(0, m - 1)], r_recv.at[index], own)
            pl.when(own)(keep)
            receive(rsbuf.at[index], r_recv.at[index], apart)
            total = rsbuf[index, 0].astype(F32)
            for other in range(1, m):
                total = total + rsbuf[index, other].astype(F32)
            span = pl.ds(pl.multiple_of(index * columns, columns), columns)
            out_ref[:, span] = total.astype(BF16)
    for p in range(4):
        drain(halves(p, n - 1), w_out.at[p], own)
        drain(halves(p, n), w_out.at[p], apart)
        drain(halves(p, n), w_part.at[p], own)
        drain(halves(p, n - 1), w_part.at[p], apart)
    drain(xbuf.at[pl.ds(0, nx * rows)], x_send, own)
    drain(xbuf.at[pl.ds(0, (nx + 1) * rows)], x_send, apart)
    drain(xbuf.at[pl.ds(0, (m - 2) * rows)], x_fwd, apart)
    drain(rsbuf.at[:, pl.ds(0, m - 1)], r_send, own)
    drain(rsbuf, r_send, apart)
    for copy, condition in started:
        guarded(condition, copy.wait_send)


def body(
    n,
    m,
    tokens,
    pre_gain,
    w_query_ret,
    w_key_ret,
    w_value_ret,
    w_query_att,
    w_key_att,
    w_value_att,
    w_out_ret,
    w_out_att,
    retain_log,
    forget_total,
):
    rows, depth = tokens.shape
    tok = rows * m
    heads = retain_log.shape[1]
    nh, nx = n // 4, m // 2
    half = HEAD // 2
    inverse = np.float32(THETA) ** (-np.arange(half, dtype=np.float32) / np.float32(half))
    angles = np.arange(n * tok, dtype=np.float32)[:, None] * inverse[None, :]
    table = np.concatenate([np.cos(angles), np.sin(angles)], axis=1).astype(np.float32)
    wide_a = 2 * HEAD + heads * HEAD
    wide_b, wide_c = 2 * heads * HEAD, heads * HEAD
    deep = w_key_ret.shape[0]
    deep_o = w_out_ret.shape[0] + w_out_att.shape[0]
    tall = (heads // 2 + 1) * HEAD
    hbm = pl.BlockSpec(memory_space=pl.ANY)
    vmem = pl.BlockSpec(memory_space=pltpu.VMEM)
    dma = pltpu.SemaphoreType.DMA
    return pl.pallas_call(
        functools.partial(kernel, n, m, heads),
        out_shape=jax.ShapeDtypeStruct((rows, depth), BF16),
        in_specs=[hbm] * 13,
        out_specs=vmem,
        scratch_shapes=[
            pltpu.VMEM(tokens.shape, BF16),
            pltpu.VMEM((tok, HEAD), F32),
            pltpu.VMEM((2,) + retain_log.shape[::-1], F32),
            pltpu.VMEM((2,) + forget_total.shape, F32),
            pltpu.VMEM((tok + rows, depth), BF16),
            pltpu.VMEM((n + 1, wide_a, deep), BF16),
            pltpu.VMEM((n + 1, wide_b, deep), BF16),
            pltpu.VMEM((n + 1, wide_c, deep), BF16),
            pltpu.VMEM((n + 1, deep_o, w_out_ret.shape[1]), BF16),
            pltpu.VMEM((n, tok, 2 * HEAD), BF16),
            pltpu.VMEM((n, tall, 2 * HEAD), BF16),
            pltpu.VMEM((heads, HEAD, HEAD), F32),
            pltpu.VMEM((heads * tok, 2 * HEAD), F32),
            pltpu.VMEM((heads * tok, 2 * HEAD), BF16),
            pltpu.VMEM((heads * tok, LANES), F32),
            pltpu.VMEM((n, tok, w_out_ret.shape[1]), BF16),
            pltpu.VMEM((n, m, rows, w_out_ret.shape[1]), BF16),
            pltpu.VMEM((1, depth), F32),
            dma((9,)),
            dma((2,)),
            dma((2,)),
            dma,
            dma,
            dma((2, TOKEN_CUT)),
            dma,
            dma((len(CUTS),)),
            dma((len(CUTS),)),
            *[dma((n, count)) for count in CUTS],
            dma((len(CUTS) - 1,)),
            dma((n,)),
            dma((2, nh - 1)),
            dma((2, nh)),
            dma((2, nh, 2)),
            dma((2, n)),
            dma,
            dma((n,)),
        ],
        compiler_params=pltpu.CompilerParams(
            collective_id=0, has_side_effects=True, vmem_limit_bytes=60 * 1024 * 1024
        ),
    )(
        tokens,
        pre_gain[None, :],
        w_query_ret.T,
        w_key_ret.T,
        w_value_ret.T,
        w_query_att.T,
        w_key_att.T,
        w_value_att.T,
        w_out_ret,
        w_out_att,
        jnp.asarray(table),
        retain_log.T,
        forget_total,
    )


def rotate(field, positions):
    half = field.shape[-1] // 2
    inverse = THETA ** (-jnp.arange(half, dtype=jnp.float32) / half)
    angles = positions[:, None] * inverse[None, :]
    cosine = jnp.cos(angles)[:, None, :]
    sine = jnp.sin(angles)[:, None, :]
    first_half = field[..., :half]
    second_half = field[..., half:]
    return jnp.concatenate(
        [first_half * cosine - second_half * sine, first_half * sine + second_half * cosine],
        axis=-1,
    )


def head_norm(values):
    centre = jnp.mean(values, axis=-1, keepdims=True)
    spread = jnp.mean(jnp.square(values - centre), axis=-1, keepdims=True)
    return (values - centre) * lax.rsqrt(spread + EPS)


def advance(state, pair):
    decay, update = pair
    return (jnp.exp(decay)[:, None, None] * state + update, state)


def plain_body(
    tokens,
    pre_gain,
    w_query_ret,
    w_key_ret,
    w_value_ret,
    w_query_att,
    w_key_att,
    w_value_att,
    w_out_ret,
    w_out_att,
    retain_log,
    forget_total,
):
    rows = tokens.astype(jnp.float32)
    normed = (
        rows * lax.rsqrt(jnp.mean(rows * rows, axis=-1, keepdims=True) + EPS) * pre_gain
    ).astype(jnp.bfloat16)
    gathered = lax.all_gather(normed, "tp", axis=0, tiled=True)
    tok_dev = gathered.shape[0]
    offset = lax.axis_index("sp") * tok_dev
    query_places = offset + jnp.arange(tok_dev, dtype=jnp.int32)
    positions = query_places.astype(jnp.float32)

    def blocked(values):
        return values.reshape((tok_dev // SPAN, SPAN) + values.shape[1:])

    pieces = (
        lax.all_gather(w_query_ret, "sp", axis=0, tiled=True),
        lax.all_gather(w_key_ret, "sp", axis=0, tiled=True),
        lax.all_gather(w_value_ret, "sp", axis=0, tiled=True),
        lax.all_gather(w_query_att, "sp", axis=0, tiled=True),
        lax.all_gather(w_key_att, "sp", axis=0, tiled=True),
        lax.all_gather(w_value_att, "sp", axis=0, tiled=True),
    )
    projected = tuple(
        (jnp.dot(gathered, piece, preferred_element_type=jnp.float32) for piece in pieces)
    )
    heads = retain_log.shape[1]
    shape = (tok_dev, heads, HEAD)
    query = blocked(
        (rotate(projected[0].reshape(shape), positions) * HEAD ** (-0.5)).astype(jnp.bfloat16)
    )
    key_rows = blocked(rotate(projected[1].reshape(shape), positions).astype(jnp.bfloat16))
    value_rows = blocked(projected[2].astype(jnp.bfloat16).reshape(shape))
    within = jnp.cumsum(blocked(retain_log), axis=1)
    causal = jnp.arange(SPAN)[:, None] >= jnp.arange(SPAN)[None, :]
    scores = jnp.einsum("bthd,bshd->bhts", query, key_rows, preferred_element_type=jnp.float32)
    turned = jnp.transpose(within, (0, 2, 1))
    gap = jnp.where(causal, turned[:, :, :, None] - turned[:, :, None, :], 0.0)
    weights = jnp.where(causal, scores * jnp.exp(gap), 0.0).astype(jnp.bfloat16)
    local = jnp.einsum("bhts,bshd->bthd", weights, value_rows, preferred_element_type=jnp.float32)
    last = within[:, -1]
    faded = (key_rows.astype(jnp.float32) * jnp.exp(last[:, None, :] - within)[..., None]).astype(
        jnp.bfloat16
    )
    updates = jnp.einsum("bshd,bshe->bhde", faded, value_rows, preferred_element_type=jnp.float32)
    zero_state = jnp.zeros((heads, HEAD, HEAD), jnp.float32)
    final, _ = lax.scan(advance, zero_state, (last, updates))
    decay_total = jnp.sum(last, axis=0)
    own_state = final.reshape(heads, HEAD * HEAD)
    every_total = lax.all_gather(
        decay_total[None].astype(jnp.bfloat16), "sp", axis=0, tiled=True
    ).astype(jnp.float32)
    every_state = lax.all_gather(
        own_state[None].astype(jnp.bfloat16), "sp", axis=0, tiled=True
    ).astype(jnp.float32)
    device_order = jnp.arange(every_total.shape[0], dtype=jnp.int32)[:, None]
    earlier = device_order < lax.axis_index("sp")
    before = jnp.sum(jnp.where(earlier, every_total, 0.0), axis=0)
    through = jnp.cumsum(every_total, axis=0)
    fading = jnp.where(earlier, jnp.exp(jnp.where(earlier, before[None, :] - through, 0.0)), 0.0)
    incoming = jnp.einsum("jh,jhe->he", fading, every_state, precision=HIGH)
    _, befores = lax.scan(advance, incoming.reshape(heads, HEAD, HEAD), (last, updates))
    lifted = (query.astype(jnp.float32) * jnp.exp(within)[..., None]).astype(jnp.bfloat16)
    carried = jnp.einsum(
        "bthd,bhde->bthe", lifted, befores.astype(jnp.bfloat16), preferred_element_type=jnp.float32
    )
    retained = (
        head_norm((local + carried).reshape(shape))
        .astype(jnp.bfloat16)
        .reshape(tok_dev, heads * HEAD)
    )
    raw_key = projected[4]
    gate_heads = forget_total.shape[0]
    kv_local = raw_key.shape[1] // HEAD
    group = gate_heads // kv_local
    query = (
        (projected[3] * HEAD ** (-0.5)).astype(jnp.bfloat16).reshape(tok_dev, kv_local, group, HEAD)
    )
    key_rows = raw_key.astype(jnp.bfloat16)
    value_rows = projected[5].astype(jnp.bfloat16)
    gate_rows = lax.dynamic_slice_in_dim(forget_total, offset, tok_dev, 1).reshape(
        kv_local, group, tok_dev
    )
    last_row = offset + tok_dev - 1
    init = (
        jnp.zeros((kv_local, group, tok_dev, HEAD), jnp.float32),
        jnp.zeros((kv_local, group, tok_dev), jnp.float32),
    )
    key_piece = lax.all_gather(key_rows, "sp", axis=0, tiled=True)
    value_piece = lax.all_gather(value_rows, "sp", axis=0, tiled=True)
    count = key_piece.shape[0] // KEY_SPAN

    def one_block(index, inner):
        first = index * KEY_SPAN

        def compute(state):
            weighted, total = state
            key_block = lax.dynamic_slice_in_dim(key_piece, index * KEY_SPAN, KEY_SPAN, 0).reshape(
                KEY_SPAN, kv_local, HEAD
            )
            value_block = lax.dynamic_slice_in_dim(
                value_piece, index * KEY_SPAN, KEY_SPAN, 0
            ).reshape(KEY_SPAN, kv_local, HEAD)
            gate_keys = lax.dynamic_slice_in_dim(forget_total, first, KEY_SPAN, 1).reshape(
                kv_local, group, KEY_SPAN
            )
            scores = jnp.einsum(
                "tcgd,scd->cgts", query, key_block, preferred_element_type=jnp.float32
            )
            logits = scores + gate_rows[:, :, :, None] - gate_keys[:, :, None, :]
            allowed = (first + jnp.arange(KEY_SPAN, dtype=jnp.int32))[None, :] <= query_places[
                :, None
            ]
            weights = jnp.exp(jnp.where(allowed, logits, -jnp.inf))
            total = total + jnp.sum(weights, axis=-1)
            weighted = weighted + jnp.einsum(
                "cgts,scd->cgtd",
                weights.astype(jnp.bfloat16),
                value_block,
                preferred_element_type=jnp.float32,
            )
            return (weighted, total)

        def skipped(state):
            return state

        return lax.cond(first <= last_row, compute, skipped, inner)

    weighted, total = lax.fori_loop(0, count, one_block, init)
    result = weighted / total[..., None]
    attended = (
        jnp.transpose(result, (2, 0, 1, 3)).reshape(tok_dev, gate_heads * HEAD).astype(jnp.bfloat16)
    )
    out_ret, out_att = (
        lax.all_gather(w_out_ret, "sp", axis=1, tiled=True),
        lax.all_gather(w_out_att, "sp", axis=1, tiled=True),
    )
    return lax.psum_scatter(
        (
            jnp.dot(retained, out_ret, preferred_element_type=jnp.float32)
            + jnp.dot(attended, out_att, preferred_element_type=jnp.float32)
        ).astype(jnp.bfloat16),
        "tp",
        scatter_dimension=0,
        tiled=True,
    )


def choose(n, m, *arrays):
    tokens, w_key_ret, w_out_ret = arrays[0], arrays[3], arrays[8]
    whole_tiles = w_out_ret.shape[1] % LANES == 0 and w_key_ret.shape[0] % LANES == 0
    heads = arrays[10].shape[1]
    small = 16 * heads <= HEAD and arrays[7].shape[1] == HEAD and arrays[11].shape[0] == heads
    paired = n % 4 == 0 and n > 4 and m % 2 == 0 and m > 2
    if paired and whole_tiles and small and tokens.shape[0] * m == SPAN:
        return body(n, m, *arrays)
    return plain_body(*arrays)


def solution(mesh):
    return jax.shard_map(
        functools.partial(choose, mesh.shape["sp"], mesh.shape["tp"]),
        mesh=mesh,
        in_specs=(
            P(("sp", "tp"), None),
            P(),
            P("sp", "tp"),
            P("sp", "tp"),
            P("sp", "tp"),
            P("sp", "tp"),
            P("sp", "tp"),
            P("sp", "tp"),
            P("tp", "sp"),
            P("tp", "sp"),
            P("sp", "tp"),
            P("tp", None),
        ),
        out_specs=P(("sp", "tp"), None),
        check_vma=False,
    )
```

```python
import functools

import jax
import jax.numpy as jnp
import numpy as np
from jax import lax
from jax.experimental import pallas as pl
from jax.experimental.pallas import tpu as pltpu
from jax.sharding import PartitionSpec as P

HEAD = 64
EPS = 1e-06
THETA = 10000.0
F32 = jnp.float32
BF16 = jnp.bfloat16
MESH = pl.DeviceIdType.MESH
SPAN = 256
KEY_SPAN = 256
LANES = 128
CUTS = (2, 2, 1, 3)
LOG2E = float(np.log2(np.e))
TOKEN_CUT = 4
HIGH = lax.Precision.HIGHEST


def dot(a, b, dims=((1,), (0,))):
    return lax.dot_general(a, b, (dims, ((), ())), preferred_element_type=F32)


def kernel(
    n,
    m,
    heads,
    tok_hbm,
    gain_hbm,
    wq_ret_hbm,
    wk_ret_hbm,
    wv_ret_hbm,
    wq_att_hbm,
    wk_att_hbm,
    wv_att_hbm,
    wo_ret_hbm,
    wo_att_hbm,
    table_hbm,
    logs_hbm,
    gate_hbm,
    out_ref,
    tokens,
    table,
    lbuf,
    gbuf,
    xbuf,
    abuf,
    bbuf,
    cbuf,
    obuf,
    kvbuf,
    stbuf,
    state,
    num,
    qbuf,
    cbuf_gate,
    outbuf,
    rsbuf,
    gain,
    load,
    small_send,
    small_recv,
    x_send,
    x_fwd,
    x_pass,
    x_other,
    w_out,
    w_part,
    first_a,
    first_b,
    first_c,
    first_o,
    w_second,
    o_second,
    k_send,
    k_y,
    k_part,
    k_recv,
    r_send,
    r_recv,
):
    s, t = lax.axis_index("sp"), lax.axis_index("tp")
    nh, nx = n // 4, m // 2
    y, zl, zh = s % 2, (s // 2) % 2, s // 4
    c, x = t % 2, t // 2
    own = zl == c
    apart = zl != c

    def sp_of(zh_, zl_, y_):
        return zh_ * 4 + zl_ * 2 + y_

    def tp_of(x_, c_):
        return x_ * 2 + c_

    def device(zh_, zl_, y_, x_, c_):
        return {"sp": sp_of(zh_, zl_, y_), "tp": tp_of(x_, c_)}

    q, g = sp_of(zh, c, y), tp_of(x, zl)
    partner = device(zh, zl, y, x, 1 - c)
    across = device(zh, zl, 1 - y, x, c)
    rows = tokens.shape[0]
    tok = rows * m
    width = heads * HEAD
    half_o = wo_ret_hbm.shape[0]

    slot = jnp.where(own, s, n)
    piece = jnp.where(own, t, m)
    groups = (
        (tokens, ((tok_hbm, tokens),)),
        (gain, ((gain_hbm, gain),)),
        (abuf.at[slot], (
            (wk_att_hbm, abuf.at[slot, pl.ds(0, HEAD)]),
            (wv_att_hbm, abuf.at[slot, pl.ds(HEAD, HEAD)]),
            (wq_att_hbm, abuf.at[slot, pl.ds(2 * HEAD, width)]),
        )),
        (bbuf.at[slot], (
            (wk_ret_hbm, bbuf.at[slot, pl.ds(0, width)]),
            (wv_ret_hbm, bbuf.at[slot, pl.ds(width, width)]),
        )),
        (cbuf.at[slot], ((wq_ret_hbm, cbuf.at[slot]),)),
        (obuf.at[slot], (
            (wo_ret_hbm, obuf.at[slot, pl.ds(0, half_o)]),
            (wo_att_hbm, obuf.at[slot, pl.ds(half_o, wo_att_hbm.shape[0])]),
        )),
        (table, ((table_hbm.at[pl.ds(pl.multiple_of(q * tok, tok), tok)], table),)),
        (lbuf.at[0], ((logs_hbm, lbuf.at[0]),)),
        (gbuf.at[0], ((gate_hbm, gbuf.at[0]),)),
    )
    loads = []
    for k, (whole, copies) in enumerate(groups):
        for source, target in copies:
            pltpu.make_async_copy(source, target, load.at[k]).start()
        loads.append(pltpu.make_async_copy(whole, whole, load.at[k]))

    barrier = pltpu.get_barrier_semaphore()
    greeted = [
        device((zh + i) % nh, zl, 1 - y, x, (c + k) % 2) for i in range(nh) for k in range(2)
    ]
    for i in reversed(range(nh)):
        for j in reversed(range(2)):
            for k in range(2):
                if i or j or k:
                    greeted.append(device((zh + i) % nh, (zl + j) % 2, y, x, (c + k) % 2))
    for r in range(1, nx):
        for j in range(2):
            for k in range(2):
                greeted.append(device(zh, (zl + j) % 2, y, (x + r) % nx, (c + k) % 2))
    for other in greeted:
        pl.semaphore_signal(barrier, inc=1, device_id=other, device_id_type=MESH)

    started = []

    def guarded(condition, action):
        if condition is None:
            action()
        else:
            pl.when(condition)(action)

    def send(source, target, send_sem, recv_sem, where, condition=None, kept=True):
        copy = pltpu.make_async_remote_copy(
            src_ref=source, dst_ref=target, send_sem=send_sem, recv_sem=recv_sem,
            device_id=where, device_id_type=MESH,
        )
        guarded(condition, copy.start)
        if kept:
            started.append((copy, condition))

    def drain(source, send_sem, condition=None):
        started.append((
            pltpu.make_async_remote_copy(
                src_ref=source, dst_ref=source, send_sem=send_sem, recv_sem=send_sem,
                device_id=partner, device_id_type=MESH,
            ),
            condition,
        ))

    def receive(target, recv_sem, condition=None):
        copy = pltpu.make_async_remote_copy(
            src_ref=target, dst_ref=target, send_sem=recv_sem, recv_sem=recv_sem,
            device_id=partner, device_id_type=MESH,
        )
        guarded(condition, copy.wait_recv)

    for copy in loads[:2]:
        copy.wait()
    values = tokens[...].astype(F32)
    scale = lax.rsqrt(jnp.mean(values * values, axis=-1, keepdims=True) + EPS)
    xbuf[pl.ds(pl.multiple_of(piece * rows, rows), rows), :] = (
        values * scale * gain[...]
    ).astype(BF16)
    for copy in loads[2:]:
        copy.wait()
    pl.semaphore_wait(barrier, len(greeted))

    parts = (abuf, bbuf, cbuf, obuf)
    cuts = CUTS

    def chunk(p, index, k, u):
        length = parts[p].shape[1] // (2 * cuts[p])
        start = pl.multiple_of((k * cuts[p] + u) * length, length)
        return parts[p].at[index, pl.ds(start, length)]

    firsts = (first_a, first_b, first_c, first_o)

    def second(p, index):
        return o_second.at[index] if p == 3 else w_second.at[p]

    def halves(p, count):
        return parts[p].at[pl.ds(0, count), pl.ds(0, parts[p].shape[1] // 2)]

    def scatter_one(p, i, k, u, condition):
        core = (c + k) % 2
        send(
            chunk(p, slot, core, u), chunk(p, s, core, u), w_out.at[p], firsts[p].at[s, u],
            device((zh + i) % nh, c, y, x, core), condition, False,
        )

    def scatter_chip(p):
        for u in range(cuts[p]):
            scatter_one(p, 0, 1, u, own)

    def scatter_near(p, u):
        for k in range(2):
            scatter_one(p, 0, k, u, apart)

    def scatter_far(p, u, condition=None):
        for i in range(1, nh):
            for k in range(2):
                scatter_one(p, i, k, u, condition)

    middle = zl != zh % 2
    outer = zl == zh % 2

    def entry(p, i, j, u, condition=None):
        index = sp_of((zh + i) % nh, (zl + j) % 2, y)
        here = i == 0 and j == 0
        spot = chunk(p, index, c, u)
        receive(spot, firsts[p].at[index, u], apart if here else condition)
        send(spot, spot, w_out.at[p], firsts[p].at[index, u], across, condition, False)
        send(
            spot, spot, w_part.at[p], second(p, index), partner,
            own if here else condition, False,
        )

    def beside(p, i, j, u):
        index = sp_of((zh + i) % nh, (zl + j) % 2, 1 - y)
        spot = chunk(p, index, c, u)
        receive(spot, firsts[p].at[index, u])
        send(spot, spot, w_part.at[p], second(p, index), partner, None, False)

    def rest(p):
        receive(halves(p, n - 1), w_second.at[p], own)
        receive(halves(p, n), w_second.at[p], apart)

    far = [(i, j) for i in range(1, nh) for j in range(2)]
    near = (0, 1)
    pieces = x_pass.shape[1]

    def rows_of(index, u):
        length = rows // pieces
        return xbuf.at[pl.ds(pl.multiple_of((index * pieces + u) * length, length), length)]

    def pass_tokens(k, u):
        core = (c + k) % 2
        index = tp_of(x, core)
        spot = rows_of(index, u)
        receive(spot, x_pass.at[core, u], apart if k == 0 else None)
        for r in range(1, nx):
            send(
                spot, spot, x_fwd, x_other, device(zh, zl, y, (x + r) % nx, c), apart, False,
            )

    send(
        lbuf.at[0], lbuf.at[1], small_send.at[0], small_recv.at[0],
        device(zh, c, y, x, zl), apart,
    )
    send(gbuf.at[0], gbuf.at[1], small_send.at[1], small_recv.at[1], partner, own)
    for u in range(cuts[0]):
        scatter_far(0, u)
    scatter_chip(0)
    def give_tokens(u):
        ours, there = rows_of(piece, u), rows_of(t, u)
        send(ours, there, x_send, x_pass.at[c, u], device(zh, 1 - zl, y, x, zl), None, False)
        for r in range(1, nx):
            send(
                ours, there, x_send, x_other, device(zh, zl, y, (x + r) % nx, zl), None, False,
            )
        send(ours, there, x_send, x_pass.at[c, u], device(zh, zl, y, x, zl), apart, False)

    for u in range(pieces // 2):
        give_tokens(u)
    for u in range(cuts[0]):
        scatter_near(0, u)
    for u in range(pieces // 2, pieces):
        give_tokens(u)
    for p in range(1, 4):
        scatter_chip(p)
    for p in range(1, 3):
        for u in range(cuts[p]):
            scatter_far(p, u)
            scatter_near(p, u)
    for p in range(4):
        for u in range(cuts[p]):
            entry(p, 0, 0, u)
    lines = lax.broadcasted_iota(jnp.int32, (tok, tok), 0)
    lanes = lax.broadcasted_iota(jnp.int32, (tok, tok), 1)
    causal = lines >= lanes
    upto = jnp.where(lines <= lanes, 1.0, 0.0)
    receive(lbuf.at[1], small_recv.at[0], apart)
    receive(gbuf.at[1], small_recv.at[1], apart)
    pick = jnp.where(own, 0, 1)
    logs = jnp.concatenate([lbuf[pick], jnp.zeros((8 - heads, tok), F32)], axis=0)
    turned = lax.dot_general(
        logs, upto, (((1,), (0,)), ((), ())),
        preferred_element_type=F32, precision=lax.Precision.HIGHEST,
    )
    fill = jnp.zeros((LANES - 8, tok), F32)
    within = jnp.concatenate([turned, fill], axis=0).T
    gates_own = gbuf[pick, :, pl.ds(pl.multiple_of(q * tok, tok), tok)]
    gate_col = jnp.concatenate(
        [gates_own, jnp.zeros((LANES - heads, tok), F32)], axis=0
    ).T
    cosine, sine = table[:, : HEAD // 2], table[:, HEAD // 2 :]

    for u in range(cuts[0]):
        beside(0, 0, 0, u)
    for a in far:
        entry(0, *a, 0)
    for u in range(pieces // 2):
        for k in range(2):
            pass_tokens(k, u)
    for u in range(cuts[1]):
        beside(1, 0, 0, u)
    for u in range(1, cuts[0]):
        for a in far:
            entry(0, *a, u)
    for a in far:
        beside(0, *a, 0)
    for u in range(cuts[0]):
        entry(0, *near, u)
    for u in range(pieces // 2, pieces):
        for k in range(2):
            pass_tokens(k, u)
    for a in far:
        entry(1, *a, 0, middle)
    for u in range(1, cuts[0]):
        for a in far:
            beside(0, *a, u)
    for p in range(2, 4):
        for u in range(cuts[p]):
            beside(p, 0, 0, u)
    for u in range(cuts[0]):
        beside(0, *near, u)
    for u in range(1, cuts[1]):
        for a in far:
            entry(1, *a, u, middle)
    for a in far:
        entry(1, *a, 0, outer)

    receive(xbuf.at[pl.ds(0, (m - 2) * rows)], x_other)
    rest(0)

    def exchange(buf, e, index, sem, where, condition):
        send(buf.at[index], buf.at[index], sem, k_recv.at[e, index], where, condition)

    def arrive(buf, e, index, condition):
        receive(buf.at[index], k_recv.at[e, index], condition)

    def exchange_send(buf, e):
        for i in range(1, nh):
            exchange(
                buf, e, q, k_send.at[e, i - 1], device((zh + i) % nh, zl, y, x, c), zh + i < nh
            )
        exchange(buf, e, q, k_y.at[e, 0], across, c + y < 2)
        exchange(buf, e, q, k_part.at[e, 0, 0], partner, c == 0)

    def exchange_across(buf, e):
        index = sp_of(zh, c, 1 - y)
        arrive(buf, e, index, c <= y)
        exchange(buf, e, index, k_part.at[e, 0, 1], partner, c == 0)

    def exchange_part(buf, e):
        for k in range(2):
            arrive(buf, e, sp_of(zh, 1 - c, (y + k) % 2), c == 1)

    def exchange_far(buf, e):
        for i in range(1, nh):
            index = sp_of((zh + nh - i) % nh, c, y)
            arrive(buf, e, index, zh >= i)
            exchange(buf, e, index, k_y.at[e, i], across, zh >= i)
            exchange(buf, e, index, k_part.at[e, i, 0], partner, zh >= i)

    def exchange_far_across(buf, e):
        for i in range(1, nh):
            index = sp_of((zh + nh - i) % nh, c, 1 - y)
            arrive(buf, e, index, zh >= i)
            exchange(buf, e, index, k_part.at[e, i, 1], partner, zh >= i)

    def exchange_far_part(buf, e):
        for i in range(1, nh):
            for k in range(2):
                arrive(buf, e, sp_of((zh + nh - i) % nh, 1 - c, (y + k) % 2), zh >= i)

    def rope(field):
        first, second = field[:, : HEAD // 2], field[:, HEAD // 2 :]
        return jnp.concatenate(
            [first * cosine - second * sine, first * sine + second * cosine], axis=-1
        )

    def project(buf):
        deep = buf.shape[2]
        return sum(
            dot(xbuf[:tok, k * deep : (k + 1) * deep], buf[k], ((1,), (1,))) for k in range(n)
        )

    proj = project(abuf)
    kvbuf[q] = proj[:, : 2 * HEAD].astype(BF16)
    exchange_send(kvbuf, 0)
    scatter_far(3, 0)
    scatter_near(3, 0)
    wide = heads * tok
    zeros = jnp.zeros((tok, HEAD), F32)
    for h in range(heads):
        query = proj[:, (2 + h) * HEAD : (3 + h) * HEAD] * (HEAD ** (-0.5) * LOG2E)
        qbuf[h * tok : (h + 1) * tok, :] = jnp.concatenate([query, zeros], axis=1).astype(BF16)
        cbuf_gate[h * tok : (h + 1) * tok, :] = jnp.broadcast_to(
            gate_col[:, h : h + 1] * LOG2E, (tok, LANES)
        )
    low_lanes = lax.broadcasted_iota(jnp.int32, (tok, 2 * HEAD), 1) < HEAD

    def attend(indices, masked=False):
        total = None if masked else num[...]
        for index in indices:
            block = kvbuf[index]
            values = jnp.where(low_lanes, jnp.ones_like(block), block)
            gates = gbuf[pick, :, pl.ds(pl.multiple_of(index * tok, tok), tok)] * LOG2E
            logits = dot(qbuf[...], block, ((1,), (1,)))
            column = cbuf_gate[...]
            column = jnp.concatenate([column] * (tok // LANES), axis=1)
            pieces_ = []
            for h in range(heads):
                part = slice(h * tok, (h + 1) * tok)
                shifted = logits[part] + column[part] - gates[h : h + 1, :]
                if masked:
                    shifted = jnp.where(causal, shifted, -jnp.inf)
                pieces_.append(jnp.exp2(shifted).astype(BF16))
            term = dot(jnp.concatenate(pieces_, axis=0), values)
            total = term if total is None else total + term
        num[...] = total

    for u in range(1, cuts[1]):
        for a in far:
            entry(1, *a, u, outer)
    attend([q], True)
    for a in far:
        beside(1, *a, 0)
    for u in range(cuts[1]):
        entry(1, *near, u)
    exchange_across(kvbuf, 0)
    exchange_part(kvbuf, 0)
    index = sp_of(zh, 0, 0)
    pl.when(index < q)(functools.partial(attend, [index]))
    pl.when(index + 1 < q)(functools.partial(attend, [index + 1]))
    for u in range(1, cuts[1]):
        for a in far:
            beside(1, *a, u)
    for u in range(cuts[2]):
        for a in far:
            entry(2, *a, u)
    pl.when(index + 2 < q)(functools.partial(attend, [index + 2]))
    for u in range(cuts[1]):
        beside(1, *near, u)
    for u in range(cuts[2]):
        entry(2, *near, u)
    exchange_far(kvbuf, 0)
    rest(1)
    proj = project(bbuf)
    keys, vals, updates, marks = [], [], [], []
    for h in range(heads):
        base = h * HEAD
        key = rope(proj[:, base : base + HEAD]).astype(BF16)
        val = proj[:, base + width : base + width + HEAD].astype(BF16)
        column = within[:, h : h + 1]
        last = column[tok - 1 :, :]
        faded = (key.astype(F32) * jnp.exp(last - column)).astype(BF16)
        updates.append(dot(faded, val, ((0,), (0,))))
        high = last.astype(BF16).astype(F32)
        low = last - high
        marks.append(jnp.broadcast_to(high, (8, HEAD)))
        marks.append(jnp.broadcast_to(low, (8, HEAD)))
        keys.append(key)
        vals.append(val)
    marks.append(jnp.zeros((HEAD - 16 * heads, HEAD), F32))
    blocks = updates + [jnp.concatenate(marks, axis=0)]
    if len(blocks) % 2:
        blocks.append(jnp.zeros((HEAD, HEAD), F32))
    for k in range(0, len(blocks), 2):
        both = jnp.concatenate(blocks[k : k + 2], axis=1).astype(BF16)
        stbuf[q, k // 2 * HEAD : (k // 2 + 1) * HEAD, :] = both

    def piece_of(index, k):
        spot = slice(k % 2 * HEAD, (k % 2 + 1) * HEAD)
        return stbuf[index, k // 2 * HEAD : (k // 2 + 1) * HEAD, spot].astype(F32)

    exchange_send(stbuf, 1)
    for u in range(1, cuts[3]):
        scatter_far(3, u)
        scatter_near(3, u)
    for a in far:
        entry(3, *a, 0)
    for u in range(cuts[2]):
        for a in far:
            beside(2, *a, u)
        beside(2, *near, u)
    exchange_far(stbuf, 1)
    entry(3, *near, 0)
    rest(2)

    proj = project(cbuf)
    local, lifts = [], []
    for h in range(heads):
        query = (rope(proj[:, h * HEAD : (h + 1) * HEAD]) * HEAD ** (-0.5)).astype(BF16)
        column = within[:, h : h + 1]
        gap = jnp.where(causal, column - turned[h : h + 1, :], 0.0)
        scores = dot(query, keys[h], ((1,), (1,)))
        weights = jnp.where(causal, scores * jnp.exp(gap), 0.0).astype(BF16)
        local.append(dot(weights, vals[h]))
        lifts.append((query.astype(F32) * jnp.exp(column)).astype(BF16))
    exchange_far_across(kvbuf, 0)
    exchange_far_part(kvbuf, 0)

    def attend_far(half):
        for i in range(1, nh):
            index = sp_of((zh + nh - i) % nh, 0, 0) + 2 * half
            pl.when(zh >= i)(functools.partial(attend, [index, index + 1]))

    attend_far(0)
    exchange_across(stbuf, 1)
    exchange_far_across(stbuf, 1)
    attend_far(1)
    for u in range(1, cuts[3]):
        for a in far:
            entry(3, *a, u)
        entry(3, *near, u)
    exchange_part(stbuf, 1)
    exchange_far_part(stbuf, 1)
    state[...] = jnp.zeros_like(state)
    for j in range(n - 1):
        def earlier(j=j):
            marked = piece_of(j, heads)
            for h in range(heads):
                total = marked[16 * h : 16 * h + 1] + marked[16 * h + 8 : 16 * h + 9]
                state[h] = jnp.exp(total) * state[h] + piece_of(j, h)

        pl.when(q > j)(earlier)
    retained, attended = [], []
    for h in range(heads):
        raw = local[h] + dot(lifts[h], state[h].astype(BF16))
        centre = jnp.mean(raw, axis=-1, keepdims=True)
        spread = jnp.mean(jnp.square(raw - centre), axis=-1, keepdims=True)
        retained.append(((raw - centre) * lax.rsqrt(spread + EPS)).astype(BF16))
        both = num[h * tok : (h + 1) * tok, :]
        attended.append((both[:, HEAD:] / both[:, :HEAD]).astype(BF16))
    mixed = jnp.concatenate(retained + attended, axis=-1)
    order = [(i, j) for i in range(nh) for j in range(2)]

    def produce(i, j, l):
        index = sp_of((zh + i) % nh, (zl + j) % 2, (y + l) % 2)
        receive(
            halves(3, 1), o_second.at[index], apart if i == 0 and j == 0 and l == 0 else None
        )
        outbuf[index] = dot(mixed, obuf[index]).astype(BF16)
        for r in reversed(range(nx)):
            for k in range(2):
                where = tp_of((x + r) % nx, (c + k) % 2)
                rows_there = pl.ds(pl.multiple_of(where * rows, rows), rows)
                send(
                    outbuf.at[index, rows_there], rsbuf.at[index, g], r_send, r_recv.at[index],
                    device(zh, c, y, (x + r) % nx, (c + k) % 2),
                    apart if r == 0 and k == 0 else None, False,
                )

    for i, j in order:
        produce(i, j, 0)
    for u in range(cuts[3]):
        beside(3, *near, u)
    for u in range(cuts[3]):
        for a in far:
            beside(3, *a, u)
    for i, j in order:
        produce(i, j, 1)
    columns = obuf.shape[2]
    for l in range(2):
        for i, j in order:
            index = sp_of((zh + i) % nh, (zl + j) % 2, (y + l) % 2)

            def keep(index=index):
                rsbuf[index, g] = outbuf[index, pl.ds(pl.multiple_of(t * rows, rows), rows)]

            receive(rsbuf.at[index, pl.ds(0, m - 1)], r_recv.at[index], own)
            pl.when(own)(keep)
            receive(rsbuf.at[index], r_recv.at[index], apart)
            total = rsbuf[index, 0].astype(F32)
            for other in range(1, m):
                total = total + rsbuf[index, other].astype(F32)
            span = pl.ds(pl.multiple_of(index * columns, columns), columns)
            out_ref[:, span] = total.astype(BF16)
    for p in range(4):
        drain(halves(p, n - 1), w_out.at[p], own)
        drain(halves(p, n), w_out.at[p], apart)
        drain(halves(p, n), w_part.at[p], own)
        drain(halves(p, n - 1), w_part.at[p], apart)
    drain(xbuf.at[pl.ds(0, nx * rows)], x_send, own)
    drain(xbuf.at[pl.ds(0, (nx + 1) * rows)], x_send, apart)
    drain(xbuf.at[pl.ds(0, (m - 2) * rows)], x_fwd, apart)
    drain(rsbuf.at[:, pl.ds(0, m - 1)], r_send, own)
    drain(rsbuf, r_send, apart)
    for copy, condition in started:
        guarded(condition, copy.wait_send)


def body(
    n,
    m,
    tokens,
    pre_gain,
    w_query_ret,
    w_key_ret,
    w_value_ret,
    w_query_att,
    w_key_att,
    w_value_att,
    w_out_ret,
    w_out_att,
    retain_log,
    forget_total,
):
    rows, depth = tokens.shape
    tok = rows * m
    heads = retain_log.shape[1]
    nh, nx = n // 4, m // 2
    half = HEAD // 2
    inverse = np.float32(THETA) ** (-np.arange(half, dtype=np.float32) / np.float32(half))
    angles = np.arange(n * tok, dtype=np.float32)[:, None] * inverse[None, :]
    table = np.concatenate([np.cos(angles), np.sin(angles)], axis=1).astype(np.float32)
    wide_a = 2 * HEAD + heads * HEAD
    wide_b, wide_c = 2 * heads * HEAD, heads * HEAD
    deep = w_key_ret.shape[0]
    deep_o = w_out_ret.shape[0] + w_out_att.shape[0]
    tall = (heads // 2 + 1) * HEAD
    hbm = pl.BlockSpec(memory_space=pl.ANY)
    vmem = pl.BlockSpec(memory_space=pltpu.VMEM)
    dma = pltpu.SemaphoreType.DMA
    return pl.pallas_call(
        functools.partial(kernel, n, m, heads),
        out_shape=jax.ShapeDtypeStruct((rows, depth), BF16),
        in_specs=[hbm] * 13,
        out_specs=vmem,
        scratch_shapes=[
            pltpu.VMEM(tokens.shape, BF16),
            pltpu.VMEM((tok, HEAD), F32),
            pltpu.VMEM((2,) + retain_log.shape[::-1], F32),
            pltpu.VMEM((2,) + forget_total.shape, F32),
            pltpu.VMEM((tok + rows, depth), BF16),
            pltpu.VMEM((n + 1, wide_a, deep), BF16),
            pltpu.VMEM((n + 1, wide_b, deep), BF16),
            pltpu.VMEM((n + 1, wide_c, deep), BF16),
            pltpu.VMEM((n + 1, deep_o, w_out_ret.shape[1]), BF16),
            pltpu.VMEM((n, tok, 2 * HEAD), BF16),
            pltpu.VMEM((n, tall, 2 * HEAD), BF16),
            pltpu.VMEM((heads, HEAD, HEAD), F32),
            pltpu.VMEM((heads * tok, 2 * HEAD), F32),
            pltpu.VMEM((heads * tok, 2 * HEAD), BF16),
            pltpu.VMEM((heads * tok, LANES), F32),
            pltpu.VMEM((n, tok, w_out_ret.shape[1]), BF16),
            pltpu.VMEM((n, m, rows, w_out_ret.shape[1]), BF16),
            pltpu.VMEM((1, depth), F32),
            dma((9,)),
            dma((2,)),
            dma((2,)),
            dma,
            dma,
            dma((2, TOKEN_CUT)),
            dma,
            dma((len(CUTS),)),
            dma((len(CUTS),)),
            *[dma((n, count)) for count in CUTS],
            dma((len(CUTS) - 1,)),
            dma((n,)),
            dma((2, nh - 1)),
            dma((2, nh)),
            dma((2, nh, 2)),
            dma((2, n)),
            dma,
            dma((n,)),
        ],
        compiler_params=pltpu.CompilerParams(
            collective_id=0, has_side_effects=True, vmem_limit_bytes=60 * 1024 * 1024
        ),
    )(
        tokens,
        pre_gain[None, :],
        w_query_ret.T,
        w_key_ret.T,
        w_value_ret.T,
        w_query_att.T,
        w_key_att.T,
        w_value_att.T,
        w_out_ret,
        w_out_att,
        jnp.asarray(table),
        retain_log.T,
        forget_total,
    )


def rotate(field, positions):
    half = field.shape[-1] // 2
    inverse = THETA ** (-jnp.arange(half, dtype=jnp.float32) / half)
    angles = positions[:, None] * inverse[None, :]
    cosine = jnp.cos(angles)[:, None, :]
    sine = jnp.sin(angles)[:, None, :]
    first_half = field[..., :half]
    second_half = field[..., half:]
    return jnp.concatenate(
        [first_half * cosine - second_half * sine, first_half * sine + second_half * cosine],
        axis=-1,
    )


def head_norm(values):
    centre = jnp.mean(values, axis=-1, keepdims=True)
    spread = jnp.mean(jnp.square(values - centre), axis=-1, keepdims=True)
    return (values - centre) * lax.rsqrt(spread + EPS)


def advance(state, pair):
    decay, update = pair
    return (jnp.exp(decay)[:, None, None] * state + update, state)


def plain_body(
    tokens,
    pre_gain,
    w_query_ret,
    w_key_ret,
    w_value_ret,
    w_query_att,
    w_key_att,
    w_value_att,
    w_out_ret,
    w_out_att,
    retain_log,
    forget_total,
):
    rows = tokens.astype(jnp.float32)
    normed = (
        rows * lax.rsqrt(jnp.mean(rows * rows, axis=-1, keepdims=True) + EPS) * pre_gain
    ).astype(jnp.bfloat16)
    gathered = lax.all_gather(normed, "tp", axis=0, tiled=True)
    tok_dev = gathered.shape[0]
    offset = lax.axis_index("sp") * tok_dev
    query_places = offset + jnp.arange(tok_dev, dtype=jnp.int32)
    positions = query_places.astype(jnp.float32)

    def blocked(values):
        return values.reshape((tok_dev // SPAN, SPAN) + values.shape[1:])

    pieces = (
        lax.all_gather(w_query_ret, "sp", axis=0, tiled=True),
        lax.all_gather(w_key_ret, "sp", axis=0, tiled=True),
        lax.all_gather(w_value_ret, "sp", axis=0, tiled=True),
        lax.all_gather(w_query_att, "sp", axis=0, tiled=True),
        lax.all_gather(w_key_att, "sp", axis=0, tiled=True),
        lax.all_gather(w_value_att, "sp", axis=0, tiled=True),
    )
    projected = tuple(
        (jnp.dot(gathered, piece, preferred_element_type=jnp.float32) for piece in pieces)
    )
    heads = retain_log.shape[1]
    shape = (tok_dev, heads, HEAD)
    query = blocked(
        (rotate(projected[0].reshape(shape), positions) * HEAD ** (-0.5)).astype(jnp.bfloat16)
    )
    key_rows = blocked(rotate(projected[1].reshape(shape), positions).astype(jnp.bfloat16))
    value_rows = blocked(projected[2].astype(jnp.bfloat16).reshape(shape))
    within = jnp.cumsum(blocked(retain_log), axis=1)
    causal = jnp.arange(SPAN)[:, None] >= jnp.arange(SPAN)[None, :]
    scores = jnp.einsum("bthd,bshd->bhts", query, key_rows, preferred_element_type=jnp.float32)
    turned = jnp.transpose(within, (0, 2, 1))
    gap = jnp.where(causal, turned[:, :, :, None] - turned[:, :, None, :], 0.0)
    weights = jnp.where(causal, scores * jnp.exp(gap), 0.0).astype(jnp.bfloat16)
    local = jnp.einsum("bhts,bshd->bthd", weights, value_rows, preferred_element_type=jnp.float32)
    last = within[:, -1]
    faded = (key_rows.astype(jnp.float32) * jnp.exp(last[:, None, :] - within)[..., None]).astype(
        jnp.bfloat16
    )
    updates = jnp.einsum("bshd,bshe->bhde", faded, value_rows, preferred_element_type=jnp.float32)
    zero_state = jnp.zeros((heads, HEAD, HEAD), jnp.float32)
    final, _ = lax.scan(advance, zero_state, (last, updates))
    decay_total = jnp.sum(last, axis=0)
    own_state = final.reshape(heads, HEAD * HEAD)
    every_total = lax.all_gather(
        decay_total[None].astype(jnp.bfloat16), "sp", axis=0, tiled=True
    ).astype(jnp.float32)
    every_state = lax.all_gather(
        own_state[None].astype(jnp.bfloat16), "sp", axis=0, tiled=True
    ).astype(jnp.float32)
    device_order = jnp.arange(every_total.shape[0], dtype=jnp.int32)[:, None]
    earlier = device_order < lax.axis_index("sp")
    before = jnp.sum(jnp.where(earlier, every_total, 0.0), axis=0)
    through = jnp.cumsum(every_total, axis=0)
    fading = jnp.where(earlier, jnp.exp(jnp.where(earlier, before[None, :] - through, 0.0)), 0.0)
    incoming = jnp.einsum("jh,jhe->he", fading, every_state, precision=HIGH)
    _, befores = lax.scan(advance, incoming.reshape(heads, HEAD, HEAD), (last, updates))
    lifted = (query.astype(jnp.float32) * jnp.exp(within)[..., None]).astype(jnp.bfloat16)
    carried = jnp.einsum(
        "bthd,bhde->bthe", lifted, befores.astype(jnp.bfloat16), preferred_element_type=jnp.float32
    )
    retained = (
        head_norm((local + carried).reshape(shape))
        .astype(jnp.bfloat16)
        .reshape(tok_dev, heads * HEAD)
    )
    raw_key = projected[4]
    gate_heads = forget_total.shape[0]
    kv_local = raw_key.shape[1] // HEAD
    group = gate_heads // kv_local
    query = (
        (projected[3] * HEAD ** (-0.5)).astype(jnp.bfloat16).reshape(tok_dev, kv_local, group, HEAD)
    )
    key_rows = raw_key.astype(jnp.bfloat16)
    value_rows = projected[5].astype(jnp.bfloat16)
    gate_rows = lax.dynamic_slice_in_dim(forget_total, offset, tok_dev, 1).reshape(
        kv_local, group, tok_dev
    )
    last_row = offset + tok_dev - 1
    init = (
        jnp.zeros((kv_local, group, tok_dev, HEAD), jnp.float32),
        jnp.zeros((kv_local, group, tok_dev), jnp.float32),
    )
    key_piece = lax.all_gather(key_rows, "sp", axis=0, tiled=True)
    value_piece = lax.all_gather(value_rows, "sp", axis=0, tiled=True)
    count = key_piece.shape[0] // KEY_SPAN

    def one_block(index, inner):
        first = index * KEY_SPAN

        def compute(state):
            weighted, total = state
            key_block = lax.dynamic_slice_in_dim(key_piece, index * KEY_SPAN, KEY_SPAN, 0).reshape(
                KEY_SPAN, kv_local, HEAD
            )
            value_block = lax.dynamic_slice_in_dim(
                value_piece, index * KEY_SPAN, KEY_SPAN, 0
            ).reshape(KEY_SPAN, kv_local, HEAD)
            gate_keys = lax.dynamic_slice_in_dim(forget_total, first, KEY_SPAN, 1).reshape(
                kv_local, group, KEY_SPAN
            )
            scores = jnp.einsum(
                "tcgd,scd->cgts", query, key_block, preferred_element_type=jnp.float32
            )
            logits = scores + gate_rows[:, :, :, None] - gate_keys[:, :, None, :]
            allowed = (first + jnp.arange(KEY_SPAN, dtype=jnp.int32))[None, :] <= query_places[
                :, None
            ]
            weights = jnp.exp(jnp.where(allowed, logits, -jnp.inf))
            total = total + jnp.sum(weights, axis=-1)
            weighted = weighted + jnp.einsum(
                "cgts,scd->cgtd",
                weights.astype(jnp.bfloat16),
                value_block,
                preferred_element_type=jnp.float32,
            )
            return (weighted, total)

        def skipped(state):
            return state

        return lax.cond(first <= last_row, compute, skipped, inner)

    weighted, total = lax.fori_loop(0, count, one_block, init)
    result = weighted / total[..., None]
    attended = (
        jnp.transpose(result, (2, 0, 1, 3)).reshape(tok_dev, gate_heads * HEAD).astype(jnp.bfloat16)
    )
    out_ret, out_att = (
        lax.all_gather(w_out_ret, "sp", axis=1, tiled=True),
        lax.all_gather(w_out_att, "sp", axis=1, tiled=True),
    )
    return lax.psum_scatter(
        (
            jnp.dot(retained, out_ret, preferred_element_type=jnp.float32)
            + jnp.dot(attended, out_att, preferred_element_type=jnp.float32)
        ).astype(jnp.bfloat16),
        "tp",
        scatter_dimension=0,
        tiled=True,
    )


def choose(n, m, *arrays):
    tokens, w_key_ret, w_out_ret = arrays[0], arrays[3], arrays[8]
    whole_tiles = w_out_ret.shape[1] % LANES == 0 and w_key_ret.shape[0] % LANES == 0
    heads = arrays[10].shape[1]
    small = 16 * heads <= HEAD and arrays[7].shape[1] == HEAD and arrays[11].shape[0] == heads
    paired = n % 4 == 0 and n > 4 and m % 2 == 0 and m > 2
    if paired and whole_tiles and small and tokens.shape[0] * m == SPAN:
        return body(n, m, *arrays)
    return plain_body(*arrays)


def solution(mesh):
    return jax.shard_map(
        functools.partial(choose, mesh.shape["sp"], mesh.shape["tp"]),
        mesh=mesh,
        in_specs=(
            P(("sp", "tp"), None),
            P(),
            P("sp", "tp"),
            P("sp", "tp"),
            P("sp", "tp"),
            P("sp", "tp"),
            P("sp", "tp"),
            P("sp", "tp"),
            P("tp", "sp"),
            P("tp", "sp"),
            P("sp", "tp"),
            P("tp", None),
        ),
        out_specs=P(("sp", "tp"), None),
        check_vma=False,
    )
```

```python
import functools

import jax
import jax.numpy as jnp
import numpy as np
from jax import lax
from jax.experimental import pallas as pl
from jax.experimental.pallas import tpu as pltpu
from jax.sharding import PartitionSpec as P

HEAD = 64
EPS = 1e-06
THETA = 10000.0
F32 = jnp.float32
BF16 = jnp.bfloat16
MESH = pl.DeviceIdType.MESH
SPAN = 256
KEY_SPAN = 256
LANES = 128
CUTS = (2, 2, 1, 3)
LOG2E = float(np.log2(np.e))
TOKEN_CUT = 4
HIGH = lax.Precision.HIGHEST


def dot(a, b, dims=((1,), (0,))):
    return lax.dot_general(a, b, (dims, ((), ())), preferred_element_type=F32)


def kernel(
    n,
    m,
    heads,
    tok_hbm,
    gain_hbm,
    wq_ret_hbm,
    wk_ret_hbm,
    wv_ret_hbm,
    wq_att_hbm,
    wk_att_hbm,
    wv_att_hbm,
    wo_ret_hbm,
    wo_att_hbm,
    table_hbm,
    logs_hbm,
    gate_hbm,
    out_ref,
    tokens,
    table,
    lbuf,
    gbuf,
    xbuf,
    abuf,
    bbuf,
    cbuf,
    obuf,
    kvbuf,
    stbuf,
    decay,
    num,
    qbuf,
    cbuf_gate,
    outbuf,
    rsbuf,
    passed,
    gain,
    load,
    small_send,
    small_recv,
    x_send,
    x_fwd,
    x_pass,
    x_other,
    w_out,
    w_part,
    first_a,
    first_b,
    first_c,
    first_o,
    w_second,
    o_second,
    k_send,
    k_y,
    k_part,
    k_recv,
    r_send,
    r_pass,
    r_recv,
):
    s, t = lax.axis_index("sp"), lax.axis_index("tp")
    nh, nx = n // 4, m // 2
    y, zl, zh = s % 2, (s // 2) % 2, s // 4
    c, x = t % 2, t // 2
    own = zl == c
    apart = zl != c

    def sp_of(zh_, zl_, y_):
        return zh_ * 4 + zl_ * 2 + y_

    def tp_of(x_, c_):
        return x_ * 2 + c_

    def device(zh_, zl_, y_, x_, c_):
        return {"sp": sp_of(zh_, zl_, y_), "tp": tp_of(x_, c_)}

    q, g = sp_of(zh, c, y), tp_of(x, zl)
    partner = device(zh, zl, y, x, 1 - c)
    across = device(zh, zl, 1 - y, x, c)
    rows = tokens.shape[0]
    tok = rows * m
    width = heads * HEAD
    half_o = wo_ret_hbm.shape[0]

    slot = jnp.where(own, s, n)
    piece = jnp.where(own, t, m)
    groups = (
        (tokens, ((tok_hbm, tokens),)),
        (gain, ((gain_hbm, gain),)),
        (abuf.at[slot], (
            (wk_att_hbm, abuf.at[slot, pl.ds(0, HEAD)]),
            (wv_att_hbm, abuf.at[slot, pl.ds(HEAD, HEAD)]),
            (wq_att_hbm, abuf.at[slot, pl.ds(2 * HEAD, width)]),
        )),
        (bbuf.at[slot], (
            (wk_ret_hbm, bbuf.at[slot, pl.ds(0, width)]),
            (wv_ret_hbm, bbuf.at[slot, pl.ds(width, width)]),
        )),
        (cbuf.at[slot], ((wq_ret_hbm, cbuf.at[slot]),)),
        (obuf.at[slot], (
            (wo_ret_hbm, obuf.at[slot, pl.ds(0, half_o)]),
            (wo_att_hbm, obuf.at[slot, pl.ds(half_o, wo_att_hbm.shape[0])]),
        )),
        (table, ((table_hbm.at[pl.ds(pl.multiple_of(q * tok, tok), tok)], table),)),
        (lbuf.at[0], ((logs_hbm, lbuf.at[0]),)),
        (gbuf.at[0], ((gate_hbm, gbuf.at[0]),)),
    )
    loads = []
    for k, (whole, copies) in enumerate(groups):
        for source, target in copies:
            pltpu.make_async_copy(source, target, load.at[k]).start()
        loads.append(pltpu.make_async_copy(whole, whole, load.at[k]))

    stbuf[...] = jnp.zeros_like(stbuf)
    barrier = pltpu.get_barrier_semaphore()
    greeted = [
        device((zh + i) % nh, zl, 1 - y, x, (c + k) % 2) for i in range(nh) for k in range(2)
    ]
    for i in reversed(range(nh)):
        for j in reversed(range(2)):
            for k in range(2):
                if i or j or k:
                    greeted.append(device((zh + i) % nh, (zl + j) % 2, y, x, (c + k) % 2))
    for r in range(1, nx):
        for j in range(2):
            for k in range(2):
                greeted.append(device(zh, (zl + j) % 2, y, (x + r) % nx, (c + k) % 2))
    for other in greeted:
        pl.semaphore_signal(barrier, inc=1, device_id=other, device_id_type=MESH)

    started = []

    def guarded(condition, action):
        if condition is None:
            action()
        else:
            pl.when(condition)(action)

    def send(source, target, send_sem, recv_sem, where, condition=None, kept=True):
        copy = pltpu.make_async_remote_copy(
            src_ref=source, dst_ref=target, send_sem=send_sem, recv_sem=recv_sem,
            device_id=where, device_id_type=MESH,
        )
        guarded(condition, copy.start)
        if kept:
            started.append((copy, condition))

    def drain(source, send_sem, condition=None):
        started.append((
            pltpu.make_async_remote_copy(
                src_ref=source, dst_ref=source, send_sem=send_sem, recv_sem=send_sem,
                device_id=partner, device_id_type=MESH,
            ),
            condition,
        ))

    def receive(target, recv_sem, condition=None):
        copy = pltpu.make_async_remote_copy(
            src_ref=target, dst_ref=target, send_sem=recv_sem, recv_sem=recv_sem,
            device_id=partner, device_id_type=MESH,
        )
        guarded(condition, copy.wait_recv)

    for copy in loads[:2]:
        copy.wait()
    values = tokens[...].astype(F32)
    scale = lax.rsqrt(jnp.mean(values * values, axis=-1, keepdims=True) + EPS)
    xbuf[pl.ds(pl.multiple_of(piece * rows, rows), rows), :] = (
        values * scale * gain[...]
    ).astype(BF16)
    for copy in loads[2:]:
        copy.wait()
    pl.semaphore_wait(barrier, len(greeted))

    parts = (abuf, bbuf, cbuf, obuf)
    cuts = CUTS

    def chunk(p, index, k, u):
        length = parts[p].shape[1] // (2 * cuts[p])
        start = pl.multiple_of((k * cuts[p] + u) * length, length)
        return parts[p].at[index, pl.ds(start, length)]

    firsts = (first_a, first_b, first_c, first_o)

    def second(p, index):
        return o_second.at[index] if p == 3 else w_second.at[p]

    def halves(p, count):
        return parts[p].at[pl.ds(0, count), pl.ds(0, parts[p].shape[1] // 2)]

    def scatter_one(p, i, k, u, condition):
        core = (c + k) % 2
        send(
            chunk(p, slot, core, u), chunk(p, s, core, u), w_out.at[p], firsts[p].at[s, u],
            device((zh + i) % nh, c, y, x, core), condition, False,
        )

    def scatter_chip(p):
        for u in range(cuts[p]):
            scatter_one(p, 0, 1, u, own)

    def scatter_near(p, u):
        for k in range(2):
            scatter_one(p, 0, k, u, apart)

    def scatter_far(p, u, condition=None):
        for i in range(1, nh):
            for k in range(2):
                scatter_one(p, i, k, u, condition)

    middle = zl != zh % 2
    outer = zl == zh % 2

    def entry(p, i, j, u, condition=None):
        index = sp_of((zh + i) % nh, (zl + j) % 2, y)
        here = i == 0 and j == 0
        spot = chunk(p, index, c, u)
        receive(spot, firsts[p].at[index, u], apart if here else condition)
        send(spot, spot, w_out.at[p], firsts[p].at[index, u], across, condition, False)
        send(
            spot, spot, w_part.at[p], second(p, index), partner,
            own if here else condition, False,
        )

    def beside(p, i, j, u):
        index = sp_of((zh + i) % nh, (zl + j) % 2, 1 - y)
        spot = chunk(p, index, c, u)
        receive(spot, firsts[p].at[index, u])
        send(spot, spot, w_part.at[p], second(p, index), partner, None, False)

    def rest(p):
        receive(halves(p, n - 1), w_second.at[p], own)
        receive(halves(p, n), w_second.at[p], apart)

    far = [(i, j) for i in range(1, nh) for j in range(2)]
    near = (0, 1)
    pieces = x_pass.shape[1]

    def rows_of(index, u):
        length = rows // pieces
        return xbuf.at[pl.ds(pl.multiple_of((index * pieces + u) * length, length), length)]

    def pass_tokens(k, u):
        core = (c + k) % 2
        index = tp_of(x, core)
        spot = rows_of(index, u)
        receive(spot, x_pass.at[core, u], apart if k == 0 else None)
        for r in range(1, nx):
            send(
                spot, spot, x_fwd, x_other, device(zh, zl, y, (x + r) % nx, c), apart, False,
            )

    send(
        lbuf.at[0], lbuf.at[1], small_send.at[0], small_recv.at[0],
        device(zh, c, y, x, zl), apart,
    )
    send(gbuf.at[0], gbuf.at[1], small_send.at[1], small_recv.at[1], partner, own)
    for u in range(cuts[0]):
        scatter_far(0, u)
    scatter_chip(0)
    def give_tokens(u):
        ours, there = rows_of(piece, u), rows_of(t, u)
        send(ours, there, x_send, x_pass.at[c, u], device(zh, 1 - zl, y, x, zl), None, False)
        for r in range(1, nx):
            send(
                ours, there, x_send, x_other, device(zh, zl, y, (x + r) % nx, zl), None, False,
            )
        send(ours, there, x_send, x_pass.at[c, u], device(zh, zl, y, x, zl), apart, False)

    for u in range(pieces // 2):
        give_tokens(u)
    for u in range(cuts[0]):
        scatter_near(0, u)
    for u in range(pieces // 2, pieces):
        give_tokens(u)
    for p in range(1, 4):
        scatter_chip(p)
    for p in range(1, 3):
        for u in range(cuts[p]):
            scatter_far(p, u)
            scatter_near(p, u)
    for p in range(4):
        for u in range(cuts[p]):
            entry(p, 0, 0, u)
    lines = lax.broadcasted_iota(jnp.int32, (tok, tok), 0)
    lanes = lax.broadcasted_iota(jnp.int32, (tok, tok), 1)
    causal = lines >= lanes
    upto = jnp.where(lines <= lanes, 1.0, 0.0)
    receive(lbuf.at[1], small_recv.at[0], apart)
    receive(gbuf.at[1], small_recv.at[1], apart)
    pick = jnp.where(own, 0, 1)
    logs = jnp.concatenate([lbuf[pick], jnp.zeros((8 - heads, tok), F32)], axis=0)
    turned = lax.dot_general(
        logs, upto, (((1,), (0,)), ((), ())),
        preferred_element_type=F32, precision=lax.Precision.HIGHEST,
    )
    fill = jnp.zeros((LANES - 8, tok), F32)
    within = jnp.concatenate([turned, fill], axis=0).T
    gates_own = gbuf[pick, :, pl.ds(pl.multiple_of(q * tok, tok), tok)]
    gate_col = jnp.concatenate(
        [gates_own, jnp.zeros((LANES - heads, tok), F32)], axis=0
    ).T
    cosine, sine = table[:, : HEAD // 2], table[:, HEAD // 2 :]
    for h in range(heads):
        gap = jnp.where(causal, within[:, h : h + 1] - turned[h : h + 1, :], 0.0)
        decay[h] = jnp.where(causal, jnp.exp(gap), 0.0)

    for u in range(cuts[0]):
        beside(0, 0, 0, u)
    for a in far:
        entry(0, *a, 0)
    for u in range(pieces // 2):
        for k in range(2):
            pass_tokens(k, u)
    for u in range(cuts[1]):
        beside(1, 0, 0, u)
    for u in range(1, cuts[0]):
        for a in far:
            entry(0, *a, u)
    for a in far:
        beside(0, *a, 0)
    for u in range(cuts[0]):
        entry(0, *near, u)
    for u in range(pieces // 2, pieces):
        for k in range(2):
            pass_tokens(k, u)
    for a in far:
        entry(1, *a, 0, middle)
    for u in range(1, cuts[0]):
        for a in far:
            beside(0, *a, u)
    for p in range(2, 4):
        for u in range(cuts[p]):
            beside(p, 0, 0, u)
    for u in range(cuts[0]):
        beside(0, *near, u)
    for u in range(1, cuts[1]):
        for a in far:
            entry(1, *a, u, middle)
    for a in far:
        entry(1, *a, 0, outer)

    receive(xbuf.at[pl.ds(0, (m - 2) * rows)], x_other)
    rest(0)

    def exchange(buf, e, index, sem, where, condition):
        send(buf.at[index], buf.at[index], sem, k_recv.at[e, index], where, condition)

    def arrive(buf, e, index, condition):
        receive(buf.at[index], k_recv.at[e, index], condition)

    def exchange_send(buf, e):
        for i in range(1, nh):
            exchange(
                buf, e, q, k_send.at[e, i - 1], device((zh + i) % nh, zl, y, x, c), zh + i < nh
            )
        exchange(buf, e, q, k_y.at[e, 0], across, c + y < 2)
        exchange(buf, e, q, k_part.at[e, 0, 0], partner, c == 0)

    def exchange_across(buf, e):
        index = sp_of(zh, c, 1 - y)
        arrive(buf, e, index, c <= y)
        exchange(buf, e, index, k_part.at[e, 0, 1], partner, c == 0)

    def exchange_part(buf, e):
        for k in range(2):
            arrive(buf, e, sp_of(zh, 1 - c, (y + k) % 2), c == 1)

    def exchange_far(buf, e, also=True):
        for i in range(1, nh):
            index = sp_of((zh + nh - i) % nh, c, y)
            condition = (zh >= i) & also
            arrive(buf, e, index, condition)
            exchange(buf, e, index, k_y.at[e, i], across, condition)
            exchange(buf, e, index, k_part.at[e, i, 0], partner, condition)

    def exchange_far_across(buf, e):
        for i in range(1, nh):
            index = sp_of((zh + nh - i) % nh, c, 1 - y)
            arrive(buf, e, index, zh >= i)
            exchange(buf, e, index, k_part.at[e, i, 1], partner, zh >= i)

    def exchange_far_part(buf, e):
        for i in range(1, nh):
            for k in range(2):
                arrive(buf, e, sp_of((zh + nh - i) % nh, 1 - c, (y + k) % 2), zh >= i)

    def rope(field):
        first, second = field[:, : HEAD // 2], field[:, HEAD // 2 :]
        return jnp.concatenate(
            [first * cosine - second * sine, first * sine + second * cosine], axis=-1
        )

    def project(buf):
        deep = buf.shape[2]
        return sum(
            dot(xbuf[:tok, k * deep : (k + 1) * deep], buf[k], ((1,), (1,))) for k in range(n)
        )

    proj = project(abuf)
    kvbuf[q] = proj[:, : 2 * HEAD].astype(BF16)
    exchange_send(kvbuf, 0)
    scatter_far(3, 0)
    scatter_near(3, 0)
    for u in range(1, cuts[3]):
        scatter_far(3, u, zh == nh - 1)
    wide = heads * tok
    zeros = jnp.zeros((tok, HEAD), F32)
    for h in range(heads):
        query = proj[:, (2 + h) * HEAD : (3 + h) * HEAD] * (HEAD ** (-0.5) * LOG2E)
        qbuf[h * tok : (h + 1) * tok, :] = jnp.concatenate([query, zeros], axis=1).astype(BF16)
        cbuf_gate[h * tok : (h + 1) * tok, :] = jnp.broadcast_to(
            gate_col[:, h : h + 1] * LOG2E, (tok, LANES)
        )
    low_lanes = lax.broadcasted_iota(jnp.int32, (tok, 2 * HEAD), 1) < HEAD

    def attend(indices, masked=False):
        total = None if masked else num[...]
        for index in indices:
            block = kvbuf[index]
            values = jnp.where(low_lanes, jnp.ones_like(block), block)
            gates = gbuf[pick, :, pl.ds(pl.multiple_of(index * tok, tok), tok)] * LOG2E
            logits = dot(qbuf[...], block, ((1,), (1,)))
            column = cbuf_gate[...]
            column = jnp.concatenate([column] * (tok // LANES), axis=1)
            pieces_ = []
            for h in range(heads):
                part = slice(h * tok, (h + 1) * tok)
                shifted = logits[part] + column[part] - gates[h : h + 1, :]
                if masked:
                    shifted = jnp.where(causal, shifted, -jnp.inf)
                pieces_.append(jnp.exp2(shifted).astype(BF16))
            term = dot(jnp.concatenate(pieces_, axis=0), values)
            total = term if total is None else total + term
        num[...] = total

    for u in range(1, cuts[1]):
        for a in far:
            entry(1, *a, u, outer)
    attend([q], True)
    for a in far:
        beside(1, *a, 0)
    for u in range(cuts[1]):
        entry(1, *near, u)
    exchange_across(kvbuf, 0)
    exchange_part(kvbuf, 0)
    index = sp_of(zh, 0, 0)
    pl.when(index < q)(functools.partial(attend, [index]))
    pl.when(index + 1 < q)(functools.partial(attend, [index + 1]))
    for u in range(1, cuts[1]):
        for a in far:
            beside(1, *a, u)
    for u in range(cuts[2]):
        for a in far:
            entry(2, *a, u)
    pl.when(index + 2 < q)(functools.partial(attend, [index + 2]))
    for u in range(cuts[1]):
        beside(1, *near, u)
    for u in range(cuts[2]):
        entry(2, *near, u)
    exchange_far(kvbuf, 0)
    rest(1)
    proj = project(bbuf)
    keys, vals, updates, marks = [], [], [], []
    for h in range(heads):
        base = h * HEAD
        key = rope(proj[:, base : base + HEAD]).astype(BF16)
        val = proj[:, base + width : base + width + HEAD].astype(BF16)
        column = within[:, h : h + 1]
        last = column[tok - 1 :, :]
        faded = (key.astype(F32) * jnp.exp(last - column)).astype(BF16)
        updates.append(dot(faded, val, ((0,), (0,))))
        high = last.astype(BF16).astype(F32)
        low = last - high
        marks.append(jnp.broadcast_to(high, (8, HEAD)))
        marks.append(jnp.broadcast_to(low, (8, HEAD)))
        keys.append(key)
        vals.append(val)
    marks.append(jnp.zeros((HEAD - 16 * heads, HEAD), F32))
    blocks = updates + [jnp.concatenate(marks, axis=0)]
    if len(blocks) % 2:
        blocks.append(jnp.zeros((HEAD, HEAD), F32))
    for k in range(0, len(blocks), 2):
        both = jnp.concatenate(blocks[k : k + 2], axis=1).astype(BF16)
        stbuf[q, k // 2 * HEAD : (k // 2 + 1) * HEAD, :] = both

    def piece_of(index, k):
        spot = slice(k % 2 * HEAD, (k % 2 + 1) * HEAD)
        return stbuf[index, k // 2 * HEAD : (k // 2 + 1) * HEAD, spot].astype(F32)

    exchange_send(stbuf, 1)
    for u in range(1, cuts[3]):
        scatter_far(3, u, zh < nh - 1)
        scatter_near(3, u)
    for a in far:
        entry(3, *a, 0)
    for u in range(cuts[2]):
        for a in far:
            beside(2, *a, u)
        beside(2, *near, u)
    exchange_far_across(kvbuf, 0)
    exchange_far(stbuf, 1, zl <= c)
    entry(3, *near, 0)
    rest(2)

    proj = project(cbuf)
    local, lifts = [], []
    for h in range(heads):
        query = (rope(proj[:, h * HEAD : (h + 1) * HEAD]) * HEAD ** (-0.5)).astype(BF16)
        column = within[:, h : h + 1]
        scores = dot(query, keys[h], ((1,), (1,)))
        weights = (scores * decay[h]).astype(BF16)
        local.append(dot(weights, vals[h]))
        lifts.append((query.astype(F32) * jnp.exp(column)).astype(BF16))
    exchange_far(stbuf, 1, zl > c)
    exchange_far_part(kvbuf, 0)

    def attend_far(half):
        for i in range(1, nh):
            index = sp_of((zh + nh - i) % nh, 0, 0) + 2 * half
            pl.when(zh >= i)(functools.partial(attend, [index, index + 1]))

    exchange_across(stbuf, 1)
    attend_far(0)
    attend_far(1)
    exchange_far_across(stbuf, 1)
    for u in range(1, cuts[3]):
        for a in far:
            entry(3, *a, u)
        entry(3, *near, u)
    exchange_part(stbuf, 1)
    exchange_far_part(stbuf, 1)
    states = [jnp.zeros((HEAD, HEAD), F32)] * heads
    for j in range(n - 1):
        marked = piece_of(j, heads)
        for h in range(heads):
            total = marked[16 * h : 16 * h + 1] + marked[16 * h + 8 : 16 * h + 9]
            moved = jnp.exp(total) * states[h] + piece_of(j, h)
            states[h] = jnp.where(q > j, moved, states[h])
    retained, attended = [], []
    for h in range(heads):
        raw = local[h] + dot(lifts[h], states[h].astype(BF16))
        centre = jnp.mean(raw, axis=-1, keepdims=True)
        spread = jnp.mean(jnp.square(raw - centre), axis=-1, keepdims=True)
        retained.append(((raw - centre) * lax.rsqrt(spread + EPS)).astype(BF16))
        both = num[h * tok : (h + 1) * tok, :]
        attended.append((both[:, HEAD:] / both[:, :HEAD]).astype(BF16))
    mixed = jnp.concatenate(retained + attended, axis=-1)
    order = [(i, j) for i in range(nh) for j in range(2)]

    pair = 2 * rows
    pair_here = pl.ds(pl.multiple_of(x * pair, pair), pair)

    def slice_of(i, j, l):
        return sp_of((zh + i) % nh, (zl + j) % 2, (y + l) % 2)

    def multiply(i, j, l):
        index = slice_of(i, j, l)
        receive(
            halves(3, 1), o_second.at[index], apart if i == 0 and j == 0 and l == 0 else None
        )
        outbuf[index] = dot(mixed, obuf[index]).astype(BF16)
        return index

    def give(index, spot, x_, c_, condition):
        where = tp_of(x_, c_)
        rows_there = pl.ds(pl.multiple_of(where * rows, rows), rows)
        send(
            outbuf.at[index, rows_there], rsbuf.at[index, spot], r_send, r_recv.at[index],
            device(zh, c, y, x_, c_), condition, False,
        )

    def produce(i, j, l):
        index = multiply(i, j, l)
        for r in reversed(range(nx)):
            for k in range(2):
                give(
                    index, g, (x + r) % nx, (c + k) % 2, apart if r == 0 and k == 0 else None
                )

    def start_pair(i, j):
        index = multiply(i, j, 0)
        if i % 2:
            send(
                outbuf.at[index], passed.at[index], r_send, r_pass.at[index],
                device(zh, 1 - zl, y, x, c), apart, False,
            )
        else:
            for r in range(1, nx):
                other = (x + r) % nx
                send(
                    outbuf.at[index, pl.ds(pl.multiple_of(other * pair, pair), pair)],
                    passed.at[index, pl.ds((r - 1) * pair, pair)], r_send, r_pass.at[index],
                    device(zh, zl, y, other, c), None, False,
                )

    def finish_pair(i, j):
        index = slice_of(i, j, 0)
        if i % 2:
            receive(passed.at[index], r_pass.at[index], own)

            def merge():
                outbuf[index] = (
                    outbuf[index].astype(F32) + passed[index].astype(F32)
                ).astype(BF16)

            pl.when(own)(merge)
            for r in reversed(range(nx)):
                for k in range(2):
                    if r or k:
                        give(index, x, (x + r) % nx, (c + k) % 2, own)
        else:
            receive(passed.at[index, pl.ds(0, (nx - 1) * pair)], r_pass.at[index])
            total = outbuf[index, pair_here].astype(F32)
            for r in range(1, nx):
                total = total + passed[index, (r - 1) * pair : r * pair].astype(F32)
            outbuf[index, pair_here] = total.astype(BF16)
            for k in (1, 0):
                give(index, zl, x, (c + k) % 2, None if k else apart)

    order = [(i, j) for i in range(nh) for j in range(2)]
    for i, j in order:
        start_pair(i, j)
    for u in range(cuts[3]):
        beside(3, *near, u)
    for u in range(cuts[3]):
        for a in far:
            beside(3, *a, u)
    for i, j in order:
        if i % 2 == 0:
            finish_pair(i, j)
    for i, j in order[: len(order) // 2]:
        produce(i, j, 1)
    for i, j in order:
        if i % 2:
            finish_pair(i, j)
    for i, j in order[len(order) // 2 :]:
        produce(i, j, 1)
    columns = obuf.shape[2]
    for l in range(2):
        for i, j in order:
            index = slice_of(i, j, l)
            if l:
                spot, count = g, m
            elif i % 2:
                spot, count = x, nx
            else:
                spot, count = zl, 2

            def keep(index=index, spot=spot):
                rsbuf[index, spot] = outbuf[index, pl.ds(pl.multiple_of(t * rows, rows), rows)]

            receive(rsbuf.at[index, pl.ds(0, count - 1)], r_recv.at[index], own)
            pl.when(own)(keep)
            receive(rsbuf.at[index, pl.ds(0, count)], r_recv.at[index], apart)
            total = rsbuf[index, 0].astype(F32)
            for other in range(1, count):
                total = total + rsbuf[index, other].astype(F32)
            span = pl.ds(pl.multiple_of(index * columns, columns), columns)
            out_ref[:, span] = total.astype(BF16)
    for p in range(4):
        drain(halves(p, n - 1), w_out.at[p], own)
        drain(halves(p, n), w_out.at[p], apart)
        drain(halves(p, n), w_part.at[p], own)
        drain(halves(p, n - 1), w_part.at[p], apart)
    drain(xbuf.at[pl.ds(0, nx * rows)], x_send, own)
    drain(xbuf.at[pl.ds(0, (nx + 1) * rows)], x_send, apart)
    drain(xbuf.at[pl.ds(0, (m - 2) * rows)], x_fwd, apart)
    drain(rsbuf.at[:, pl.ds(0, m - 1)], r_send, own)
    drain(rsbuf, r_send, apart)
    for copy, condition in started:
        guarded(condition, copy.wait_send)


def body(
    n,
    m,
    tokens,
    pre_gain,
    w_query_ret,
    w_key_ret,
    w_value_ret,
    w_query_att,
    w_key_att,
    w_value_att,
    w_out_ret,
    w_out_att,
    retain_log,
    forget_total,
):
    rows, depth = tokens.shape
    tok = rows * m
    heads = retain_log.shape[1]
    nh, nx = n // 4, m // 2
    half = HEAD // 2
    inverse = np.float32(THETA) ** (-np.arange(half, dtype=np.float32) / np.float32(half))
    angles = np.arange(n * tok, dtype=np.float32)[:, None] * inverse[None, :]
    table = np.concatenate([np.cos(angles), np.sin(angles)], axis=1).astype(np.float32)
    wide_a = 2 * HEAD + heads * HEAD
    wide_b, wide_c = 2 * heads * HEAD, heads * HEAD
    deep = w_key_ret.shape[0]
    deep_o = w_out_ret.shape[0] + w_out_att.shape[0]
    tall = (heads // 2 + 1) * HEAD
    hbm = pl.BlockSpec(memory_space=pl.ANY)
    vmem = pl.BlockSpec(memory_space=pltpu.VMEM)
    dma = pltpu.SemaphoreType.DMA
    return pl.pallas_call(
        functools.partial(kernel, n, m, heads),
        out_shape=jax.ShapeDtypeStruct((rows, depth), BF16),
        in_specs=[hbm] * 13,
        out_specs=vmem,
        scratch_shapes=[
            pltpu.VMEM(tokens.shape, BF16),
            pltpu.VMEM((tok, HEAD), F32),
            pltpu.VMEM((2,) + retain_log.shape[::-1], F32),
            pltpu.VMEM((2,) + forget_total.shape, F32),
            pltpu.VMEM((tok + rows, depth), BF16),
            pltpu.VMEM((n + 1, wide_a, deep), BF16),
            pltpu.VMEM((n + 1, wide_b, deep), BF16),
            pltpu.VMEM((n + 1, wide_c, deep), BF16),
            pltpu.VMEM((n + 1, deep_o, w_out_ret.shape[1]), BF16),
            pltpu.VMEM((n, tok, 2 * HEAD), BF16),
            pltpu.VMEM((n, tall, 2 * HEAD), BF16),
            pltpu.VMEM((heads, tok, tok), F32),
            pltpu.VMEM((heads * tok, 2 * HEAD), F32),
            pltpu.VMEM((heads * tok, 2 * HEAD), BF16),
            pltpu.VMEM((heads * tok, LANES), F32),
            pltpu.VMEM((n, tok, w_out_ret.shape[1]), BF16),
            pltpu.VMEM((n, m, rows, w_out_ret.shape[1]), BF16),
            pltpu.VMEM((n, tok, w_out_ret.shape[1]), BF16),
            pltpu.VMEM((1, depth), F32),
            dma((9,)),
            dma((2,)),
            dma((2,)),
            dma,
            dma,
            dma((2, TOKEN_CUT)),
            dma,
            dma((len(CUTS),)),
            dma((len(CUTS),)),
            *[dma((n, count)) for count in CUTS],
            dma((len(CUTS) - 1,)),
            dma((n,)),
            dma((2, nh - 1)),
            dma((2, nh)),
            dma((2, nh, 2)),
            dma((2, n)),
            dma,
            dma((n,)),
            dma((n,)),
        ],
        compiler_params=pltpu.CompilerParams(
            collective_id=0, has_side_effects=True, vmem_limit_bytes=60 * 1024 * 1024
        ),
    )(
        tokens,
        pre_gain[None, :],
        w_query_ret.T,
        w_key_ret.T,
        w_value_ret.T,
        w_query_att.T,
        w_key_att.T,
        w_value_att.T,
        w_out_ret,
        w_out_att,
        jnp.asarray(table),
        retain_log.T,
        forget_total,
    )


def rotate(field, positions):
    half = field.shape[-1] // 2
    inverse = THETA ** (-jnp.arange(half, dtype=jnp.float32) / half)
    angles = positions[:, None] * inverse[None, :]
    cosine = jnp.cos(angles)[:, None, :]
    sine = jnp.sin(angles)[:, None, :]
    first_half = field[..., :half]
    second_half = field[..., half:]
    return jnp.concatenate(
        [first_half * cosine - second_half * sine, first_half * sine + second_half * cosine],
        axis=-1,
    )


def head_norm(values):
    centre = jnp.mean(values, axis=-1, keepdims=True)
    spread = jnp.mean(jnp.square(values - centre), axis=-1, keepdims=True)
    return (values - centre) * lax.rsqrt(spread + EPS)


def advance(state, pair):
    decay, update = pair
    return (jnp.exp(decay)[:, None, None] * state + update, state)


def plain_body(
    tokens,
    pre_gain,
    w_query_ret,
    w_key_ret,
    w_value_ret,
    w_query_att,
    w_key_att,
    w_value_att,
    w_out_ret,
    w_out_att,
    retain_log,
    forget_total,
):
    rows = tokens.astype(jnp.float32)
    normed = (
        rows * lax.rsqrt(jnp.mean(rows * rows, axis=-1, keepdims=True) + EPS) * pre_gain
    ).astype(jnp.bfloat16)
    gathered = lax.all_gather(normed, "tp", axis=0, tiled=True)
    tok_dev = gathered.shape[0]
    offset = lax.axis_index("sp") * tok_dev
    query_places = offset + jnp.arange(tok_dev, dtype=jnp.int32)
    positions = query_places.astype(jnp.float32)

    def blocked(values):
        return values.reshape((tok_dev // SPAN, SPAN) + values.shape[1:])

    pieces = (
        lax.all_gather(w_query_ret, "sp", axis=0, tiled=True),
        lax.all_gather(w_key_ret, "sp", axis=0, tiled=True),
        lax.all_gather(w_value_ret, "sp", axis=0, tiled=True),
        lax.all_gather(w_query_att, "sp", axis=0, tiled=True),
        lax.all_gather(w_key_att, "sp", axis=0, tiled=True),
        lax.all_gather(w_value_att, "sp", axis=0, tiled=True),
    )
    projected = tuple(
        (jnp.dot(gathered, piece, preferred_element_type=jnp.float32) for piece in pieces)
    )
    heads = retain_log.shape[1]
    shape = (tok_dev, heads, HEAD)
    query = blocked(
        (rotate(projected[0].reshape(shape), positions) * HEAD ** (-0.5)).astype(jnp.bfloat16)
    )
    key_rows = blocked(rotate(projected[1].reshape(shape), positions).astype(jnp.bfloat16))
    value_rows = blocked(projected[2].astype(jnp.bfloat16).reshape(shape))
    within = jnp.cumsum(blocked(retain_log), axis=1)
    causal = jnp.arange(SPAN)[:, None] >= jnp.arange(SPAN)[None, :]
    scores = jnp.einsum("bthd,bshd->bhts", query, key_rows, preferred_element_type=jnp.float32)
    turned = jnp.transpose(within, (0, 2, 1))
    gap = jnp.where(causal, turned[:, :, :, None] - turned[:, :, None, :], 0.0)
    weights = jnp.where(causal, scores * jnp.exp(gap), 0.0).astype(jnp.bfloat16)
    local = jnp.einsum("bhts,bshd->bthd", weights, value_rows, preferred_element_type=jnp.float32)
    last = within[:, -1]
    faded = (key_rows.astype(jnp.float32) * jnp.exp(last[:, None, :] - within)[..., None]).astype(
        jnp.bfloat16
    )
    updates = jnp.einsum("bshd,bshe->bhde", faded, value_rows, preferred_element_type=jnp.float32)
    zero_state = jnp.zeros((heads, HEAD, HEAD), jnp.float32)
    final, _ = lax.scan(advance, zero_state, (last, updates))
    decay_total = jnp.sum(last, axis=0)
    own_state = final.reshape(heads, HEAD * HEAD)
    every_total = lax.all_gather(
        decay_total[None].astype(jnp.bfloat16), "sp", axis=0, tiled=True
    ).astype(jnp.float32)
    every_state = lax.all_gather(
        own_state[None].astype(jnp.bfloat16), "sp", axis=0, tiled=True
    ).astype(jnp.float32)
    device_order = jnp.arange(every_total.shape[0], dtype=jnp.int32)[:, None]
    earlier = device_order < lax.axis_index("sp")
    before = jnp.sum(jnp.where(earlier, every_total, 0.0), axis=0)
    through = jnp.cumsum(every_total, axis=0)
    fading = jnp.where(earlier, jnp.exp(jnp.where(earlier, before[None, :] - through, 0.0)), 0.0)
    incoming = jnp.einsum("jh,jhe->he", fading, every_state, precision=HIGH)
    _, befores = lax.scan(advance, incoming.reshape(heads, HEAD, HEAD), (last, updates))
    lifted = (query.astype(jnp.float32) * jnp.exp(within)[..., None]).astype(jnp.bfloat16)
    carried = jnp.einsum(
        "bthd,bhde->bthe", lifted, befores.astype(jnp.bfloat16), preferred_element_type=jnp.float32
    )
    retained = (
        head_norm((local + carried).reshape(shape))
        .astype(jnp.bfloat16)
        .reshape(tok_dev, heads * HEAD)
    )
    raw_key = projected[4]
    gate_heads = forget_total.shape[0]
    kv_local = raw_key.shape[1] // HEAD
    group = gate_heads // kv_local
    query = (
        (projected[3] * HEAD ** (-0.5)).astype(jnp.bfloat16).reshape(tok_dev, kv_local, group, HEAD)
    )
    key_rows = raw_key.astype(jnp.bfloat16)
    value_rows = projected[5].astype(jnp.bfloat16)
    gate_rows = lax.dynamic_slice_in_dim(forget_total, offset, tok_dev, 1).reshape(
        kv_local, group, tok_dev
    )
    last_row = offset + tok_dev - 1
    init = (
        jnp.zeros((kv_local, group, tok_dev, HEAD), jnp.float32),
        jnp.zeros((kv_local, group, tok_dev), jnp.float32),
    )
    key_piece = lax.all_gather(key_rows, "sp", axis=0, tiled=True)
    value_piece = lax.all_gather(value_rows, "sp", axis=0, tiled=True)
    count = key_piece.shape[0] // KEY_SPAN

    def one_block(index, inner):
        first = index * KEY_SPAN

        def compute(state):
            weighted, total = state
            key_block = lax.dynamic_slice_in_dim(key_piece, index * KEY_SPAN, KEY_SPAN, 0).reshape(
                KEY_SPAN, kv_local, HEAD
            )
            value_block = lax.dynamic_slice_in_dim(
                value_piece, index * KEY_SPAN, KEY_SPAN, 0
            ).reshape(KEY_SPAN, kv_local, HEAD)
            gate_keys = lax.dynamic_slice_in_dim(forget_total, first, KEY_SPAN, 1).reshape(
                kv_local, group, KEY_SPAN
            )
            scores = jnp.einsum(
                "tcgd,scd->cgts", query, key_block, preferred_element_type=jnp.float32
            )
            logits = scores + gate_rows[:, :, :, None] - gate_keys[:, :, None, :]
            allowed = (first + jnp.arange(KEY_SPAN, dtype=jnp.int32))[None, :] <= query_places[
                :, None
            ]
            weights = jnp.exp(jnp.where(allowed, logits, -jnp.inf))
            total = total + jnp.sum(weights, axis=-1)
            weighted = weighted + jnp.einsum(
                "cgts,scd->cgtd",
                weights.astype(jnp.bfloat16),
                value_block,
                preferred_element_type=jnp.float32,
            )
            return (weighted, total)

        def skipped(state):
            return state

        return lax.cond(first <= last_row, compute, skipped, inner)

    weighted, total = lax.fori_loop(0, count, one_block, init)
    result = weighted / total[..., None]
    attended = (
        jnp.transpose(result, (2, 0, 1, 3)).reshape(tok_dev, gate_heads * HEAD).astype(jnp.bfloat16)
    )
    out_ret, out_att = (
        lax.all_gather(w_out_ret, "sp", axis=1, tiled=True),
        lax.all_gather(w_out_att, "sp", axis=1, tiled=True),
    )
    return lax.psum_scatter(
        (
            jnp.dot(retained, out_ret, preferred_element_type=jnp.float32)
            + jnp.dot(attended, out_att, preferred_element_type=jnp.float32)
        ).astype(jnp.bfloat16),
        "tp",
        scatter_dimension=0,
        tiled=True,
    )


def choose(n, m, *arrays):
    tokens, w_key_ret, w_out_ret = arrays[0], arrays[3], arrays[8]
    whole_tiles = w_out_ret.shape[1] % LANES == 0 and w_key_ret.shape[0] % LANES == 0
    heads = arrays[10].shape[1]
    small = 16 * heads <= HEAD and arrays[7].shape[1] == HEAD and arrays[11].shape[0] == heads
    paired = n % 4 == 0 and n > 4 and m % 2 == 0 and m > 2
    if paired and whole_tiles and small and tokens.shape[0] * m == SPAN:
        return body(n, m, *arrays)
    return plain_body(*arrays)


def solution(mesh):
    return jax.shard_map(
        functools.partial(choose, mesh.shape["sp"], mesh.shape["tp"]),
        mesh=mesh,
        in_specs=(
            P(("sp", "tp"), None),
            P(),
            P("sp", "tp"),
            P("sp", "tp"),
            P("sp", "tp"),
            P("sp", "tp"),
            P("sp", "tp"),
            P("sp", "tp"),
            P("tp", "sp"),
            P("tp", "sp"),
            P("sp", "tp"),
            P("tp", None),
        ),
        out_specs=P(("sp", "tp"), None),
        check_vma=False,
    )
```

```python
import functools

import jax
import jax.numpy as jnp
import numpy as np
from jax import lax
from jax.experimental import pallas as pl
from jax.experimental.pallas import tpu as pltpu
from jax.sharding import PartitionSpec as P

HEAD = 64
EPS = 1e-06
THETA = 10000.0
F32 = jnp.float32
BF16 = jnp.bfloat16
MESH = pl.DeviceIdType.MESH
SPAN = 256
KEY_SPAN = 256
LANES = 128
CUTS = (2, 2, 1, 3)
LOG2E = float(np.log2(np.e))
TOKEN_CUT = 4
HIGH = lax.Precision.HIGHEST


def dot(a, b, dims=((1,), (0,))):
    return lax.dot_general(a, b, (dims, ((), ())), preferred_element_type=F32)


def kernel(
    n,
    m,
    heads,
    tok_hbm,
    gain_hbm,
    wq_ret_hbm,
    wk_ret_hbm,
    wv_ret_hbm,
    wq_att_hbm,
    wk_att_hbm,
    wv_att_hbm,
    wo_ret_hbm,
    wo_att_hbm,
    table_hbm,
    logs_hbm,
    gate_hbm,
    out_ref,
    tokens,
    table,
    lbuf,
    gbuf,
    xbuf,
    abuf,
    bbuf,
    cbuf,
    obuf,
    kvbuf,
    stbuf,
    decay,
    num,
    qbuf,
    cbuf_gate,
    outbuf,
    rsbuf,
    passed,
    mixed,
    gain,
    load,
    small_send,
    small_recv,
    x_send,
    x_fwd,
    x_pass,
    x_other,
    w_out,
    w_part,
    first_a,
    first_b,
    first_c,
    first_o,
    w_second,
    o_second,
    k_send,
    k_y,
    k_part,
    k_recv,
    r_send,
    r_pass,
    r_recv,
):
    s, t = lax.axis_index("sp"), lax.axis_index("tp")
    nh, nx = n // 4, m // 2
    y, zl, zh = s % 2, (s // 2) % 2, s // 4
    c, x = t % 2, t // 2
    own = zl == c
    apart = zl != c

    def sp_of(zh_, zl_, y_):
        return zh_ * 4 + zl_ * 2 + y_

    def tp_of(x_, c_):
        return x_ * 2 + c_

    def device(zh_, zl_, y_, x_, c_):
        return {"sp": sp_of(zh_, zl_, y_), "tp": tp_of(x_, c_)}

    q, g = sp_of(zh, c, y), tp_of(x, zl)
    partner = device(zh, zl, y, x, 1 - c)
    across = device(zh, zl, 1 - y, x, c)
    rows = tokens.shape[0]
    tok = rows * m
    width = heads * HEAD
    half_o = wo_ret_hbm.shape[0]

    slot = jnp.where(own, s, n)
    piece = jnp.where(own, t, m)
    groups = (
        (tokens, ((tok_hbm, tokens),)),
        (gain, ((gain_hbm, gain),)),
        (abuf.at[slot], (
            (wk_att_hbm, abuf.at[slot, pl.ds(0, HEAD)]),
            (wv_att_hbm, abuf.at[slot, pl.ds(HEAD, HEAD)]),
            (wq_att_hbm, abuf.at[slot, pl.ds(2 * HEAD, width)]),
        )),
        (bbuf.at[slot], (
            (wk_ret_hbm, bbuf.at[slot, pl.ds(0, width)]),
            (wv_ret_hbm, bbuf.at[slot, pl.ds(width, width)]),
        )),
        (cbuf.at[slot], ((wq_ret_hbm, cbuf.at[slot]),)),
        (obuf.at[slot], (
            (wo_ret_hbm, obuf.at[slot, pl.ds(0, half_o)]),
            (wo_att_hbm, obuf.at[slot, pl.ds(half_o, wo_att_hbm.shape[0])]),
        )),
        (table, ((table_hbm.at[pl.ds(pl.multiple_of(q * tok, tok), tok)], table),)),
        (lbuf.at[0], ((logs_hbm, lbuf.at[0]),)),
        (gbuf.at[0], ((gate_hbm, gbuf.at[0]),)),
    )
    loads = []
    for k, (whole, copies) in enumerate(groups):
        for source, target in copies:
            pltpu.make_async_copy(source, target, load.at[k]).start()
        loads.append(pltpu.make_async_copy(whole, whole, load.at[k]))

    stbuf[...] = jnp.zeros_like(stbuf)
    barrier = pltpu.get_barrier_semaphore()
    greeted = [
        device((zh + i) % nh, zl, 1 - y, x, (c + k) % 2) for i in range(nh) for k in range(2)
    ]
    for i in reversed(range(nh)):
        for j in reversed(range(2)):
            for k in range(2):
                if i or j or k:
                    greeted.append(device((zh + i) % nh, (zl + j) % 2, y, x, (c + k) % 2))
    for r in range(1, nx):
        for j in range(2):
            for k in range(2):
                greeted.append(device(zh, (zl + j) % 2, y, (x + r) % nx, (c + k) % 2))
    for other in greeted:
        pl.semaphore_signal(barrier, inc=1, device_id=other, device_id_type=MESH)

    started = []

    def guarded(condition, action):
        if condition is None:
            action()
        else:
            pl.when(condition)(action)

    def send(source, target, send_sem, recv_sem, where, condition=None, kept=True):
        copy = pltpu.make_async_remote_copy(
            src_ref=source, dst_ref=target, send_sem=send_sem, recv_sem=recv_sem,
            device_id=where, device_id_type=MESH,
        )
        guarded(condition, copy.start)
        if kept:
            started.append((copy, condition))

    def drain(source, send_sem, condition=None):
        started.append((
            pltpu.make_async_remote_copy(
                src_ref=source, dst_ref=source, send_sem=send_sem, recv_sem=send_sem,
                device_id=partner, device_id_type=MESH,
            ),
            condition,
        ))

    def receive(target, recv_sem, condition=None):
        copy = pltpu.make_async_remote_copy(
            src_ref=target, dst_ref=target, send_sem=recv_sem, recv_sem=recv_sem,
            device_id=partner, device_id_type=MESH,
        )
        guarded(condition, copy.wait_recv)

    for copy in loads[:2]:
        copy.wait()
    values = tokens[...].astype(F32)
    scale = lax.rsqrt(jnp.mean(values * values, axis=-1, keepdims=True) + EPS)
    xbuf[pl.ds(pl.multiple_of(piece * rows, rows), rows), :] = (
        values * scale * gain[...]
    ).astype(BF16)
    for copy in loads[2:]:
        copy.wait()
    pl.semaphore_wait(barrier, len(greeted))

    parts = (abuf, bbuf, cbuf, obuf)
    cuts = CUTS

    def chunk(p, index, k, u):
        length = parts[p].shape[1] // (2 * cuts[p])
        start = pl.multiple_of((k * cuts[p] + u) * length, length)
        return parts[p].at[index, pl.ds(start, length)]

    firsts = (first_a, first_b, first_c, first_o)

    def second(p, index):
        return o_second.at[index] if p == 3 else w_second.at[p]

    def halves(p, count):
        return parts[p].at[pl.ds(0, count), pl.ds(0, parts[p].shape[1] // 2)]

    def scatter_one(p, i, k, u, condition):
        core = (c + k) % 2
        send(
            chunk(p, slot, core, u), chunk(p, s, core, u), w_out.at[p], firsts[p].at[s, u],
            device((zh + i) % nh, c, y, x, core), condition, False,
        )

    def scatter_chip(p):
        for u in range(cuts[p]):
            scatter_one(p, 0, 1, u, own)

    def scatter_near(p, u, also=True):
        for k in range(2):
            scatter_one(p, 0, k, u, apart & also)

    def scatter_far(p, u, condition=None):
        for i in range(1, nh):
            for k in range(2):
                scatter_one(p, i, k, u, condition)

    middle = zl != zh % 2
    outer = zl == zh % 2

    def entry(p, i, j, u, condition=None):
        index = sp_of((zh + i) % nh, (zl + j) % 2, y)
        here = i == 0 and j == 0
        spot = chunk(p, index, c, u)
        receive(spot, firsts[p].at[index, u], apart if here else condition)
        send(spot, spot, w_out.at[p], firsts[p].at[index, u], across, condition, False)
        send(
            spot, spot, w_part.at[p], second(p, index), partner,
            own if here else condition, False,
        )

    def beside(p, i, j, u):
        index = sp_of((zh + i) % nh, (zl + j) % 2, 1 - y)
        spot = chunk(p, index, c, u)
        receive(spot, firsts[p].at[index, u])
        send(spot, spot, w_part.at[p], second(p, index), partner, None, False)

    def rest(p):
        receive(halves(p, n - 1), w_second.at[p], own)
        receive(halves(p, n), w_second.at[p], apart)

    far = [(i, j) for i in range(1, nh) for j in range(2)]
    near = (0, 1)
    pieces = x_pass.shape[1]

    def rows_of(index, u):
        length = rows // pieces
        return xbuf.at[pl.ds(pl.multiple_of((index * pieces + u) * length, length), length)]

    def pass_tokens(k, u):
        core = (c + k) % 2
        index = tp_of(x, core)
        spot = rows_of(index, u)
        receive(spot, x_pass.at[core, u], apart if k == 0 else None)
        for r in range(1, nx):
            send(
                spot, spot, x_fwd, x_other, device(zh, zl, y, (x + r) % nx, c), apart, False,
            )

    send(
        lbuf.at[0], lbuf.at[1], small_send.at[0], small_recv.at[0],
        device(zh, c, y, x, zl), apart,
    )
    send(gbuf.at[0], gbuf.at[1], small_send.at[1], small_recv.at[1], partner, own)
    for u in range(cuts[0]):
        scatter_far(0, u)
    scatter_chip(0)
    def give_tokens(u):
        ours, there = rows_of(piece, u), rows_of(t, u)
        send(ours, there, x_send, x_pass.at[c, u], device(zh, 1 - zl, y, x, zl), None, False)
        for r in range(1, nx):
            send(
                ours, there, x_send, x_other, device(zh, zl, y, (x + r) % nx, zl), None, False,
            )
        send(ours, there, x_send, x_pass.at[c, u], device(zh, zl, y, x, zl), apart, False)

    for u in range(pieces // 2):
        give_tokens(u)
    for u in range(cuts[0]):
        scatter_near(0, u)
    for u in range(pieces // 2, pieces):
        give_tokens(u)
    for p in range(1, 4):
        scatter_chip(p)
    for p in range(1, 3):
        for u in range(cuts[p]):
            scatter_far(p, u)
            scatter_near(p, u)
    for p in range(4):
        for u in range(cuts[p]):
            entry(p, 0, 0, u)
    lines = lax.broadcasted_iota(jnp.int32, (tok, tok), 0)
    lanes = lax.broadcasted_iota(jnp.int32, (tok, tok), 1)
    causal = lines >= lanes
    upto = jnp.where(lines <= lanes, 1.0, 0.0)
    receive(lbuf.at[1], small_recv.at[0], apart)
    receive(gbuf.at[1], small_recv.at[1], apart)
    pick = jnp.where(own, 0, 1)
    logs = jnp.concatenate([lbuf[pick], jnp.zeros((8 - heads, tok), F32)], axis=0)
    turned = lax.dot_general(
        logs, upto, (((1,), (0,)), ((), ())),
        preferred_element_type=F32, precision=lax.Precision.HIGHEST,
    )
    fill = jnp.zeros((LANES - 8, tok), F32)
    within = jnp.concatenate([turned, fill], axis=0).T
    gates_own = gbuf[pick, :, pl.ds(pl.multiple_of(q * tok, tok), tok)]
    gate_col = jnp.concatenate(
        [gates_own, jnp.zeros((LANES - heads, tok), F32)], axis=0
    ).T
    cosine, sine = table[:, : HEAD // 2], table[:, HEAD // 2 :]
    for h in range(heads):
        gap = jnp.where(causal, within[:, h : h + 1] - turned[h : h + 1, :], 0.0)
        decay[h] = jnp.where(causal, jnp.exp(gap), 0.0)

    for u in range(cuts[0]):
        beside(0, 0, 0, u)
    for a in far:
        entry(0, *a, 0)
    for u in range(pieces // 2):
        for k in range(2):
            pass_tokens(k, u)
    for u in range(cuts[1]):
        beside(1, 0, 0, u)
    for u in range(1, cuts[0]):
        for a in far:
            entry(0, *a, u)
    for a in far:
        beside(0, *a, 0)
    for u in range(cuts[0]):
        entry(0, *near, u)
    for u in range(pieces // 2, pieces):
        for k in range(2):
            pass_tokens(k, u)
    for a in far:
        entry(1, *a, 0, middle)
    for u in range(1, cuts[0]):
        for a in far:
            beside(0, *a, u)
    for p in range(2, 4):
        for u in range(cuts[p]):
            beside(p, 0, 0, u)
    for u in range(cuts[0]):
        beside(0, *near, u)
    for u in range(1, cuts[1]):
        for a in far:
            entry(1, *a, u, middle)
    for a in far:
        entry(1, *a, 0, outer)

    receive(xbuf.at[pl.ds(0, (m - 2) * rows)], x_other)
    rest(0)

    def exchange(buf, e, index, sem, where, condition):
        send(buf.at[index], buf.at[index], sem, k_recv.at[e, index], where, condition)

    def arrive(buf, e, index, condition):
        receive(buf.at[index], k_recv.at[e, index], condition)

    def exchange_send(buf, e):
        for i in range(1, nh):
            exchange(
                buf, e, q, k_send.at[e, i - 1], device((zh + i) % nh, zl, y, x, c), zh + i < nh
            )
        exchange(buf, e, q, k_y.at[e, 0], across, c + y < 2)
        exchange(buf, e, q, k_part.at[e, 0, 0], partner, c == 0)

    def exchange_across(buf, e):
        index = sp_of(zh, c, 1 - y)
        arrive(buf, e, index, c <= y)
        exchange(buf, e, index, k_part.at[e, 0, 1], partner, c == 0)

    def exchange_part(buf, e):
        for k in range(2):
            arrive(buf, e, sp_of(zh, 1 - c, (y + k) % 2), c == 1)

    def exchange_far(buf, e, also=True):
        for i in range(1, nh):
            index = sp_of((zh + nh - i) % nh, c, y)
            condition = (zh >= i) & also
            arrive(buf, e, index, condition)
            exchange(buf, e, index, k_y.at[e, i], across, condition)
            exchange(buf, e, index, k_part.at[e, i, 0], partner, condition)

    def exchange_far_across(buf, e):
        for i in range(1, nh):
            index = sp_of((zh + nh - i) % nh, c, 1 - y)
            arrive(buf, e, index, zh >= i)
            exchange(buf, e, index, k_part.at[e, i, 1], partner, zh >= i)

    def exchange_far_part(buf, e):
        for i in range(1, nh):
            for k in range(2):
                arrive(buf, e, sp_of((zh + nh - i) % nh, 1 - c, (y + k) % 2), zh >= i)

    def rope(field):
        first, second = field[:, : HEAD // 2], field[:, HEAD // 2 :]
        return jnp.concatenate(
            [first * cosine - second * sine, first * sine + second * cosine], axis=-1
        )

    def project(buf):
        deep = buf.shape[2]
        return sum(
            dot(xbuf[:tok, k * deep : (k + 1) * deep], buf[k], ((1,), (1,))) for k in range(n)
        )

    proj = project(abuf)
    kvbuf[q] = proj[:, : 2 * HEAD].astype(BF16)
    exchange_send(kvbuf, 0)
    scatter_far(3, 0)
    scatter_near(3, 0)
    for u in range(1, cuts[3]):
        scatter_far(3, u, zh == nh - 1)
    wide = heads * tok
    zeros = jnp.zeros((tok, HEAD), F32)
    for h in range(heads):
        query = proj[:, (2 + h) * HEAD : (3 + h) * HEAD] * (HEAD ** (-0.5) * LOG2E)
        qbuf[h * tok : (h + 1) * tok, :] = jnp.concatenate([query, zeros], axis=1).astype(BF16)
        cbuf_gate[h * tok : (h + 1) * tok, :] = jnp.broadcast_to(
            gate_col[:, h : h + 1] * LOG2E, (tok, LANES)
        )
    low_lanes = lax.broadcasted_iota(jnp.int32, (tok, 2 * HEAD), 1) < HEAD

    def attend(indices, masked=False):
        total = None if masked else num[...]
        for index in indices:
            block = kvbuf[index]
            values = jnp.where(low_lanes, jnp.ones_like(block), block)
            gates = gbuf[pick, :, pl.ds(pl.multiple_of(index * tok, tok), tok)] * LOG2E
            logits = dot(qbuf[...], block, ((1,), (1,)))
            column = cbuf_gate[...]
            column = jnp.concatenate([column] * (tok // LANES), axis=1)
            pieces_ = []
            for h in range(heads):
                part = slice(h * tok, (h + 1) * tok)
                shifted = logits[part] + column[part] - gates[h : h + 1, :]
                if masked:
                    shifted = jnp.where(causal, shifted, -jnp.inf)
                pieces_.append(jnp.exp2(shifted).astype(BF16))
            term = dot(jnp.concatenate(pieces_, axis=0), values)
            total = term if total is None else total + term
        num[...] = total

    for u in range(1, cuts[1]):
        for a in far:
            entry(1, *a, u, outer)
    attend([q], True)
    for a in far:
        beside(1, *a, 0)
    for u in range(cuts[1]):
        entry(1, *near, u)
    exchange_across(kvbuf, 0)
    exchange_part(kvbuf, 0)
    index = sp_of(zh, 0, 0)
    pl.when(index < q)(functools.partial(attend, [index]))
    pl.when(index + 1 < q)(functools.partial(attend, [index + 1]))
    for u in range(1, cuts[1]):
        for a in far:
            beside(1, *a, u)
    for u in range(cuts[2]):
        for a in far:
            entry(2, *a, u)
    pl.when(index + 2 < q)(functools.partial(attend, [index + 2]))
    for u in range(cuts[1]):
        beside(1, *near, u)
    for u in range(cuts[2]):
        entry(2, *near, u)
    exchange_far(kvbuf, 0)
    rest(1)
    proj = project(bbuf)
    keys, vals, updates, marks = [], [], [], []
    for h in range(heads):
        base = h * HEAD
        key = rope(proj[:, base : base + HEAD]).astype(BF16)
        val = proj[:, base + width : base + width + HEAD].astype(BF16)
        column = within[:, h : h + 1]
        last = column[tok - 1 :, :]
        faded = (key.astype(F32) * jnp.exp(last - column)).astype(BF16)
        updates.append(dot(faded, val, ((0,), (0,))))
        high = last.astype(BF16).astype(F32)
        low = last - high
        marks.append(jnp.broadcast_to(high, (8, HEAD)))
        marks.append(jnp.broadcast_to(low, (8, HEAD)))
        keys.append(key)
        vals.append(val)
    marks.append(jnp.zeros((HEAD - 16 * heads, HEAD), F32))
    blocks = updates + [jnp.concatenate(marks, axis=0)]
    if len(blocks) % 2:
        blocks.append(jnp.zeros((HEAD, HEAD), F32))
    for k in range(0, len(blocks), 2):
        both = jnp.concatenate(blocks[k : k + 2], axis=1).astype(BF16)
        stbuf[q, k // 2 * HEAD : (k // 2 + 1) * HEAD, :] = both

    def piece_of(index, k):
        spot = slice(k % 2 * HEAD, (k % 2 + 1) * HEAD)
        return stbuf[index, k // 2 * HEAD : (k // 2 + 1) * HEAD, spot].astype(F32)

    exchange_send(stbuf, 1)
    for u in range(1, cuts[3]):
        scatter_near(3, u)
    for u in range(1, cuts[3]):
        scatter_far(3, u, zh < nh - 1)
    for a in far:
        entry(3, *a, 0)
    for u in range(cuts[2]):
        for a in far:
            beside(2, *a, u)
        beside(2, *near, u)
    exchange_far_across(kvbuf, 0)
    exchange_far(stbuf, 1, zl <= c)
    entry(3, *near, 0)
    rest(2)

    proj = project(cbuf)
    local, lifts = [], []
    for h in range(heads):
        query = (rope(proj[:, h * HEAD : (h + 1) * HEAD]) * HEAD ** (-0.5)).astype(BF16)
        column = within[:, h : h + 1]
        scores = dot(query, keys[h], ((1,), (1,)))
        weights = (scores * decay[h]).astype(BF16)
        local.append(dot(weights, vals[h]))
        lifts.append((query.astype(F32) * jnp.exp(column)).astype(BF16))
    exchange_far(stbuf, 1, zl > c)
    for u in range(1, cuts[3]):
        entry(3, *near, u)
    exchange_far_part(kvbuf, 0)

    def attend_far(half):
        for i in range(1, nh):
            index = sp_of((zh + nh - i) % nh, 0, 0) + 2 * half
            pl.when(zh >= i)(functools.partial(attend, [index, index + 1]))

    exchange_across(stbuf, 1)
    attend_far(0)
    attend_far(1)
    for h in range(heads):
        both = num[h * tok : (h + 1) * tok, :]
        mixed[:, width + h * HEAD : width + (h + 1) * HEAD] = (
            both[:, HEAD:] / both[:, :HEAD]
        ).astype(BF16)
    exchange_far_across(stbuf, 1)
    for u in range(1, cuts[3]):
        for a in far:
            entry(3, *a, u)
    exchange_part(stbuf, 1)
    exchange_far_part(stbuf, 1)
    states = [jnp.zeros((HEAD, HEAD), F32)] * heads
    for j in range(n - 1):
        marked = piece_of(j, heads)
        for h in range(heads):
            total = marked[16 * h : 16 * h + 1] + marked[16 * h + 8 : 16 * h + 9]
            moved = jnp.exp(total) * states[h] + piece_of(j, h)
            states[h] = jnp.where(q > j, moved, states[h])
    retained = []
    for h in range(heads):
        raw = local[h] + dot(lifts[h], states[h].astype(BF16))
        centre = jnp.mean(raw, axis=-1, keepdims=True)
        spread = jnp.mean(jnp.square(raw - centre), axis=-1, keepdims=True)
        retained.append(((raw - centre) * lax.rsqrt(spread + EPS)).astype(BF16))
    mixed[:, :width] = jnp.concatenate(retained, axis=-1)
    order = [(i, j) for i in range(nh) for j in range(2)]

    pair = 2 * rows
    pair_here = pl.ds(pl.multiple_of(x * pair, pair), pair)

    def slice_of(i, j, l):
        return sp_of((zh + i) % nh, (zl + j) % 2, (y + l) % 2)

    def multiply(i, j, l):
        index = slice_of(i, j, l)
        receive(
            halves(3, 1), o_second.at[index], apart if i == 0 and j == 0 and l == 0 else None
        )
        outbuf[index] = dot(mixed[...], obuf[index]).astype(BF16)
        return index

    def give(index, spot, x_, c_, condition):
        where = tp_of(x_, c_)
        rows_there = pl.ds(pl.multiple_of(where * rows, rows), rows)
        send(
            outbuf.at[index, rows_there], rsbuf.at[index, spot], r_send, r_recv.at[index],
            device(zh, c, y, x_, c_), condition, False,
        )

    def produce(i, j, l):
        index = multiply(i, j, l)
        for r in reversed(range(nx)):
            for k in range(2):
                give(
                    index, g, (x + r) % nx, (c + k) % 2, apart if r == 0 and k == 0 else None
                )

    def start_pair(i, j):
        index = multiply(i, j, 0)
        if i % 2:
            send(
                outbuf.at[index], passed.at[index], r_send, r_pass.at[index],
                device(zh, 1 - zl, y, x, c), apart, False,
            )
        else:
            for r in range(1, nx):
                other = (x + r) % nx
                send(
                    outbuf.at[index, pl.ds(pl.multiple_of(other * pair, pair), pair)],
                    passed.at[index, pl.ds((r - 1) * pair, pair)], r_send, r_pass.at[index],
                    device(zh, zl, y, other, c), None, False,
                )

    def finish_pair(i, j):
        index = slice_of(i, j, 0)
        if i % 2:
            receive(passed.at[index], r_pass.at[index], own)

            def merge():
                outbuf[index] = (
                    outbuf[index].astype(F32) + passed[index].astype(F32)
                ).astype(BF16)

            pl.when(own)(merge)
            for r in reversed(range(nx)):
                for k in range(2):
                    if r or k:
                        give(index, x, (x + r) % nx, (c + k) % 2, own)
        else:
            receive(passed.at[index, pl.ds(0, (nx - 1) * pair)], r_pass.at[index])
            total = outbuf[index, pair_here].astype(F32)
            for r in range(1, nx):
                total = total + passed[index, (r - 1) * pair : r * pair].astype(F32)
            outbuf[index, pair_here] = total.astype(BF16)
            for k in (1, 0):
                give(index, zl, x, (c + k) % 2, None if k else apart)

    order = [(i, j) for i in range(nh) for j in range(2)]
    for i, j in order:
        start_pair(i, j)
    for u in range(cuts[3]):
        beside(3, *near, u)
    for i, j in order[:2]:
        produce(i, j, 1)
    for u in range(cuts[3]):
        for a in far:
            beside(3, *a, u)
    for i, j in order:
        if i % 2 == 0:
            finish_pair(i, j)
    for i, j in order[2:]:
        produce(i, j, 1)
    for i, j in order:
        if i % 2:
            finish_pair(i, j)
    columns = obuf.shape[2]
    for l in range(2):
        for i, j in order:
            index = slice_of(i, j, l)
            if l:
                spot, count = g, m
            elif i % 2:
                spot, count = x, nx
            else:
                spot, count = zl, 2

            def keep(index=index, spot=spot):
                rsbuf[index, spot] = outbuf[index, pl.ds(pl.multiple_of(t * rows, rows), rows)]

            receive(rsbuf.at[index, pl.ds(0, count - 1)], r_recv.at[index], own)
            pl.when(own)(keep)
            receive(rsbuf.at[index, pl.ds(0, count)], r_recv.at[index], apart)
            total = rsbuf[index, 0].astype(F32)
            for other in range(1, count):
                total = total + rsbuf[index, other].astype(F32)
            span = pl.ds(pl.multiple_of(index * columns, columns), columns)
            out_ref[:, span] = total.astype(BF16)
    for p in range(4):
        drain(halves(p, n - 1), w_out.at[p], own)
        drain(halves(p, n), w_out.at[p], apart)
        drain(halves(p, n), w_part.at[p], own)
        drain(halves(p, n - 1), w_part.at[p], apart)
    drain(xbuf.at[pl.ds(0, nx * rows)], x_send, own)
    drain(xbuf.at[pl.ds(0, (nx + 1) * rows)], x_send, apart)
    drain(xbuf.at[pl.ds(0, (m - 2) * rows)], x_fwd, apart)
    drain(rsbuf.at[:, pl.ds(0, m - 1)], r_send, own)
    drain(rsbuf, r_send, apart)
    for copy, condition in started:
        guarded(condition, copy.wait_send)


def body(
    n,
    m,
    tokens,
    pre_gain,
    w_query_ret,
    w_key_ret,
    w_value_ret,
    w_query_att,
    w_key_att,
    w_value_att,
    w_out_ret,
    w_out_att,
    retain_log,
    forget_total,
):
    rows, depth = tokens.shape
    tok = rows * m
    heads = retain_log.shape[1]
    nh, nx = n // 4, m // 2
    half = HEAD // 2
    inverse = np.float32(THETA) ** (-np.arange(half, dtype=np.float32) / np.float32(half))
    angles = np.arange(n * tok, dtype=np.float32)[:, None] * inverse[None, :]
    table = np.concatenate([np.cos(angles), np.sin(angles)], axis=1).astype(np.float32)
    wide_a = 2 * HEAD + heads * HEAD
    wide_b, wide_c = 2 * heads * HEAD, heads * HEAD
    deep = w_key_ret.shape[0]
    deep_o = w_out_ret.shape[0] + w_out_att.shape[0]
    tall = (heads // 2 + 1) * HEAD
    hbm = pl.BlockSpec(memory_space=pl.ANY)
    vmem = pl.BlockSpec(memory_space=pltpu.VMEM)
    dma = pltpu.SemaphoreType.DMA
    return pl.pallas_call(
        functools.partial(kernel, n, m, heads),
        out_shape=jax.ShapeDtypeStruct((rows, depth), BF16),
        in_specs=[hbm] * 13,
        out_specs=vmem,
        scratch_shapes=[
            pltpu.VMEM(tokens.shape, BF16),
            pltpu.VMEM((tok, HEAD), F32),
            pltpu.VMEM((2,) + retain_log.shape[::-1], F32),
            pltpu.VMEM((2,) + forget_total.shape, F32),
            pltpu.VMEM((tok + rows, depth), BF16),
            pltpu.VMEM((n + 1, wide_a, deep), BF16),
            pltpu.VMEM((n + 1, wide_b, deep), BF16),
            pltpu.VMEM((n + 1, wide_c, deep), BF16),
            pltpu.VMEM((n + 1, deep_o, w_out_ret.shape[1]), BF16),
            pltpu.VMEM((n, tok, 2 * HEAD), BF16),
            pltpu.VMEM((n, tall, 2 * HEAD), BF16),
            pltpu.VMEM((heads, tok, tok), F32),
            pltpu.VMEM((heads * tok, 2 * HEAD), F32),
            pltpu.VMEM((heads * tok, 2 * HEAD), BF16),
            pltpu.VMEM((heads * tok, LANES), F32),
            pltpu.VMEM((n, tok, w_out_ret.shape[1]), BF16),
            pltpu.VMEM((n, m, rows, w_out_ret.shape[1]), BF16),
            pltpu.VMEM((n, tok, w_out_ret.shape[1]), BF16),
            pltpu.VMEM((tok, 2 * heads * HEAD), BF16),
            pltpu.VMEM((1, depth), F32),
            dma((9,)),
            dma((2,)),
            dma((2,)),
            dma,
            dma,
            dma((2, TOKEN_CUT)),
            dma,
            dma((len(CUTS),)),
            dma((len(CUTS),)),
            *[dma((n, count)) for count in CUTS],
            dma((len(CUTS) - 1,)),
            dma((n,)),
            dma((2, nh - 1)),
            dma((2, nh)),
            dma((2, nh, 2)),
            dma((2, n)),
            dma,
            dma((n,)),
            dma((n,)),
        ],
        compiler_params=pltpu.CompilerParams(
            collective_id=0, has_side_effects=True, vmem_limit_bytes=60 * 1024 * 1024
        ),
    )(
        tokens,
        pre_gain[None, :],
        w_query_ret.T,
        w_key_ret.T,
        w_value_ret.T,
        w_query_att.T,
        w_key_att.T,
        w_value_att.T,
        w_out_ret,
        w_out_att,
        jnp.asarray(table),
        retain_log.T,
        forget_total,
    )


def rotate(field, positions):
    half = field.shape[-1] // 2
    inverse = THETA ** (-jnp.arange(half, dtype=jnp.float32) / half)
    angles = positions[:, None] * inverse[None, :]
    cosine = jnp.cos(angles)[:, None, :]
    sine = jnp.sin(angles)[:, None, :]
    first_half = field[..., :half]
    second_half = field[..., half:]
    return jnp.concatenate(
        [first_half * cosine - second_half * sine, first_half * sine + second_half * cosine],
        axis=-1,
    )


def head_norm(values):
    centre = jnp.mean(values, axis=-1, keepdims=True)
    spread = jnp.mean(jnp.square(values - centre), axis=-1, keepdims=True)
    return (values - centre) * lax.rsqrt(spread + EPS)


def advance(state, pair):
    decay, update = pair
    return (jnp.exp(decay)[:, None, None] * state + update, state)


def plain_body(
    tokens,
    pre_gain,
    w_query_ret,
    w_key_ret,
    w_value_ret,
    w_query_att,
    w_key_att,
    w_value_att,
    w_out_ret,
    w_out_att,
    retain_log,
    forget_total,
):
    rows = tokens.astype(jnp.float32)
    normed = (
        rows * lax.rsqrt(jnp.mean(rows * rows, axis=-1, keepdims=True) + EPS) * pre_gain
    ).astype(jnp.bfloat16)
    gathered = lax.all_gather(normed, "tp", axis=0, tiled=True)
    tok_dev = gathered.shape[0]
    offset = lax.axis_index("sp") * tok_dev
    query_places = offset + jnp.arange(tok_dev, dtype=jnp.int32)
    positions = query_places.astype(jnp.float32)

    def blocked(values):
        return values.reshape((tok_dev // SPAN, SPAN) + values.shape[1:])

    pieces = (
        lax.all_gather(w_query_ret, "sp", axis=0, tiled=True),
        lax.all_gather(w_key_ret, "sp", axis=0, tiled=True),
        lax.all_gather(w_value_ret, "sp", axis=0, tiled=True),
        lax.all_gather(w_query_att, "sp", axis=0, tiled=True),
        lax.all_gather(w_key_att, "sp", axis=0, tiled=True),
        lax.all_gather(w_value_att, "sp", axis=0, tiled=True),
    )
    projected = tuple(
        (jnp.dot(gathered, piece, preferred_element_type=jnp.float32) for piece in pieces)
    )
    heads = retain_log.shape[1]
    shape = (tok_dev, heads, HEAD)
    query = blocked(
        (rotate(projected[0].reshape(shape), positions) * HEAD ** (-0.5)).astype(jnp.bfloat16)
    )
    key_rows = blocked(rotate(projected[1].reshape(shape), positions).astype(jnp.bfloat16))
    value_rows = blocked(projected[2].astype(jnp.bfloat16).reshape(shape))
    within = jnp.cumsum(blocked(retain_log), axis=1)
    causal = jnp.arange(SPAN)[:, None] >= jnp.arange(SPAN)[None, :]
    scores = jnp.einsum("bthd,bshd->bhts", query, key_rows, preferred_element_type=jnp.float32)
    turned = jnp.transpose(within, (0, 2, 1))
    gap = jnp.where(causal, turned[:, :, :, None] - turned[:, :, None, :], 0.0)
    weights = jnp.where(causal, scores * jnp.exp(gap), 0.0).astype(jnp.bfloat16)
    local = jnp.einsum("bhts,bshd->bthd", weights, value_rows, preferred_element_type=jnp.float32)
    last = within[:, -1]
    faded = (key_rows.astype(jnp.float32) * jnp.exp(last[:, None, :] - within)[..., None]).astype(
        jnp.bfloat16
    )
    updates = jnp.einsum("bshd,bshe->bhde", faded, value_rows, preferred_element_type=jnp.float32)
    zero_state = jnp.zeros((heads, HEAD, HEAD), jnp.float32)
    final, _ = lax.scan(advance, zero_state, (last, updates))
    decay_total = jnp.sum(last, axis=0)
    own_state = final.reshape(heads, HEAD * HEAD)
    every_total = lax.all_gather(
        decay_total[None].astype(jnp.bfloat16), "sp", axis=0, tiled=True
    ).astype(jnp.float32)
    every_state = lax.all_gather(
        own_state[None].astype(jnp.bfloat16), "sp", axis=0, tiled=True
    ).astype(jnp.float32)
    device_order = jnp.arange(every_total.shape[0], dtype=jnp.int32)[:, None]
    earlier = device_order < lax.axis_index("sp")
    before = jnp.sum(jnp.where(earlier, every_total, 0.0), axis=0)
    through = jnp.cumsum(every_total, axis=0)
    fading = jnp.where(earlier, jnp.exp(jnp.where(earlier, before[None, :] - through, 0.0)), 0.0)
    incoming = jnp.einsum("jh,jhe->he", fading, every_state, precision=HIGH)
    _, befores = lax.scan(advance, incoming.reshape(heads, HEAD, HEAD), (last, updates))
    lifted = (query.astype(jnp.float32) * jnp.exp(within)[..., None]).astype(jnp.bfloat16)
    carried = jnp.einsum(
        "bthd,bhde->bthe", lifted, befores.astype(jnp.bfloat16), preferred_element_type=jnp.float32
    )
    retained = (
        head_norm((local + carried).reshape(shape))
        .astype(jnp.bfloat16)
        .reshape(tok_dev, heads * HEAD)
    )
    raw_key = projected[4]
    gate_heads = forget_total.shape[0]
    kv_local = raw_key.shape[1] // HEAD
    group = gate_heads // kv_local
    query = (
        (projected[3] * HEAD ** (-0.5)).astype(jnp.bfloat16).reshape(tok_dev, kv_local, group, HEAD)
    )
    key_rows = raw_key.astype(jnp.bfloat16)
    value_rows = projected[5].astype(jnp.bfloat16)
    gate_rows = lax.dynamic_slice_in_dim(forget_total, offset, tok_dev, 1).reshape(
        kv_local, group, tok_dev
    )
    last_row = offset + tok_dev - 1
    init = (
        jnp.zeros((kv_local, group, tok_dev, HEAD), jnp.float32),
        jnp.zeros((kv_local, group, tok_dev), jnp.float32),
    )
    key_piece = lax.all_gather(key_rows, "sp", axis=0, tiled=True)
    value_piece = lax.all_gather(value_rows, "sp", axis=0, tiled=True)
    count = key_piece.shape[0] // KEY_SPAN

    def one_block(index, inner):
        first = index * KEY_SPAN

        def compute(state):
            weighted, total = state
            key_block = lax.dynamic_slice_in_dim(key_piece, index * KEY_SPAN, KEY_SPAN, 0).reshape(
                KEY_SPAN, kv_local, HEAD
            )
            value_block = lax.dynamic_slice_in_dim(
                value_piece, index * KEY_SPAN, KEY_SPAN, 0
            ).reshape(KEY_SPAN, kv_local, HEAD)
            gate_keys = lax.dynamic_slice_in_dim(forget_total, first, KEY_SPAN, 1).reshape(
                kv_local, group, KEY_SPAN
            )
            scores = jnp.einsum(
                "tcgd,scd->cgts", query, key_block, preferred_element_type=jnp.float32
            )
            logits = scores + gate_rows[:, :, :, None] - gate_keys[:, :, None, :]
            allowed = (first + jnp.arange(KEY_SPAN, dtype=jnp.int32))[None, :] <= query_places[
                :, None
            ]
            weights = jnp.exp(jnp.where(allowed, logits, -jnp.inf))
            total = total + jnp.sum(weights, axis=-1)
            weighted = weighted + jnp.einsum(
                "cgts,scd->cgtd",
                weights.astype(jnp.bfloat16),
                value_block,
                preferred_element_type=jnp.float32,
            )
            return (weighted, total)

        def skipped(state):
            return state

        return lax.cond(first <= last_row, compute, skipped, inner)

    weighted, total = lax.fori_loop(0, count, one_block, init)
    result = weighted / total[..., None]
    attended = (
        jnp.transpose(result, (2, 0, 1, 3)).reshape(tok_dev, gate_heads * HEAD).astype(jnp.bfloat16)
    )
    out_ret, out_att = (
        lax.all_gather(w_out_ret, "sp", axis=1, tiled=True),
        lax.all_gather(w_out_att, "sp", axis=1, tiled=True),
    )
    return lax.psum_scatter(
        (
            jnp.dot(retained, out_ret, preferred_element_type=jnp.float32)
            + jnp.dot(attended, out_att, preferred_element_type=jnp.float32)
        ).astype(jnp.bfloat16),
        "tp",
        scatter_dimension=0,
        tiled=True,
    )


def choose(n, m, *arrays):
    tokens, w_key_ret, w_out_ret = arrays[0], arrays[3], arrays[8]
    whole_tiles = w_out_ret.shape[1] % LANES == 0 and w_key_ret.shape[0] % LANES == 0
    heads = arrays[10].shape[1]
    small = 16 * heads <= HEAD and arrays[7].shape[1] == HEAD and arrays[11].shape[0] == heads
    paired = n % 4 == 0 and n > 4 and m % 2 == 0 and m > 2
    if paired and whole_tiles and small and tokens.shape[0] * m == SPAN:
        return body(n, m, *arrays)
    return plain_body(*arrays)


def solution(mesh):
    return jax.shard_map(
        functools.partial(choose, mesh.shape["sp"], mesh.shape["tp"]),
        mesh=mesh,
        in_specs=(
            P(("sp", "tp"), None),
            P(),
            P("sp", "tp"),
            P("sp", "tp"),
            P("sp", "tp"),
            P("sp", "tp"),
            P("sp", "tp"),
            P("sp", "tp"),
            P("tp", "sp"),
            P("tp", "sp"),
            P("sp", "tp"),
            P("tp", None),
        ),
        out_specs=P(("sp", "tp"), None),
        check_vma=False,
    )
```

```python
import functools

import jax
import jax.numpy as jnp
import numpy as np
from jax import lax
from jax.experimental import pallas as pl
from jax.experimental.pallas import tpu as pltpu
from jax.sharding import PartitionSpec as P

HEAD = 64
EPS = 1e-06
THETA = 10000.0
F32 = jnp.float32
BF16 = jnp.bfloat16
MESH = pl.DeviceIdType.MESH
SPAN = 256
KEY_SPAN = 256
LANES = 128
CUTS = (2, 2, 1, 3)
LOG2E = float(np.log2(np.e))
TOKEN_CUT = 4
HIGH = lax.Precision.HIGHEST


def dot(a, b, dims=((1,), (0,))):
    return lax.dot_general(a, b, (dims, ((), ())), preferred_element_type=F32)


def kernel(
    n,
    m,
    heads,
    tok_hbm,
    gain_hbm,
    wq_ret_hbm,
    wk_ret_hbm,
    wv_ret_hbm,
    wq_att_hbm,
    wk_att_hbm,
    wv_att_hbm,
    wo_ret_hbm,
    wo_att_hbm,
    table_hbm,
    logs_hbm,
    gate_hbm,
    out_ref,
    tokens,
    table,
    lbuf,
    gbuf,
    xbuf,
    abuf,
    bbuf,
    cbuf,
    obuf,
    kvbuf,
    stbuf,
    decay,
    num,
    qbuf,
    cbuf_gate,
    outbuf,
    rsbuf,
    passed,
    mixed,
    gain,
    load,
    small_send,
    small_recv,
    x_send,
    x_fwd,
    x_pass,
    x_other,
    w_out,
    w_part,
    first_a,
    first_b,
    first_c,
    first_o,
    w_second,
    o_second,
    k_send,
    k_y,
    k_part,
    k_recv,
    r_send,
    r_pass,
    r_recv,
):
    s, t = lax.axis_index("sp"), lax.axis_index("tp")
    nh, nx = n // 4, m // 2
    y, zl, zh = s % 2, (s // 2) % 2, s // 4
    c, x = t % 2, t // 2
    own = zl == c
    apart = zl != c

    def sp_of(zh_, zl_, y_):
        return zh_ * 4 + zl_ * 2 + y_

    def tp_of(x_, c_):
        return x_ * 2 + c_

    def device(zh_, zl_, y_, x_, c_):
        return {"sp": sp_of(zh_, zl_, y_), "tp": tp_of(x_, c_)}

    q, g = sp_of(zh, c, y), tp_of(x, zl)
    partner = device(zh, zl, y, x, 1 - c)
    across = device(zh, zl, 1 - y, x, c)
    rows = tokens.shape[0]
    tok = rows * m
    width = heads * HEAD
    half_o = wo_ret_hbm.shape[0]

    slot = jnp.where(own, s, n)
    piece = jnp.where(own, t, m)
    groups = (
        (tokens, ((tok_hbm, tokens),)),
        (gain, ((gain_hbm, gain),)),
        (abuf.at[slot], (
            (wk_att_hbm, abuf.at[slot, pl.ds(0, HEAD)]),
            (wv_att_hbm, abuf.at[slot, pl.ds(HEAD, HEAD)]),
            (wq_att_hbm, abuf.at[slot, pl.ds(2 * HEAD, width)]),
        )),
        (bbuf.at[slot], (
            (wk_ret_hbm, bbuf.at[slot, pl.ds(0, width)]),
            (wv_ret_hbm, bbuf.at[slot, pl.ds(width, width)]),
        )),
        (cbuf.at[slot], ((wq_ret_hbm, cbuf.at[slot]),)),
        (obuf.at[slot], (
            (wo_ret_hbm, obuf.at[slot, pl.ds(0, half_o)]),
            (wo_att_hbm, obuf.at[slot, pl.ds(half_o, wo_att_hbm.shape[0])]),
        )),
        (table, ((table_hbm.at[pl.ds(pl.multiple_of(q * tok, tok), tok)], table),)),
        (lbuf.at[0], ((logs_hbm, lbuf.at[0]),)),
        (gbuf.at[0], ((gate_hbm, gbuf.at[0]),)),
    )
    loads = []
    for k, (whole, copies) in enumerate(groups):
        for source, target in copies:
            pltpu.make_async_copy(source, target, load.at[k]).start()
        loads.append(pltpu.make_async_copy(whole, whole, load.at[k]))

    stbuf[...] = jnp.zeros_like(stbuf)
    barrier = pltpu.get_barrier_semaphore()
    greeted = [
        device((zh + i) % nh, zl, 1 - y, x, (c + k) % 2) for i in range(nh) for k in range(2)
    ]
    for i in reversed(range(nh)):
        for j in reversed(range(2)):
            for k in range(2):
                if i or j or k:
                    greeted.append(device((zh + i) % nh, (zl + j) % 2, y, x, (c + k) % 2))
    for r in range(1, nx):
        for j in range(2):
            for k in range(2):
                greeted.append(device(zh, (zl + j) % 2, y, (x + r) % nx, (c + k) % 2))
    for other in greeted:
        pl.semaphore_signal(barrier, inc=1, device_id=other, device_id_type=MESH)

    started = []

    def guarded(condition, action):
        if condition is None:
            action()
        else:
            pl.when(condition)(action)

    def send(source, target, send_sem, recv_sem, where, condition=None, kept=True):
        copy = pltpu.make_async_remote_copy(
            src_ref=source, dst_ref=target, send_sem=send_sem, recv_sem=recv_sem,
            device_id=where, device_id_type=MESH,
        )
        guarded(condition, copy.start)
        if kept:
            started.append((copy, condition))

    def drain(source, send_sem, condition=None):
        started.append((
            pltpu.make_async_remote_copy(
                src_ref=source, dst_ref=source, send_sem=send_sem, recv_sem=send_sem,
                device_id=partner, device_id_type=MESH,
            ),
            condition,
        ))

    def receive(target, recv_sem, condition=None):
        copy = pltpu.make_async_remote_copy(
            src_ref=target, dst_ref=target, send_sem=recv_sem, recv_sem=recv_sem,
            device_id=partner, device_id_type=MESH,
        )
        guarded(condition, copy.wait_recv)

    for copy in loads[:2]:
        copy.wait()
    values = tokens[...].astype(F32)
    scale = lax.rsqrt(jnp.mean(values * values, axis=-1, keepdims=True) + EPS)
    xbuf[pl.ds(pl.multiple_of(piece * rows, rows), rows), :] = (
        values * scale * gain[...]
    ).astype(BF16)
    for copy in loads[2:]:
        copy.wait()
    pl.semaphore_wait(barrier, len(greeted))

    parts = (abuf, bbuf, cbuf, obuf)
    cuts = CUTS

    def chunk(p, index, k, u):
        length = parts[p].shape[1] // (2 * cuts[p])
        start = pl.multiple_of((k * cuts[p] + u) * length, length)
        return parts[p].at[index, pl.ds(start, length)]

    firsts = (first_a, first_b, first_c, first_o)

    def second(p, index):
        return o_second.at[index] if p == 3 else w_second.at[p]

    def halves(p, count):
        return parts[p].at[pl.ds(0, count), pl.ds(0, parts[p].shape[1] // 2)]

    def scatter_one(p, i, k, u, condition):
        core = (c + k) % 2
        send(
            chunk(p, slot, core, u), chunk(p, s, core, u), w_out.at[p], firsts[p].at[s, u],
            device((zh + i) % nh, c, y, x, core), condition, False,
        )

    def scatter_chip(p):
        for u in range(cuts[p]):
            scatter_one(p, 0, 1, u, own)

    def scatter_near(p, u, also=True):
        for k in range(2):
            scatter_one(p, 0, k, u, apart & also)

    def scatter_far(p, u, condition=None):
        for i in range(1, nh):
            for k in range(2):
                scatter_one(p, i, k, u, condition)

    middle = zl != zh % 2
    outer = zl == zh % 2

    def entry(p, i, j, u, condition=None):
        index = sp_of((zh + i) % nh, (zl + j) % 2, y)
        here = i == 0 and j == 0
        spot = chunk(p, index, c, u)
        receive(spot, firsts[p].at[index, u], apart if here else condition)
        send(spot, spot, w_out.at[p], firsts[p].at[index, u], across, condition, False)
        send(
            spot, spot, w_part.at[p], second(p, index), partner,
            own if here else condition, False,
        )

    def beside(p, i, j, u):
        index = sp_of((zh + i) % nh, (zl + j) % 2, 1 - y)
        spot = chunk(p, index, c, u)
        receive(spot, firsts[p].at[index, u])
        send(spot, spot, w_part.at[p], second(p, index), partner, None, False)

    def rest(p):
        receive(halves(p, n - 1), w_second.at[p], own)
        receive(halves(p, n), w_second.at[p], apart)

    far = [(i, j) for i in range(1, nh) for j in range(2)]
    near = (0, 1)
    pieces = x_pass.shape[1]

    def rows_of(index, u):
        length = rows // pieces
        return xbuf.at[pl.ds(pl.multiple_of((index * pieces + u) * length, length), length)]

    def pass_tokens(k, u):
        core = (c + k) % 2
        index = tp_of(x, core)
        spot = rows_of(index, u)
        receive(spot, x_pass.at[core, u], apart if k == 0 else None)
        for r in range(1, nx):
            send(
                spot, spot, x_fwd, x_other, device(zh, zl, y, (x + r) % nx, c), apart, False,
            )

    send(
        lbuf.at[0], lbuf.at[1], small_send.at[0], small_recv.at[0],
        device(zh, c, y, x, zl), apart,
    )
    send(gbuf.at[0], gbuf.at[1], small_send.at[1], small_recv.at[1], partner, own)
    for u in range(cuts[0]):
        scatter_far(0, u)
    scatter_chip(0)
    def give_tokens(u):
        ours, there = rows_of(piece, u), rows_of(t, u)
        send(ours, there, x_send, x_pass.at[c, u], device(zh, 1 - zl, y, x, zl), None, False)
        for r in range(1, nx):
            send(
                ours, there, x_send, x_other, device(zh, zl, y, (x + r) % nx, zl), None, False,
            )
        send(ours, there, x_send, x_pass.at[c, u], device(zh, zl, y, x, zl), apart, False)

    for u in range(pieces // 2):
        give_tokens(u)
    for u in range(cuts[0]):
        scatter_near(0, u)
    for u in range(pieces // 2, pieces):
        give_tokens(u)
    for p in range(1, 4):
        scatter_chip(p)
    for p in range(1, 3):
        for u in range(cuts[p]):
            scatter_far(p, u)
            scatter_near(p, u)
    for p in range(4):
        for u in range(cuts[p]):
            entry(p, 0, 0, u)
    lines = lax.broadcasted_iota(jnp.int32, (tok, tok), 0)
    lanes = lax.broadcasted_iota(jnp.int32, (tok, tok), 1)
    causal = lines >= lanes
    upto = jnp.where(lines <= lanes, 1.0, 0.0)
    receive(lbuf.at[1], small_recv.at[0], apart)
    receive(gbuf.at[1], small_recv.at[1], apart)
    pick = jnp.where(own, 0, 1)
    logs = jnp.concatenate([lbuf[pick], jnp.zeros((8 - heads, tok), F32)], axis=0)
    turned = lax.dot_general(
        logs, upto, (((1,), (0,)), ((), ())),
        preferred_element_type=F32, precision=lax.Precision.HIGHEST,
    )
    fill = jnp.zeros((LANES - 8, tok), F32)
    within = jnp.concatenate([turned, fill], axis=0).T
    gates_own = gbuf[pick, :, pl.ds(pl.multiple_of(q * tok, tok), tok)]
    gate_col = jnp.concatenate(
        [gates_own, jnp.zeros((LANES - heads, tok), F32)], axis=0
    ).T
    cosine, sine = table[:, : HEAD // 2], table[:, HEAD // 2 :]
    for h in range(heads):
        gap = jnp.where(causal, within[:, h : h + 1] - turned[h : h + 1, :], 0.0)
        decay[h] = jnp.where(causal, jnp.exp(gap), 0.0)

    for u in range(cuts[0]):
        beside(0, 0, 0, u)
    for a in far:
        entry(0, *a, 0)
    for u in range(pieces // 2):
        for k in range(2):
            pass_tokens(k, u)
    for u in range(cuts[1]):
        beside(1, 0, 0, u)
    for u in range(1, cuts[0]):
        for a in far:
            entry(0, *a, u)
    for a in far:
        beside(0, *a, 0)
    for u in range(cuts[0]):
        entry(0, *near, u)
    for u in range(pieces // 2, pieces):
        for k in range(2):
            pass_tokens(k, u)
    for a in far:
        entry(1, *a, 0, middle)
    for u in range(1, cuts[0]):
        for a in far:
            beside(0, *a, u)
    for p in range(2, 4):
        for u in range(cuts[p]):
            beside(p, 0, 0, u)
    for u in range(cuts[0]):
        beside(0, *near, u)
    for u in range(1, cuts[1]):
        for a in far:
            entry(1, *a, u, middle)
    for a in far:
        entry(1, *a, 0, outer)

    receive(xbuf.at[pl.ds(0, (m - 2) * rows)], x_other)
    rest(0)

    def exchange(buf, e, index, sem, where, condition):
        send(buf.at[index], buf.at[index], sem, k_recv.at[e, index], where, condition)

    def arrive(buf, e, index, condition):
        receive(buf.at[index], k_recv.at[e, index], condition)

    def exchange_send(buf, e):
        for i in range(1, nh):
            exchange(
                buf, e, q, k_send.at[e, i - 1], device((zh + i) % nh, zl, y, x, c), zh + i < nh
            )
        exchange(buf, e, q, k_y.at[e, 0], across, c + y < 2)
        exchange(buf, e, q, k_part.at[e, 0, 0], partner, c == 0)

    def exchange_across(buf, e):
        index = sp_of(zh, c, 1 - y)
        arrive(buf, e, index, c <= y)
        exchange(buf, e, index, k_part.at[e, 0, 1], partner, c == 0)

    def exchange_part(buf, e):
        for k in range(2):
            arrive(buf, e, sp_of(zh, 1 - c, (y + k) % 2), c == 1)

    def exchange_far(buf, e, also=True):
        for i in range(1, nh):
            index = sp_of((zh + nh - i) % nh, c, y)
            condition = (zh >= i) & also
            arrive(buf, e, index, condition)
            exchange(buf, e, index, k_y.at[e, i], across, condition)
            exchange(buf, e, index, k_part.at[e, i, 0], partner, condition)

    def exchange_far_across(buf, e):
        for i in range(1, nh):
            index = sp_of((zh + nh - i) % nh, c, 1 - y)
            arrive(buf, e, index, zh >= i)
            exchange(buf, e, index, k_part.at[e, i, 1], partner, zh >= i)

    def exchange_far_part(buf, e):
        for i in range(1, nh):
            for k in range(2):
                arrive(buf, e, sp_of((zh + nh - i) % nh, 1 - c, (y + k) % 2), zh >= i)

    def rope(field):
        first, second = field[:, : HEAD // 2], field[:, HEAD // 2 :]
        return jnp.concatenate(
            [first * cosine - second * sine, first * sine + second * cosine], axis=-1
        )

    def project(buf):
        deep = buf.shape[2]
        return sum(
            dot(xbuf[:tok, k * deep : (k + 1) * deep], buf[k], ((1,), (1,))) for k in range(n)
        )

    proj = project(abuf)
    kvbuf[q] = proj[:, : 2 * HEAD].astype(BF16)
    exchange_send(kvbuf, 0)
    scatter_far(3, 0)
    scatter_near(3, 0)
    for u in range(1, cuts[3]):
        scatter_far(3, u, zh == nh - 1)
    wide = heads * tok
    zeros = jnp.zeros((tok, HEAD), F32)
    for h in range(heads):
        query = proj[:, (2 + h) * HEAD : (3 + h) * HEAD] * (HEAD ** (-0.5) * LOG2E)
        qbuf[h * tok : (h + 1) * tok, :] = jnp.concatenate([query, zeros], axis=1).astype(BF16)
        cbuf_gate[h * tok : (h + 1) * tok, :] = jnp.broadcast_to(
            gate_col[:, h : h + 1] * LOG2E, (tok, LANES)
        )
    low_lanes = lax.broadcasted_iota(jnp.int32, (tok, 2 * HEAD), 1) < HEAD

    def attend(indices, masked=False):
        total = None if masked else num[...]
        for index in indices:
            block = kvbuf[index]
            values = jnp.where(low_lanes, jnp.ones_like(block), block)
            gates = gbuf[pick, :, pl.ds(pl.multiple_of(index * tok, tok), tok)] * LOG2E
            logits = dot(qbuf[...], block, ((1,), (1,)))
            column = cbuf_gate[...]
            column = jnp.concatenate([column] * (tok // LANES), axis=1)
            pieces_ = []
            for h in range(heads):
                part = slice(h * tok, (h + 1) * tok)
                shifted = logits[part] + column[part] - gates[h : h + 1, :]
                if masked:
                    shifted = jnp.where(causal, shifted, -jnp.inf)
                pieces_.append(jnp.exp2(shifted).astype(BF16))
            term = dot(jnp.concatenate(pieces_, axis=0), values)
            total = term if total is None else total + term
        num[...] = total

    for u in range(1, cuts[1]):
        for a in far:
            entry(1, *a, u, outer)
    attend([q], True)
    for a in far:
        beside(1, *a, 0)
    for u in range(cuts[1]):
        entry(1, *near, u)
    exchange_across(kvbuf, 0)
    exchange_part(kvbuf, 0)
    index = sp_of(zh, 0, 0)
    pl.when(index < q)(functools.partial(attend, [index]))
    pl.when(index + 1 < q)(functools.partial(attend, [index + 1]))
    for u in range(1, cuts[1]):
        for a in far:
            beside(1, *a, u)
    for u in range(cuts[2]):
        for a in far:
            entry(2, *a, u)
    pl.when(index + 2 < q)(functools.partial(attend, [index + 2]))
    for u in range(cuts[1]):
        beside(1, *near, u)
    for u in range(cuts[2]):
        entry(2, *near, u)
    exchange_far(kvbuf, 0)
    rest(1)
    proj = project(bbuf)
    keys, vals, updates, marks = [], [], [], []
    for h in range(heads):
        base = h * HEAD
        key = rope(proj[:, base : base + HEAD]).astype(BF16)
        val = proj[:, base + width : base + width + HEAD].astype(BF16)
        column = within[:, h : h + 1]
        last = column[tok - 1 :, :]
        faded = (key.astype(F32) * jnp.exp(last - column)).astype(BF16)
        updates.append(dot(faded, val, ((0,), (0,))))
        high = last.astype(BF16).astype(F32)
        low = last - high
        marks.append(jnp.broadcast_to(high, (8, HEAD)))
        marks.append(jnp.broadcast_to(low, (8, HEAD)))
        keys.append(key)
        vals.append(val)
    marks.append(jnp.zeros((HEAD - 16 * heads, HEAD), F32))
    blocks = updates + [jnp.concatenate(marks, axis=0)]
    if len(blocks) % 2:
        blocks.append(jnp.zeros((HEAD, HEAD), F32))
    for k in range(0, len(blocks), 2):
        both = jnp.concatenate(blocks[k : k + 2], axis=1).astype(BF16)
        stbuf[q, k // 2 * HEAD : (k // 2 + 1) * HEAD, :] = both

    def piece_of(index, k):
        spot = slice(k % 2 * HEAD, (k % 2 + 1) * HEAD)
        return stbuf[index, k // 2 * HEAD : (k // 2 + 1) * HEAD, spot].astype(F32)

    exchange_send(stbuf, 1)
    for u in range(1, cuts[3]):
        scatter_near(3, u)
    for u in range(1, cuts[3]):
        scatter_far(3, u, zh < nh - 1)
    for a in far:
        entry(3, *a, 0)
    for u in range(cuts[2]):
        for a in far:
            beside(2, *a, u)
        beside(2, *near, u)
    exchange_far_across(kvbuf, 0)
    exchange_far(stbuf, 1, zl <= c)
    entry(3, *near, 0)
    rest(2)

    proj = project(cbuf)
    local, lifts = [], []
    for h in range(heads):
        query = (rope(proj[:, h * HEAD : (h + 1) * HEAD]) * HEAD ** (-0.5)).astype(BF16)
        column = within[:, h : h + 1]
        scores = dot(query, keys[h], ((1,), (1,)))
        weights = (scores * decay[h]).astype(BF16)
        local.append(dot(weights, vals[h]))
        lifts.append((query.astype(F32) * jnp.exp(column)).astype(BF16))
    exchange_far(stbuf, 1, zl > c)
    for u in range(1, cuts[3]):
        entry(3, *near, u, zh == nh - 1)
    exchange_far_part(kvbuf, 0)

    def attend_far(half):
        for i in range(1, nh):
            index = sp_of((zh + nh - i) % nh, 0, 0) + 2 * half
            pl.when(zh >= i)(functools.partial(attend, [index, index + 1]))

    exchange_across(stbuf, 1)
    attend_far(0)
    attend_far(1)
    for h in range(heads):
        both = num[h * tok : (h + 1) * tok, :]
        mixed[:, width + h * HEAD : width + (h + 1) * HEAD] = (
            both[:, HEAD:] / both[:, :HEAD]
        ).astype(BF16)
    exchange_far_across(stbuf, 1)
    for u in range(1, cuts[3]):
        for a in far:
            entry(3, *a, u)
    exchange_part(stbuf, 1)
    exchange_far_part(stbuf, 1)
    states = [jnp.zeros((HEAD, HEAD), F32)] * heads
    for j in range(n - 1):
        marked = piece_of(j, heads)
        for h in range(heads):
            total = marked[16 * h : 16 * h + 1] + marked[16 * h + 8 : 16 * h + 9]
            moved = jnp.exp(total) * states[h] + piece_of(j, h)
            states[h] = jnp.where(q > j, moved, states[h])
    retained = []
    for h in range(heads):
        raw = local[h] + dot(lifts[h], states[h].astype(BF16))
        centre = jnp.mean(raw, axis=-1, keepdims=True)
        spread = jnp.mean(jnp.square(raw - centre), axis=-1, keepdims=True)
        retained.append(((raw - centre) * lax.rsqrt(spread + EPS)).astype(BF16))
    mixed[:, :width] = jnp.concatenate(retained, axis=-1)
    order = [(i, j) for i in range(nh) for j in range(2)]

    pair = 2 * rows
    pair_here = pl.ds(pl.multiple_of(x * pair, pair), pair)

    def slice_of(i, j, l):
        return sp_of((zh + i) % nh, (zl + j) % 2, (y + l) % 2)

    def multiply(i, j, l):
        index = slice_of(i, j, l)
        receive(
            halves(3, 1), o_second.at[index], apart if i == 0 and j == 0 and l == 0 else None
        )
        outbuf[index] = dot(mixed[...], obuf[index]).astype(BF16)
        return index

    def give(index, spot, x_, c_, condition):
        where = tp_of(x_, c_)
        rows_there = pl.ds(pl.multiple_of(where * rows, rows), rows)
        send(
            outbuf.at[index, rows_there], rsbuf.at[index, spot], r_send, r_recv.at[index],
            device(zh, c, y, x_, c_), condition, False,
        )

    def produce(i, j, l):
        index = multiply(i, j, l)
        for r in reversed(range(nx)):
            for k in range(2):
                give(
                    index, g, (x + r) % nx, (c + k) % 2, apart if r == 0 and k == 0 else None
                )

    def start_pair(i, j):
        index = multiply(i, j, 0)
        if i % 2:
            send(
                outbuf.at[index], passed.at[index], r_send, r_pass.at[index],
                device(zh, 1 - zl, y, x, c), apart, False,
            )
        else:
            for r in range(1, nx):
                other = (x + r) % nx
                send(
                    outbuf.at[index, pl.ds(pl.multiple_of(other * pair, pair), pair)],
                    passed.at[index, pl.ds((r - 1) * pair, pair)], r_send, r_pass.at[index],
                    device(zh, zl, y, other, c), None, False,
                )

    def finish_pair(i, j):
        index = slice_of(i, j, 0)
        if i % 2:
            receive(passed.at[index], r_pass.at[index], own)

            def merge():
                outbuf[index] = (
                    outbuf[index].astype(F32) + passed[index].astype(F32)
                ).astype(BF16)

            pl.when(own)(merge)
            for r in reversed(range(nx)):
                for k in range(2):
                    if r or k:
                        give(index, x, (x + r) % nx, (c + k) % 2, own)
        else:
            receive(passed.at[index, pl.ds(0, (nx - 1) * pair)], r_pass.at[index])
            total = outbuf[index, pair_here].astype(F32)
            for r in range(1, nx):
                total = total + passed[index, (r - 1) * pair : r * pair].astype(F32)
            outbuf[index, pair_here] = total.astype(BF16)
            for k in (1, 0):
                give(index, zl, x, (c + k) % 2, None if k else apart)

    order = [(i, j) for i in range(nh) for j in range(2)]
    start_pair(*order[0])
    for u in range(1, cuts[3]):
        entry(3, *near, u, zh < nh - 1)
    for i, j in order[2:] + order[1:2]:
        start_pair(i, j)
    for u in range(cuts[3]):
        beside(3, *near, u)
    for i, j in order[:2]:
        produce(i, j, 1)
    for u in range(cuts[3]):
        for a in far:
            beside(3, *a, u)
    for i, j in order:
        if i % 2 == 0:
            finish_pair(i, j)
    for i, j in order[2:]:
        produce(i, j, 1)
    for i, j in order:
        if i % 2:
            finish_pair(i, j)
    columns = obuf.shape[2]
    for l in range(2):
        for i, j in order:
            index = slice_of(i, j, l)
            if l:
                spot, count = g, m
            elif i % 2:
                spot, count = x, nx
            else:
                spot, count = zl, 2

            def keep(index=index, spot=spot):
                rsbuf[index, spot] = outbuf[index, pl.ds(pl.multiple_of(t * rows, rows), rows)]

            receive(rsbuf.at[index, pl.ds(0, count - 1)], r_recv.at[index], own)
            pl.when(own)(keep)
            receive(rsbuf.at[index, pl.ds(0, count)], r_recv.at[index], apart)
            total = rsbuf[index, 0].astype(F32)
            for other in range(1, count):
                total = total + rsbuf[index, other].astype(F32)
            span = pl.ds(pl.multiple_of(index * columns, columns), columns)
            out_ref[:, span] = total.astype(BF16)
    for p in range(4):
        drain(halves(p, n - 1), w_out.at[p], own)
        drain(halves(p, n), w_out.at[p], apart)
        drain(halves(p, n), w_part.at[p], own)
        drain(halves(p, n - 1), w_part.at[p], apart)
    drain(xbuf.at[pl.ds(0, nx * rows)], x_send, own)
    drain(xbuf.at[pl.ds(0, (nx + 1) * rows)], x_send, apart)
    drain(xbuf.at[pl.ds(0, (m - 2) * rows)], x_fwd, apart)
    drain(rsbuf.at[:, pl.ds(0, m - 1)], r_send, own)
    drain(rsbuf, r_send, apart)
    for copy, condition in started:
        guarded(condition, copy.wait_send)


def body(
    n,
    m,
    tokens,
    pre_gain,
    w_query_ret,
    w_key_ret,
    w_value_ret,
    w_query_att,
    w_key_att,
    w_value_att,
    w_out_ret,
    w_out_att,
    retain_log,
    forget_total,
):
    rows, depth = tokens.shape
    tok = rows * m
    heads = retain_log.shape[1]
    nh, nx = n // 4, m // 2
    half = HEAD // 2
    inverse = np.float32(THETA) ** (-np.arange(half, dtype=np.float32) / np.float32(half))
    angles = np.arange(n * tok, dtype=np.float32)[:, None] * inverse[None, :]
    table = np.concatenate([np.cos(angles), np.sin(angles)], axis=1).astype(np.float32)
    wide_a = 2 * HEAD + heads * HEAD
    wide_b, wide_c = 2 * heads * HEAD, heads * HEAD
    deep = w_key_ret.shape[0]
    deep_o = w_out_ret.shape[0] + w_out_att.shape[0]
    tall = (heads // 2 + 1) * HEAD
    hbm = pl.BlockSpec(memory_space=pl.ANY)
    vmem = pl.BlockSpec(memory_space=pltpu.VMEM)
    dma = pltpu.SemaphoreType.DMA
    return pl.pallas_call(
        functools.partial(kernel, n, m, heads),
        out_shape=jax.ShapeDtypeStruct((rows, depth), BF16),
        in_specs=[hbm] * 13,
        out_specs=vmem,
        scratch_shapes=[
            pltpu.VMEM(tokens.shape, BF16),
            pltpu.VMEM((tok, HEAD), F32),
            pltpu.VMEM((2,) + retain_log.shape[::-1], F32),
            pltpu.VMEM((2,) + forget_total.shape, F32),
            pltpu.VMEM((tok + rows, depth), BF16),
            pltpu.VMEM((n + 1, wide_a, deep), BF16),
            pltpu.VMEM((n + 1, wide_b, deep), BF16),
            pltpu.VMEM((n + 1, wide_c, deep), BF16),
            pltpu.VMEM((n + 1, deep_o, w_out_ret.shape[1]), BF16),
            pltpu.VMEM((n, tok, 2 * HEAD), BF16),
            pltpu.VMEM((n, tall, 2 * HEAD), BF16),
            pltpu.VMEM((heads, tok, tok), F32),
            pltpu.VMEM((heads * tok, 2 * HEAD), F32),
            pltpu.VMEM((heads * tok, 2 * HEAD), BF16),
            pltpu.VMEM((heads * tok, LANES), F32),
            pltpu.VMEM((n, tok, w_out_ret.shape[1]), BF16),
            pltpu.VMEM((n, m, rows, w_out_ret.shape[1]), BF16),
            pltpu.VMEM((n, tok, w_out_ret.shape[1]), BF16),
            pltpu.VMEM((tok, 2 * heads * HEAD), BF16),
            pltpu.VMEM((1, depth), F32),
            dma((9,)),
            dma((2,)),
            dma((2,)),
            dma,
            dma,
            dma((2, TOKEN_CUT)),
            dma,
            dma((len(CUTS),)),
            dma((len(CUTS),)),
            *[dma((n, count)) for count in CUTS],
            dma((len(CUTS) - 1,)),
            dma((n,)),
            dma((2, nh - 1)),
            dma((2, nh)),
            dma((2, nh, 2)),
            dma((2, n)),
            dma,
            dma((n,)),
            dma((n,)),
        ],
        compiler_params=pltpu.CompilerParams(
            collective_id=0, has_side_effects=True, vmem_limit_bytes=60 * 1024 * 1024
        ),
    )(
        tokens,
        pre_gain[None, :],
        w_query_ret.T,
        w_key_ret.T,
        w_value_ret.T,
        w_query_att.T,
        w_key_att.T,
        w_value_att.T,
        w_out_ret,
        w_out_att,
        jnp.asarray(table),
        retain_log.T,
        forget_total,
    )


def rotate(field, positions):
    half = field.shape[-1] // 2
    inverse = THETA ** (-jnp.arange(half, dtype=jnp.float32) / half)
    angles = positions[:, None] * inverse[None, :]
    cosine = jnp.cos(angles)[:, None, :]
    sine = jnp.sin(angles)[:, None, :]
    first_half = field[..., :half]
    second_half = field[..., half:]
    return jnp.concatenate(
        [first_half * cosine - second_half * sine, first_half * sine + second_half * cosine],
        axis=-1,
    )


def head_norm(values):
    centre = jnp.mean(values, axis=-1, keepdims=True)
    spread = jnp.mean(jnp.square(values - centre), axis=-1, keepdims=True)
    return (values - centre) * lax.rsqrt(spread + EPS)


def advance(state, pair):
    decay, update = pair
    return (jnp.exp(decay)[:, None, None] * state + update, state)


def plain_body(
    tokens,
    pre_gain,
    w_query_ret,
    w_key_ret,
    w_value_ret,
    w_query_att,
    w_key_att,
    w_value_att,
    w_out_ret,
    w_out_att,
    retain_log,
    forget_total,
):
    rows = tokens.astype(jnp.float32)
    normed = (
        rows * lax.rsqrt(jnp.mean(rows * rows, axis=-1, keepdims=True) + EPS) * pre_gain
    ).astype(jnp.bfloat16)
    gathered = lax.all_gather(normed, "tp", axis=0, tiled=True)
    tok_dev = gathered.shape[0]
    offset = lax.axis_index("sp") * tok_dev
    query_places = offset + jnp.arange(tok_dev, dtype=jnp.int32)
    positions = query_places.astype(jnp.float32)

    def blocked(values):
        return values.reshape((tok_dev // SPAN, SPAN) + values.shape[1:])

    pieces = (
        lax.all_gather(w_query_ret, "sp", axis=0, tiled=True),
        lax.all_gather(w_key_ret, "sp", axis=0, tiled=True),
        lax.all_gather(w_value_ret, "sp", axis=0, tiled=True),
        lax.all_gather(w_query_att, "sp", axis=0, tiled=True),
        lax.all_gather(w_key_att, "sp", axis=0, tiled=True),
        lax.all_gather(w_value_att, "sp", axis=0, tiled=True),
    )
    projected = tuple(
        (jnp.dot(gathered, piece, preferred_element_type=jnp.float32) for piece in pieces)
    )
    heads = retain_log.shape[1]
    shape = (tok_dev, heads, HEAD)
    query = blocked(
        (rotate(projected[0].reshape(shape), positions) * HEAD ** (-0.5)).astype(jnp.bfloat16)
    )
    key_rows = blocked(rotate(projected[1].reshape(shape), positions).astype(jnp.bfloat16))
    value_rows = blocked(projected[2].astype(jnp.bfloat16).reshape(shape))
    within = jnp.cumsum(blocked(retain_log), axis=1)
    causal = jnp.arange(SPAN)[:, None] >= jnp.arange(SPAN)[None, :]
    scores = jnp.einsum("bthd,bshd->bhts", query, key_rows, preferred_element_type=jnp.float32)
    turned = jnp.transpose(within, (0, 2, 1))
    gap = jnp.where(causal, turned[:, :, :, None] - turned[:, :, None, :], 0.0)
    weights = jnp.where(causal, scores * jnp.exp(gap), 0.0).astype(jnp.bfloat16)
    local = jnp.einsum("bhts,bshd->bthd", weights, value_rows, preferred_element_type=jnp.float32)
    last = within[:, -1]
    faded = (key_rows.astype(jnp.float32) * jnp.exp(last[:, None, :] - within)[..., None]).astype(
        jnp.bfloat16
    )
    updates = jnp.einsum("bshd,bshe->bhde", faded, value_rows, preferred_element_type=jnp.float32)
    zero_state = jnp.zeros((heads, HEAD, HEAD), jnp.float32)
    final, _ = lax.scan(advance, zero_state, (last, updates))
    decay_total = jnp.sum(last, axis=0)
    own_state = final.reshape(heads, HEAD * HEAD)
    every_total = lax.all_gather(
        decay_total[None].astype(jnp.bfloat16), "sp", axis=0, tiled=True
    ).astype(jnp.float32)
    every_state = lax.all_gather(
        own_state[None].astype(jnp.bfloat16), "sp", axis=0, tiled=True
    ).astype(jnp.float32)
    device_order = jnp.arange(every_total.shape[0], dtype=jnp.int32)[:, None]
    earlier = device_order < lax.axis_index("sp")
    before = jnp.sum(jnp.where(earlier, every_total, 0.0), axis=0)
    through = jnp.cumsum(every_total, axis=0)
    fading = jnp.where(earlier, jnp.exp(jnp.where(earlier, before[None, :] - through, 0.0)), 0.0)
    incoming = jnp.einsum("jh,jhe->he", fading, every_state, precision=HIGH)
    _, befores = lax.scan(advance, incoming.reshape(heads, HEAD, HEAD), (last, updates))
    lifted = (query.astype(jnp.float32) * jnp.exp(within)[..., None]).astype(jnp.bfloat16)
    carried = jnp.einsum(
        "bthd,bhde->bthe", lifted, befores.astype(jnp.bfloat16), preferred_element_type=jnp.float32
    )
    retained = (
        head_norm((local + carried).reshape(shape))
        .astype(jnp.bfloat16)
        .reshape(tok_dev, heads * HEAD)
    )
    raw_key = projected[4]
    gate_heads = forget_total.shape[0]
    kv_local = raw_key.shape[1] // HEAD
    group = gate_heads // kv_local
    query = (
        (projected[3] * HEAD ** (-0.5)).astype(jnp.bfloat16).reshape(tok_dev, kv_local, group, HEAD)
    )
    key_rows = raw_key.astype(jnp.bfloat16)
    value_rows = projected[5].astype(jnp.bfloat16)
    gate_rows = lax.dynamic_slice_in_dim(forget_total, offset, tok_dev, 1).reshape(
        kv_local, group, tok_dev
    )
    last_row = offset + tok_dev - 1
    init = (
        jnp.zeros((kv_local, group, tok_dev, HEAD), jnp.float32),
        jnp.zeros((kv_local, group, tok_dev), jnp.float32),
    )
    key_piece = lax.all_gather(key_rows, "sp", axis=0, tiled=True)
    value_piece = lax.all_gather(value_rows, "sp", axis=0, tiled=True)
    count = key_piece.shape[0] // KEY_SPAN

    def one_block(index, inner):
        first = index * KEY_SPAN

        def compute(state):
            weighted, total = state
            key_block = lax.dynamic_slice_in_dim(key_piece, index * KEY_SPAN, KEY_SPAN, 0).reshape(
                KEY_SPAN, kv_local, HEAD
            )
            value_block = lax.dynamic_slice_in_dim(
                value_piece, index * KEY_SPAN, KEY_SPAN, 0
            ).reshape(KEY_SPAN, kv_local, HEAD)
            gate_keys = lax.dynamic_slice_in_dim(forget_total, first, KEY_SPAN, 1).reshape(
                kv_local, group, KEY_SPAN
            )
            scores = jnp.einsum(
                "tcgd,scd->cgts", query, key_block, preferred_element_type=jnp.float32
            )
            logits = scores + gate_rows[:, :, :, None] - gate_keys[:, :, None, :]
            allowed = (first + jnp.arange(KEY_SPAN, dtype=jnp.int32))[None, :] <= query_places[
                :, None
            ]
            weights = jnp.exp(jnp.where(allowed, logits, -jnp.inf))
            total = total + jnp.sum(weights, axis=-1)
            weighted = weighted + jnp.einsum(
                "cgts,scd->cgtd",
                weights.astype(jnp.bfloat16),
                value_block,
                preferred_element_type=jnp.float32,
            )
            return (weighted, total)

        def skipped(state):
            return state

        return lax.cond(first <= last_row, compute, skipped, inner)

    weighted, total = lax.fori_loop(0, count, one_block, init)
    result = weighted / total[..., None]
    attended = (
        jnp.transpose(result, (2, 0, 1, 3)).reshape(tok_dev, gate_heads * HEAD).astype(jnp.bfloat16)
    )
    out_ret, out_att = (
        lax.all_gather(w_out_ret, "sp", axis=1, tiled=True),
        lax.all_gather(w_out_att, "sp", axis=1, tiled=True),
    )
    return lax.psum_scatter(
        (
            jnp.dot(retained, out_ret, preferred_element_type=jnp.float32)
            + jnp.dot(attended, out_att, preferred_element_type=jnp.float32)
        ).astype(jnp.bfloat16),
        "tp",
        scatter_dimension=0,
        tiled=True,
    )


def choose(n, m, *arrays):
    tokens, w_key_ret, w_out_ret = arrays[0], arrays[3], arrays[8]
    whole_tiles = w_out_ret.shape[1] % LANES == 0 and w_key_ret.shape[0] % LANES == 0
    heads = arrays[10].shape[1]
    small = 16 * heads <= HEAD and arrays[7].shape[1] == HEAD and arrays[11].shape[0] == heads
    paired = n % 4 == 0 and n > 4 and m % 2 == 0 and m > 2
    if paired and whole_tiles and small and tokens.shape[0] * m == SPAN:
        return body(n, m, *arrays)
    return plain_body(*arrays)


def solution(mesh):
    return jax.shard_map(
        functools.partial(choose, mesh.shape["sp"], mesh.shape["tp"]),
        mesh=mesh,
        in_specs=(
            P(("sp", "tp"), None),
            P(),
            P("sp", "tp"),
            P("sp", "tp"),
            P("sp", "tp"),
            P("sp", "tp"),
            P("sp", "tp"),
            P("sp", "tp"),
            P("tp", "sp"),
            P("tp", "sp"),
            P("sp", "tp"),
            P("tp", None),
        ),
        out_specs=P(("sp", "tp"), None),
        check_vma=False,
    )
```

```python
import functools

import jax
import jax.numpy as jnp
import numpy as np
from jax import lax
from jax.experimental import pallas as pl
from jax.experimental.pallas import tpu as pltpu
from jax.sharding import PartitionSpec as P

HEAD = 64
EPS = 1e-06
THETA = 10000.0
F32 = jnp.float32
BF16 = jnp.bfloat16
MESH = pl.DeviceIdType.MESH
SPAN = 256
KEY_SPAN = 256
LANES = 128
CUTS = (2, 2, 1, 4)
LOG2E = float(np.log2(np.e))
TOKEN_CUT = 4
HIGH = lax.Precision.HIGHEST


def dot(a, b, dims=((1,), (0,))):
    return lax.dot_general(a, b, (dims, ((), ())), preferred_element_type=F32)


def kernel(
    n,
    m,
    heads,
    tok_hbm,
    gain_hbm,
    wq_ret_hbm,
    wk_ret_hbm,
    wv_ret_hbm,
    wq_att_hbm,
    wk_att_hbm,
    wv_att_hbm,
    wo_ret_hbm,
    wo_att_hbm,
    table_hbm,
    logs_hbm,
    gate_hbm,
    out_ref,
    tokens,
    table,
    lbuf,
    gbuf,
    xbuf,
    abuf,
    bbuf,
    cbuf,
    obuf,
    kvbuf,
    stbuf,
    decay,
    num,
    qbuf,
    cbuf_gate,
    outbuf,
    rsbuf,
    passed,
    mixed,
    gain,
    load,
    small_send,
    small_recv,
    x_send,
    x_fwd,
    x_pass,
    x_other,
    w_out,
    w_part,
    first_a,
    first_b,
    first_c,
    first_o,
    w_second,
    o_second,
    k_send,
    k_y,
    k_part,
    k_recv,
    r_send,
    r_pass,
    r_recv,
):
    s, t = lax.axis_index("sp"), lax.axis_index("tp")
    nh, nx = n // 4, m // 2
    y, zl, zh = s % 2, (s // 2) % 2, s // 4
    c, x = t % 2, t // 2
    own = zl == c
    apart = zl != c

    def sp_of(zh_, zl_, y_):
        return zh_ * 4 + zl_ * 2 + y_

    def tp_of(x_, c_):
        return x_ * 2 + c_

    def device(zh_, zl_, y_, x_, c_):
        return {"sp": sp_of(zh_, zl_, y_), "tp": tp_of(x_, c_)}

    q, g = sp_of(zh, c, y), tp_of(x, zl)
    partner = device(zh, zl, y, x, 1 - c)
    across = device(zh, zl, 1 - y, x, c)
    rows = tokens.shape[0]
    tok = rows * m
    width = heads * HEAD
    half_o = wo_ret_hbm.shape[0]

    slot = jnp.where(own, s, n)
    piece = jnp.where(own, t, m)
    groups = (
        (tokens, ((tok_hbm, tokens),)),
        (gain, ((gain_hbm, gain),)),
        (abuf.at[slot], (
            (wk_att_hbm, abuf.at[slot, pl.ds(0, HEAD)]),
            (wv_att_hbm, abuf.at[slot, pl.ds(HEAD, HEAD)]),
            (wq_att_hbm, abuf.at[slot, pl.ds(2 * HEAD, width)]),
        )),
        (bbuf.at[slot], (
            (wk_ret_hbm, bbuf.at[slot, pl.ds(0, width)]),
            (wv_ret_hbm, bbuf.at[slot, pl.ds(width, width)]),
        )),
        (cbuf.at[slot], ((wq_ret_hbm, cbuf.at[slot]),)),
        (obuf.at[slot], (
            (wo_ret_hbm, obuf.at[slot, pl.ds(0, half_o)]),
            (wo_att_hbm, obuf.at[slot, pl.ds(half_o, wo_att_hbm.shape[0])]),
        )),
        (table, ((table_hbm.at[pl.ds(pl.multiple_of(q * tok, tok), tok)], table),)),
        (lbuf.at[0], ((logs_hbm, lbuf.at[0]),)),
        (gbuf.at[0], ((gate_hbm, gbuf.at[0]),)),
    )
    loads = []
    for k, (whole, copies) in enumerate(groups):
        for source, target in copies:
            pltpu.make_async_copy(source, target, load.at[k]).start()
        loads.append(pltpu.make_async_copy(whole, whole, load.at[k]))

    stbuf[...] = jnp.zeros_like(stbuf)
    barrier = pltpu.get_barrier_semaphore()
    greeted = [
        device((zh + i) % nh, zl, 1 - y, x, (c + k) % 2) for i in range(nh) for k in range(2)
    ]
    for i in reversed(range(nh)):
        for j in reversed(range(2)):
            for k in range(2):
                if i or j or k:
                    greeted.append(device((zh + i) % nh, (zl + j) % 2, y, x, (c + k) % 2))
    for r in range(1, nx):
        for j in range(2):
            for k in range(2):
                greeted.append(device(zh, (zl + j) % 2, y, (x + r) % nx, (c + k) % 2))
    for other in greeted:
        pl.semaphore_signal(barrier, inc=1, device_id=other, device_id_type=MESH)

    started = []

    def guarded(condition, action):
        if condition is None:
            action()
        else:
            pl.when(condition)(action)

    def send(source, target, send_sem, recv_sem, where, condition=None, kept=True):
        copy = pltpu.make_async_remote_copy(
            src_ref=source, dst_ref=target, send_sem=send_sem, recv_sem=recv_sem,
            device_id=where, device_id_type=MESH,
        )
        guarded(condition, copy.start)
        if kept:
            started.append((copy, condition))

    def drain(source, send_sem, condition=None):
        started.append((
            pltpu.make_async_remote_copy(
                src_ref=source, dst_ref=source, send_sem=send_sem, recv_sem=send_sem,
                device_id=partner, device_id_type=MESH,
            ),
            condition,
        ))

    def receive(target, recv_sem, condition=None):
        copy = pltpu.make_async_remote_copy(
            src_ref=target, dst_ref=target, send_sem=recv_sem, recv_sem=recv_sem,
            device_id=partner, device_id_type=MESH,
        )
        guarded(condition, copy.wait_recv)

    for copy in loads[:2]:
        copy.wait()
    values = tokens[...].astype(F32)
    scale = lax.rsqrt(jnp.mean(values * values, axis=-1, keepdims=True) + EPS)
    xbuf[pl.ds(pl.multiple_of(piece * rows, rows), rows), :] = (
        values * scale * gain[...]
    ).astype(BF16)
    for copy in loads[2:]:
        copy.wait()
    pl.semaphore_wait(barrier, len(greeted))

    parts = (abuf, bbuf, cbuf, obuf)
    cuts = CUTS

    def chunk(p, index, k, u):
        length = parts[p].shape[1] // (2 * cuts[p])
        start = pl.multiple_of((k * cuts[p] + u) * length, length)
        return parts[p].at[index, pl.ds(start, length)]

    firsts = (first_a, first_b, first_c, first_o)

    def second(p, index):
        return o_second.at[index] if p == 3 else w_second.at[p]

    def halves(p, count):
        return parts[p].at[pl.ds(0, count), pl.ds(0, parts[p].shape[1] // 2)]

    def scatter_one(p, i, k, u, condition):
        core = (c + k) % 2
        send(
            chunk(p, slot, core, u), chunk(p, s, core, u), w_out.at[p], firsts[p].at[s, u],
            device((zh + i) % nh, c, y, x, core), condition, False,
        )

    def scatter_chip(p):
        for u in range(cuts[p]):
            scatter_one(p, 0, 1, u, own)

    def scatter_near(p, u, also=True):
        for k in range(2):
            scatter_one(p, 0, k, u, apart & also)

    def scatter_far(p, u, condition=None):
        for i in range(1, nh):
            for k in range(2):
                scatter_one(p, i, k, u, condition)

    middle = zl != zh % 2
    outer = zl == zh % 2

    def entry(p, i, j, u, condition=None):
        index = sp_of((zh + i) % nh, (zl + j) % 2, y)
        here = i == 0 and j == 0
        spot = chunk(p, index, c, u)
        receive(spot, firsts[p].at[index, u], apart if here else condition)
        send(spot, spot, w_out.at[p], firsts[p].at[index, u], across, condition, False)
        send(
            spot, spot, w_part.at[p], second(p, index), partner,
            own if here else condition, False,
        )

    def beside(p, i, j, u):
        index = sp_of((zh + i) % nh, (zl + j) % 2, 1 - y)
        spot = chunk(p, index, c, u)
        receive(spot, firsts[p].at[index, u])
        send(spot, spot, w_part.at[p], second(p, index), partner, None, False)

    def rest(p):
        receive(halves(p, n - 1), w_second.at[p], own)
        receive(halves(p, n), w_second.at[p], apart)

    far = [(i, j) for i in range(1, nh) for j in range(2)]
    near = (0, 1)
    pieces = x_pass.shape[1]

    def rows_of(index, u):
        length = rows // pieces
        return xbuf.at[pl.ds(pl.multiple_of((index * pieces + u) * length, length), length)]

    def pass_tokens(k, u):
        core = (c + k) % 2
        index = tp_of(x, core)
        spot = rows_of(index, u)
        receive(spot, x_pass.at[core, u], apart if k == 0 else None)
        for r in range(1, nx):
            send(
                spot, spot, x_fwd, x_other, device(zh, zl, y, (x + r) % nx, c), apart, False,
            )

    send(
        lbuf.at[0], lbuf.at[1], small_send.at[0], small_recv.at[0],
        device(zh, c, y, x, zl), apart,
    )
    send(gbuf.at[0], gbuf.at[1], small_send.at[1], small_recv.at[1], partner, own)
    for u in range(cuts[0]):
        scatter_far(0, u)
    scatter_chip(0)
    def give_tokens(u):
        ours, there = rows_of(piece, u), rows_of(t, u)
        send(ours, there, x_send, x_pass.at[c, u], device(zh, 1 - zl, y, x, zl), None, False)
        for r in range(1, nx):
            send(
                ours, there, x_send, x_other, device(zh, zl, y, (x + r) % nx, zl), None, False,
            )
        send(ours, there, x_send, x_pass.at[c, u], device(zh, zl, y, x, zl), apart, False)

    for u in range(pieces // 2):
        give_tokens(u)
    for u in range(cuts[0]):
        scatter_near(0, u)
    for u in range(pieces // 2, pieces):
        give_tokens(u)
    for p in range(1, 4):
        scatter_chip(p)
    for p in range(1, 3):
        for u in range(cuts[p]):
            scatter_far(p, u)
            scatter_near(p, u)
    for p in range(4):
        for u in range(cuts[p]):
            entry(p, 0, 0, u)
    lines = lax.broadcasted_iota(jnp.int32, (tok, tok), 0)
    lanes = lax.broadcasted_iota(jnp.int32, (tok, tok), 1)
    causal = lines >= lanes
    upto = jnp.where(lines <= lanes, 1.0, 0.0)
    receive(lbuf.at[1], small_recv.at[0], apart)
    receive(gbuf.at[1], small_recv.at[1], apart)
    pick = jnp.where(own, 0, 1)
    logs = jnp.concatenate([lbuf[pick], jnp.zeros((8 - heads, tok), F32)], axis=0)
    turned = lax.dot_general(
        logs, upto, (((1,), (0,)), ((), ())),
        preferred_element_type=F32, precision=lax.Precision.HIGHEST,
    )
    fill = jnp.zeros((LANES - 8, tok), F32)
    within = jnp.concatenate([turned, fill], axis=0).T
    gates_own = gbuf[pick, :, pl.ds(pl.multiple_of(q * tok, tok), tok)]
    gate_col = jnp.concatenate(
        [gates_own, jnp.zeros((LANES - heads, tok), F32)], axis=0
    ).T
    cosine, sine = table[:, : HEAD // 2], table[:, HEAD // 2 :]
    for h in range(heads):
        gap = jnp.where(causal, within[:, h : h + 1] - turned[h : h + 1, :], 0.0)
        decay[h] = jnp.where(causal, jnp.exp(gap), 0.0)

    for u in range(cuts[0]):
        beside(0, 0, 0, u)
    for a in far:
        entry(0, *a, 0)
    for u in range(pieces // 2):
        for k in range(2):
            pass_tokens(k, u)
    for u in range(cuts[1]):
        beside(1, 0, 0, u)
    for u in range(1, cuts[0]):
        for a in far:
            entry(0, *a, u)
    for a in far:
        beside(0, *a, 0)
    for u in range(cuts[0]):
        entry(0, *near, u)
    for u in range(pieces // 2, pieces):
        for k in range(2):
            pass_tokens(k, u)
    for a in far:
        entry(1, *a, 0, middle)
    for u in range(1, cuts[0]):
        for a in far:
            beside(0, *a, u)
    for p in range(2, 4):
        for u in range(cuts[p]):
            beside(p, 0, 0, u)
    for u in range(cuts[0]):
        beside(0, *near, u)
    for u in range(1, cuts[1]):
        for a in far:
            entry(1, *a, u, middle)
    for a in far:
        entry(1, *a, 0, outer)

    receive(xbuf.at[pl.ds(0, (m - 2) * rows)], x_other)
    rest(0)

    def exchange(buf, e, index, sem, where, condition):
        send(buf.at[index], buf.at[index], sem, k_recv.at[e, index], where, condition)

    def arrive(buf, e, index, condition):
        receive(buf.at[index], k_recv.at[e, index], condition)

    def exchange_send(buf, e):
        for i in range(1, nh):
            exchange(
                buf, e, q, k_send.at[e, i - 1], device((zh + i) % nh, zl, y, x, c), zh + i < nh
            )
        exchange(buf, e, q, k_y.at[e, 0], across, c + y < 2)
        exchange(buf, e, q, k_part.at[e, 0, 0], partner, c == 0)

    def exchange_across(buf, e):
        index = sp_of(zh, c, 1 - y)
        arrive(buf, e, index, c <= y)
        exchange(buf, e, index, k_part.at[e, 0, 1], partner, c == 0)

    def exchange_part(buf, e):
        for k in range(2):
            arrive(buf, e, sp_of(zh, 1 - c, (y + k) % 2), c == 1)

    def exchange_far(buf, e, also=True):
        for i in range(1, nh):
            index = sp_of((zh + nh - i) % nh, c, y)
            condition = (zh >= i) & also
            arrive(buf, e, index, condition)
            exchange(buf, e, index, k_y.at[e, i], across, condition)
            exchange(buf, e, index, k_part.at[e, i, 0], partner, condition)

    def exchange_far_across(buf, e):
        for i in range(1, nh):
            index = sp_of((zh + nh - i) % nh, c, 1 - y)
            arrive(buf, e, index, zh >= i)
            exchange(buf, e, index, k_part.at[e, i, 1], partner, zh >= i)

    def exchange_far_part(buf, e):
        for i in range(1, nh):
            for k in range(2):
                arrive(buf, e, sp_of((zh + nh - i) % nh, 1 - c, (y + k) % 2), zh >= i)

    def rope(field):
        first, second = field[:, : HEAD // 2], field[:, HEAD // 2 :]
        return jnp.concatenate(
            [first * cosine - second * sine, first * sine + second * cosine], axis=-1
        )

    def project(buf):
        deep = buf.shape[2]
        return sum(
            dot(xbuf[:tok, k * deep : (k + 1) * deep], buf[k], ((1,), (1,))) for k in range(n)
        )

    proj = project(abuf)
    kvbuf[q] = proj[:, : 2 * HEAD].astype(BF16)
    exchange_send(kvbuf, 0)
    scatter_far(3, 0)
    scatter_near(3, 0)
    for u in range(1, cuts[3]):
        scatter_far(3, u, zh == nh - 1)
    wide = heads * tok
    zeros = jnp.zeros((tok, HEAD), F32)
    for h in range(heads):
        query = proj[:, (2 + h) * HEAD : (3 + h) * HEAD] * (HEAD ** (-0.5) * LOG2E)
        qbuf[h * tok : (h + 1) * tok, :] = jnp.concatenate([query, zeros], axis=1).astype(BF16)
        cbuf_gate[h * tok : (h + 1) * tok, :] = jnp.broadcast_to(
            gate_col[:, h : h + 1] * LOG2E, (tok, LANES)
        )
    low_lanes = lax.broadcasted_iota(jnp.int32, (tok, 2 * HEAD), 1) < HEAD

    def attend(indices, masked=False):
        total = None if masked else num[...]
        for index in indices:
            block = kvbuf[index]
            values = jnp.where(low_lanes, jnp.ones_like(block), block)
            gates = gbuf[pick, :, pl.ds(pl.multiple_of(index * tok, tok), tok)] * LOG2E
            logits = dot(qbuf[...], block, ((1,), (1,)))
            column = cbuf_gate[...]
            column = jnp.concatenate([column] * (tok // LANES), axis=1)
            pieces_ = []
            for h in range(heads):
                part = slice(h * tok, (h + 1) * tok)
                shifted = logits[part] + column[part] - gates[h : h + 1, :]
                if masked:
                    shifted = jnp.where(causal, shifted, -jnp.inf)
                pieces_.append(jnp.exp2(shifted).astype(BF16))
            term = dot(jnp.concatenate(pieces_, axis=0), values)
            total = term if total is None else total + term
        num[...] = total

    for u in range(1, cuts[1]):
        for a in far:
            entry(1, *a, u, outer)
    attend([q], True)
    for a in far:
        beside(1, *a, 0)
    for u in range(cuts[1]):
        entry(1, *near, u)
    exchange_across(kvbuf, 0)
    exchange_part(kvbuf, 0)
    index = sp_of(zh, 0, 0)
    pl.when(index < q)(functools.partial(attend, [index]))
    pl.when(index + 1 < q)(functools.partial(attend, [index + 1]))
    for u in range(1, cuts[1]):
        for a in far:
            beside(1, *a, u)
    for u in range(cuts[2]):
        for a in far:
            entry(2, *a, u)
    pl.when(index + 2 < q)(functools.partial(attend, [index + 2]))
    for u in range(cuts[1]):
        beside(1, *near, u)
    for u in range(cuts[2]):
        entry(2, *near, u)
    exchange_far(kvbuf, 0)
    rest(1)
    proj = project(bbuf)
    keys, vals, updates, marks = [], [], [], []
    for h in range(heads):
        base = h * HEAD
        key = rope(proj[:, base : base + HEAD]).astype(BF16)
        val = proj[:, base + width : base + width + HEAD].astype(BF16)
        column = within[:, h : h + 1]
        last = column[tok - 1 :, :]
        faded = (key.astype(F32) * jnp.exp(last - column)).astype(BF16)
        updates.append(dot(faded, val, ((0,), (0,))))
        high = last.astype(BF16).astype(F32)
        low = last - high
        marks.append(jnp.broadcast_to(high, (8, HEAD)))
        marks.append(jnp.broadcast_to(low, (8, HEAD)))
        keys.append(key)
        vals.append(val)
    marks.append(jnp.zeros((HEAD - 16 * heads, HEAD), F32))
    blocks = updates + [jnp.concatenate(marks, axis=0)]
    if len(blocks) % 2:
        blocks.append(jnp.zeros((HEAD, HEAD), F32))
    for k in range(0, len(blocks), 2):
        both = jnp.concatenate(blocks[k : k + 2], axis=1).astype(BF16)
        stbuf[q, k // 2 * HEAD : (k // 2 + 1) * HEAD, :] = both

    def piece_of(index, k):
        spot = slice(k % 2 * HEAD, (k % 2 + 1) * HEAD)
        return stbuf[index, k // 2 * HEAD : (k // 2 + 1) * HEAD, spot].astype(F32)

    exchange_send(stbuf, 1)
    for u in range(1, cuts[3]):
        scatter_near(3, u)
    for u in range(1, cuts[3]):
        scatter_far(3, u, zh < nh - 1)
    for a in far:
        entry(3, *a, 0)
    for u in range(cuts[2]):
        for a in far:
            beside(2, *a, u)
        beside(2, *near, u)
    exchange_far_across(kvbuf, 0)
    exchange_far(stbuf, 1, zl <= c)
    entry(3, *near, 0)
    rest(2)

    proj = project(cbuf)
    local, lifts = [], []
    for h in range(heads):
        query = (rope(proj[:, h * HEAD : (h + 1) * HEAD]) * HEAD ** (-0.5)).astype(BF16)
        column = within[:, h : h + 1]
        scores = dot(query, keys[h], ((1,), (1,)))
        weights = (scores * decay[h]).astype(BF16)
        local.append(dot(weights, vals[h]))
        lifts.append((query.astype(F32) * jnp.exp(column)).astype(BF16))
    exchange_far(stbuf, 1, zl > c)
    for u in range(1, cuts[3]):
        entry(3, *near, u, zh == nh - 1)
    exchange_far_part(kvbuf, 0)

    def attend_far(half):
        for i in range(1, nh):
            index = sp_of((zh + nh - i) % nh, 0, 0) + 2 * half
            pl.when(zh >= i)(functools.partial(attend, [index, index + 1]))

    exchange_across(stbuf, 1)
    attend_far(0)
    attend_far(1)
    for h in range(heads):
        both = num[h * tok : (h + 1) * tok, :]
        mixed[:, width + h * HEAD : width + (h + 1) * HEAD] = (
            both[:, HEAD:] / both[:, :HEAD]
        ).astype(BF16)
    exchange_far_across(stbuf, 1)
    for u in range(1, cuts[3]):
        for a in far:
            entry(3, *a, u)
    exchange_part(stbuf, 1)
    exchange_far_part(stbuf, 1)
    states = [jnp.zeros((HEAD, HEAD), F32)] * heads
    for j in range(n - 1):
        marked = piece_of(j, heads)
        for h in range(heads):
            total = marked[16 * h : 16 * h + 1] + marked[16 * h + 8 : 16 * h + 9]
            moved = jnp.exp(total) * states[h] + piece_of(j, h)
            states[h] = jnp.where(q > j, moved, states[h])
    retained = []
    for h in range(heads):
        raw = local[h] + dot(lifts[h], states[h].astype(BF16))
        centre = jnp.mean(raw, axis=-1, keepdims=True)
        spread = jnp.mean(jnp.square(raw - centre), axis=-1, keepdims=True)
        retained.append(((raw - centre) * lax.rsqrt(spread + EPS)).astype(BF16))
    mixed[:, :width] = jnp.concatenate(retained, axis=-1)
    order = [(i, j) for i in range(nh) for j in range(2)]

    pair = 2 * rows
    pair_here = pl.ds(pl.multiple_of(x * pair, pair), pair)

    def slice_of(i, j, l):
        return sp_of((zh + i) % nh, (zl + j) % 2, (y + l) % 2)

    def multiply(i, j, l):
        index = slice_of(i, j, l)
        receive(
            halves(3, 1), o_second.at[index], apart if i == 0 and j == 0 and l == 0 else None
        )
        outbuf[index] = dot(mixed[...], obuf[index]).astype(BF16)
        return index

    def give(index, spot, x_, c_, condition):
        where = tp_of(x_, c_)
        rows_there = pl.ds(pl.multiple_of(where * rows, rows), rows)
        send(
            outbuf.at[index, rows_there], rsbuf.at[index, spot], r_send, r_recv.at[index],
            device(zh, c, y, x_, c_), condition, False,
        )

    def produce(i, j, l):
        index = multiply(i, j, l)
        for r in reversed(range(nx)):
            for k in range(2):
                give(
                    index, g, (x + r) % nx, (c + k) % 2, apart if r == 0 and k == 0 else None
                )

    def start_pair(i, j):
        index = multiply(i, j, 0)
        if i % 2:
            send(
                outbuf.at[index], passed.at[index], r_send, r_pass.at[index],
                device(zh, 1 - zl, y, x, c), apart, False,
            )
        else:
            for r in range(1, nx):
                other = (x + r) % nx
                send(
                    outbuf.at[index, pl.ds(pl.multiple_of(other * pair, pair), pair)],
                    passed.at[index, pl.ds((r - 1) * pair, pair)], r_send, r_pass.at[index],
                    device(zh, zl, y, other, c), None, False,
                )

    def finish_pair(i, j):
        index = slice_of(i, j, 0)
        if i % 2:
            receive(passed.at[index], r_pass.at[index], own)

            def merge():
                outbuf[index] = (
                    outbuf[index].astype(F32) + passed[index].astype(F32)
                ).astype(BF16)

            pl.when(own)(merge)
            for r in reversed(range(nx)):
                for k in range(2):
                    if r or k:
                        give(index, x, (x + r) % nx, (c + k) % 2, own)
        else:
            receive(passed.at[index, pl.ds(0, (nx - 1) * pair)], r_pass.at[index])
            total = outbuf[index, pair_here].astype(F32)
            for r in range(1, nx):
                total = total + passed[index, (r - 1) * pair : r * pair].astype(F32)
            outbuf[index, pair_here] = total.astype(BF16)
            for k in (1, 0):
                give(index, zl, x, (c + k) % 2, None if k else apart)

    order = [(i, j) for i in range(nh) for j in range(2)]
    start_pair(*order[0])
    for u in range(1, cuts[3]):
        entry(3, *near, u, zh < nh - 1)
    for i, j in order[2:] + order[1:2]:
        start_pair(i, j)
    for u in range(cuts[3]):
        beside(3, *near, u)
    for i, j in order[:2]:
        produce(i, j, 1)
    for u in range(cuts[3]):
        for a in far:
            beside(3, *a, u)
    for i, j in order:
        if i % 2 == 0:
            finish_pair(i, j)
    for i, j in order[2:]:
        produce(i, j, 1)
    for i, j in order:
        if i % 2:
            finish_pair(i, j)
    columns = obuf.shape[2]
    for l in range(2):
        for i, j in order:
            index = slice_of(i, j, l)
            if l:
                spot, count = g, m
            elif i % 2:
                spot, count = x, nx
            else:
                spot, count = zl, 2

            def keep(index=index, spot=spot):
                rsbuf[index, spot] = outbuf[index, pl.ds(pl.multiple_of(t * rows, rows), rows)]

            receive(rsbuf.at[index, pl.ds(0, count - 1)], r_recv.at[index], own)
            pl.when(own)(keep)
            receive(rsbuf.at[index, pl.ds(0, count)], r_recv.at[index], apart)
            total = rsbuf[index, 0].astype(F32)
            for other in range(1, count):
                total = total + rsbuf[index, other].astype(F32)
            span = pl.ds(pl.multiple_of(index * columns, columns), columns)
            out_ref[:, span] = total.astype(BF16)
    for p in range(4):
        drain(halves(p, n - 1), w_out.at[p], own)
        drain(halves(p, n), w_out.at[p], apart)
        drain(halves(p, n), w_part.at[p], own)
        drain(halves(p, n - 1), w_part.at[p], apart)
    drain(xbuf.at[pl.ds(0, nx * rows)], x_send, own)
    drain(xbuf.at[pl.ds(0, (nx + 1) * rows)], x_send, apart)
    drain(xbuf.at[pl.ds(0, (m - 2) * rows)], x_fwd, apart)
    drain(rsbuf.at[:, pl.ds(0, m - 1)], r_send, own)
    drain(rsbuf, r_send, apart)
    for copy, condition in started:
        guarded(condition, copy.wait_send)


def body(
    n,
    m,
    tokens,
    pre_gain,
    w_query_ret,
    w_key_ret,
    w_value_ret,
    w_query_att,
    w_key_att,
    w_value_att,
    w_out_ret,
    w_out_att,
    retain_log,
    forget_total,
):
    rows, depth = tokens.shape
    tok = rows * m
    heads = retain_log.shape[1]
    nh, nx = n // 4, m // 2
    half = HEAD // 2
    inverse = np.float32(THETA) ** (-np.arange(half, dtype=np.float32) / np.float32(half))
    angles = np.arange(n * tok, dtype=np.float32)[:, None] * inverse[None, :]
    table = np.concatenate([np.cos(angles), np.sin(angles)], axis=1).astype(np.float32)
    wide_a = 2 * HEAD + heads * HEAD
    wide_b, wide_c = 2 * heads * HEAD, heads * HEAD
    deep = w_key_ret.shape[0]
    deep_o = w_out_ret.shape[0] + w_out_att.shape[0]
    tall = (heads // 2 + 1) * HEAD
    hbm = pl.BlockSpec(memory_space=pl.ANY)
    vmem = pl.BlockSpec(memory_space=pltpu.VMEM)
    dma = pltpu.SemaphoreType.DMA
    return pl.pallas_call(
        functools.partial(kernel, n, m, heads),
        out_shape=jax.ShapeDtypeStruct((rows, depth), BF16),
        in_specs=[hbm] * 13,
        out_specs=vmem,
        scratch_shapes=[
            pltpu.VMEM(tokens.shape, BF16),
            pltpu.VMEM((tok, HEAD), F32),
            pltpu.VMEM((2,) + retain_log.shape[::-1], F32),
            pltpu.VMEM((2,) + forget_total.shape, F32),
            pltpu.VMEM((tok + rows, depth), BF16),
            pltpu.VMEM((n + 1, wide_a, deep), BF16),
            pltpu.VMEM((n + 1, wide_b, deep), BF16),
            pltpu.VMEM((n + 1, wide_c, deep), BF16),
            pltpu.VMEM((n + 1, deep_o, w_out_ret.shape[1]), BF16),
            pltpu.VMEM((n, tok, 2 * HEAD), BF16),
            pltpu.VMEM((n, tall, 2 * HEAD), BF16),
            pltpu.VMEM((heads, tok, tok), F32),
            pltpu.VMEM((heads * tok, 2 * HEAD), F32),
            pltpu.VMEM((heads * tok, 2 * HEAD), BF16),
            pltpu.VMEM((heads * tok, LANES), F32),
            pltpu.VMEM((n, tok, w_out_ret.shape[1]), BF16),
            pltpu.VMEM((n, m, rows, w_out_ret.shape[1]), BF16),
            pltpu.VMEM((n, tok, w_out_ret.shape[1]), BF16),
            pltpu.VMEM((tok, 2 * heads * HEAD), BF16),
            pltpu.VMEM((1, depth), F32),
            dma((9,)),
            dma((2,)),
            dma((2,)),
            dma,
            dma,
            dma((2, TOKEN_CUT)),
            dma,
            dma((len(CUTS),)),
            dma((len(CUTS),)),
            *[dma((n, count)) for count in CUTS],
            dma((len(CUTS) - 1,)),
            dma((n,)),
            dma((2, nh - 1)),
            dma((2, nh)),
            dma((2, nh, 2)),
            dma((2, n)),
            dma,
            dma((n,)),
            dma((n,)),
        ],
        compiler_params=pltpu.CompilerParams(
            collective_id=0, has_side_effects=True, vmem_limit_bytes=60 * 1024 * 1024
        ),
    )(
        tokens,
        pre_gain[None, :],
        w_query_ret.T,
        w_key_ret.T,
        w_value_ret.T,
        w_query_att.T,
        w_key_att.T,
        w_value_att.T,
        w_out_ret,
        w_out_att,
        jnp.asarray(table),
        retain_log.T,
        forget_total,
    )


def rotate(field, positions):
    half = field.shape[-1] // 2
    inverse = THETA ** (-jnp.arange(half, dtype=jnp.float32) / half)
    angles = positions[:, None] * inverse[None, :]
    cosine = jnp.cos(angles)[:, None, :]
    sine = jnp.sin(angles)[:, None, :]
    first_half = field[..., :half]
    second_half = field[..., half:]
    return jnp.concatenate(
        [first_half * cosine - second_half * sine, first_half * sine + second_half * cosine],
        axis=-1,
    )


def head_norm(values):
    centre = jnp.mean(values, axis=-1, keepdims=True)
    spread = jnp.mean(jnp.square(values - centre), axis=-1, keepdims=True)
    return (values - centre) * lax.rsqrt(spread + EPS)


def advance(state, pair):
    decay, update = pair
    return (jnp.exp(decay)[:, None, None] * state + update, state)


def plain_body(
    tokens,
    pre_gain,
    w_query_ret,
    w_key_ret,
    w_value_ret,
    w_query_att,
    w_key_att,
    w_value_att,
    w_out_ret,
    w_out_att,
    retain_log,
    forget_total,
):
    rows = tokens.astype(jnp.float32)
    normed = (
        rows * lax.rsqrt(jnp.mean(rows * rows, axis=-1, keepdims=True) + EPS) * pre_gain
    ).astype(jnp.bfloat16)
    gathered = lax.all_gather(normed, "tp", axis=0, tiled=True)
    tok_dev = gathered.shape[0]
    offset = lax.axis_index("sp") * tok_dev
    query_places = offset + jnp.arange(tok_dev, dtype=jnp.int32)
    positions = query_places.astype(jnp.float32)

    def blocked(values):
        return values.reshape((tok_dev // SPAN, SPAN) + values.shape[1:])

    pieces = (
        lax.all_gather(w_query_ret, "sp", axis=0, tiled=True),
        lax.all_gather(w_key_ret, "sp", axis=0, tiled=True),
        lax.all_gather(w_value_ret, "sp", axis=0, tiled=True),
        lax.all_gather(w_query_att, "sp", axis=0, tiled=True),
        lax.all_gather(w_key_att, "sp", axis=0, tiled=True),
        lax.all_gather(w_value_att, "sp", axis=0, tiled=True),
    )
    projected = tuple(
        (jnp.dot(gathered, piece, preferred_element_type=jnp.float32) for piece in pieces)
    )
    heads = retain_log.shape[1]
    shape = (tok_dev, heads, HEAD)
    query = blocked(
        (rotate(projected[0].reshape(shape), positions) * HEAD ** (-0.5)).astype(jnp.bfloat16)
    )
    key_rows = blocked(rotate(projected[1].reshape(shape), positions).astype(jnp.bfloat16))
    value_rows = blocked(projected[2].astype(jnp.bfloat16).reshape(shape))
    within = jnp.cumsum(blocked(retain_log), axis=1)
    causal = jnp.arange(SPAN)[:, None] >= jnp.arange(SPAN)[None, :]
    scores = jnp.einsum("bthd,bshd->bhts", query, key_rows, preferred_element_type=jnp.float32)
    turned = jnp.transpose(within, (0, 2, 1))
    gap = jnp.where(causal, turned[:, :, :, None] - turned[:, :, None, :], 0.0)
    weights = jnp.where(causal, scores * jnp.exp(gap), 0.0).astype(jnp.bfloat16)
    local = jnp.einsum("bhts,bshd->bthd", weights, value_rows, preferred_element_type=jnp.float32)
    last = within[:, -1]
    faded = (key_rows.astype(jnp.float32) * jnp.exp(last[:, None, :] - within)[..., None]).astype(
        jnp.bfloat16
    )
    updates = jnp.einsum("bshd,bshe->bhde", faded, value_rows, preferred_element_type=jnp.float32)
    zero_state = jnp.zeros((heads, HEAD, HEAD), jnp.float32)
    final, _ = lax.scan(advance, zero_state, (last, updates))
    decay_total = jnp.sum(last, axis=0)
    own_state = final.reshape(heads, HEAD * HEAD)
    every_total = lax.all_gather(
        decay_total[None].astype(jnp.bfloat16), "sp", axis=0, tiled=True
    ).astype(jnp.float32)
    every_state = lax.all_gather(
        own_state[None].astype(jnp.bfloat16), "sp", axis=0, tiled=True
    ).astype(jnp.float32)
    device_order = jnp.arange(every_total.shape[0], dtype=jnp.int32)[:, None]
    earlier = device_order < lax.axis_index("sp")
    before = jnp.sum(jnp.where(earlier, every_total, 0.0), axis=0)
    through = jnp.cumsum(every_total, axis=0)
    fading = jnp.where(earlier, jnp.exp(jnp.where(earlier, before[None, :] - through, 0.0)), 0.0)
    incoming = jnp.einsum("jh,jhe->he", fading, every_state, precision=HIGH)
    _, befores = lax.scan(advance, incoming.reshape(heads, HEAD, HEAD), (last, updates))
    lifted = (query.astype(jnp.float32) * jnp.exp(within)[..., None]).astype(jnp.bfloat16)
    carried = jnp.einsum(
        "bthd,bhde->bthe", lifted, befores.astype(jnp.bfloat16), preferred_element_type=jnp.float32
    )
    retained = (
        head_norm((local + carried).reshape(shape))
        .astype(jnp.bfloat16)
        .reshape(tok_dev, heads * HEAD)
    )
    raw_key = projected[4]
    gate_heads = forget_total.shape[0]
    kv_local = raw_key.shape[1] // HEAD
    group = gate_heads // kv_local
    query = (
        (projected[3] * HEAD ** (-0.5)).astype(jnp.bfloat16).reshape(tok_dev, kv_local, group, HEAD)
    )
    key_rows = raw_key.astype(jnp.bfloat16)
    value_rows = projected[5].astype(jnp.bfloat16)
    gate_rows = lax.dynamic_slice_in_dim(forget_total, offset, tok_dev, 1).reshape(
        kv_local, group, tok_dev
    )
    last_row = offset + tok_dev - 1
    init = (
        jnp.zeros((kv_local, group, tok_dev, HEAD), jnp.float32),
        jnp.zeros((kv_local, group, tok_dev), jnp.float32),
    )
    key_piece = lax.all_gather(key_rows, "sp", axis=0, tiled=True)
    value_piece = lax.all_gather(value_rows, "sp", axis=0, tiled=True)
    count = key_piece.shape[0] // KEY_SPAN

    def one_block(index, inner):
        first = index * KEY_SPAN

        def compute(state):
            weighted, total = state
            key_block = lax.dynamic_slice_in_dim(key_piece, index * KEY_SPAN, KEY_SPAN, 0).reshape(
                KEY_SPAN, kv_local, HEAD
            )
            value_block = lax.dynamic_slice_in_dim(
                value_piece, index * KEY_SPAN, KEY_SPAN, 0
            ).reshape(KEY_SPAN, kv_local, HEAD)
            gate_keys = lax.dynamic_slice_in_dim(forget_total, first, KEY_SPAN, 1).reshape(
                kv_local, group, KEY_SPAN
            )
            scores = jnp.einsum(
                "tcgd,scd->cgts", query, key_block, preferred_element_type=jnp.float32
            )
            logits = scores + gate_rows[:, :, :, None] - gate_keys[:, :, None, :]
            allowed = (first + jnp.arange(KEY_SPAN, dtype=jnp.int32))[None, :] <= query_places[
                :, None
            ]
            weights = jnp.exp(jnp.where(allowed, logits, -jnp.inf))
            total = total + jnp.sum(weights, axis=-1)
            weighted = weighted + jnp.einsum(
                "cgts,scd->cgtd",
                weights.astype(jnp.bfloat16),
                value_block,
                preferred_element_type=jnp.float32,
            )
            return (weighted, total)

        def skipped(state):
            return state

        return lax.cond(first <= last_row, compute, skipped, inner)

    weighted, total = lax.fori_loop(0, count, one_block, init)
    result = weighted / total[..., None]
    attended = (
        jnp.transpose(result, (2, 0, 1, 3)).reshape(tok_dev, gate_heads * HEAD).astype(jnp.bfloat16)
    )
    out_ret, out_att = (
        lax.all_gather(w_out_ret, "sp", axis=1, tiled=True),
        lax.all_gather(w_out_att, "sp", axis=1, tiled=True),
    )
    return lax.psum_scatter(
        (
            jnp.dot(retained, out_ret, preferred_element_type=jnp.float32)
            + jnp.dot(attended, out_att, preferred_element_type=jnp.float32)
        ).astype(jnp.bfloat16),
        "tp",
        scatter_dimension=0,
        tiled=True,
    )


def choose(n, m, *arrays):
    tokens, w_key_ret, w_out_ret = arrays[0], arrays[3], arrays[8]
    whole_tiles = w_out_ret.shape[1] % LANES == 0 and w_key_ret.shape[0] % LANES == 0
    heads = arrays[10].shape[1]
    small = 16 * heads <= HEAD and arrays[7].shape[1] == HEAD and arrays[11].shape[0] == heads
    paired = n % 4 == 0 and n > 4 and m % 2 == 0 and m > 2
    if paired and whole_tiles and small and tokens.shape[0] * m == SPAN:
        return body(n, m, *arrays)
    return plain_body(*arrays)


def solution(mesh):
    return jax.shard_map(
        functools.partial(choose, mesh.shape["sp"], mesh.shape["tp"]),
        mesh=mesh,
        in_specs=(
            P(("sp", "tp"), None),
            P(),
            P("sp", "tp"),
            P("sp", "tp"),
            P("sp", "tp"),
            P("sp", "tp"),
            P("sp", "tp"),
            P("sp", "tp"),
            P("tp", "sp"),
            P("tp", "sp"),
            P("sp", "tp"),
            P("tp", None),
        ),
        out_specs=P(("sp", "tp"), None),
        check_vma=False,
    )
```
